32 devices in a mesh: sp: 4 (over y, x), tp: 8 (over z, core).
Axes of the slice: x: 2, y: 2, z: 4, core: 2. Of those that a mesh axis runs over, the one named last changes fastest.
Arguments:
- conv_value: bfloat16 [6144, 2048], P('sp', 'tp'), may hold values from -48 to 48
- conv_gate: bfloat16 [6144, 2048], P('sp', 'tp'), may hold values from -6 to 6
- doc_ids: int32 [6144], P('sp'), may hold values from 0 to 3, never falling along the last dimension, each value on 1 to 4608 neighbouring positions
- conv_kernel: bfloat16 [31, 2048], P(None, 'tp'), may hold values from -1 to 1
- norm_gain_conv: float32 [2048], replicated, may hold values from 0.1 to 1.9
- norm_bias_conv: float32 [2048], replicated, may hold values from -3 to 3
- proj_weight: bfloat16 [2048, 2048], P('tp'), may hold values from -0.125 to 0.125
- residual: bfloat16 [6144, 2048], P(('sp', 'tp')), may hold values from -6 to 6
- norm_gain_moe: float32 [2048], replicated, may hold values from 0.1 to 1.9
- group_router: bfloat16 [2048, 2], replicated, may hold values from -0.125 to 0.125
- expert_router: bfloat16 [2048, 4], replicated, may hold values from -0.125 to 0.125
- routing: int32 [6144, 2], P(('sp', 'tp')), may hold values from 0 to 3, as said below
- expert_gate_w: bfloat16 [4, 2048, 512], P('sp'), may hold values from -0.125 to 0.125
- expert_up_w: bfloat16 [4, 2048, 512], P('sp'), may hold values from -0.125 to 0.125
- expert_down_w: bfloat16 [4, 512, 2048], P('sp'), may hold values from -0.25 to 0.25
Outputs:
- output: bfloat16 [6144, 2048], P(('sp', 'tp'))
The draws below stay inside these ranges and needn't reach their ends.
Inputs may be any that keep to these rules, and one draw needn't show every extreme that they name: `routing`: both numbers of a row are different experts of one group (expert // 2); within the rows of one device (aligned blocks of 192 rows) every expert is named exactly 96 times.
All inputs are finite; a program needn't handle non-finite values.
Results may differ from the reference program's by a relative error of at most 0.015.
Values may be sent and summed in bfloat16 or wider, within the bound.
A program may use at most 64 MiB of HBM per device.

```python
import math
import jax
import jax.numpy as jnp
import numpy as np
from jax import lax

D = 2048
CH = 2048
KW = 31
FF = 512
GROUPS = 2
TOK_DEV = 192
EXPERTS = 4
TOKENS = 6144
DOCS = 4
DOC_MOST = 4608


def draw_conv_value(key, part):
    base_key = jax.random.fold_in(key, 101)
    column_key = jax.random.fold_in(key, 102)
    column_scale = 3.0 ** (jnp.arange(CH, dtype=jnp.float32) / CH) * jax.random.uniform(column_key, (CH,), jnp.float32, 0.6, 1.6)
    base = jnp.clip(jax.random.normal(base_key, (TOKENS, CH), jnp.float32), -6.0, 6.0)
    return (base * column_scale[None, :]).astype(jnp.bfloat16)


def draw_routing(key, part):
    blocks = TOKENS // TOK_DEV
    per_group = EXPERTS // GROUPS
    group_rows = TOK_DEV // GROUPS
    per_expert = TOK_DEV // EXPERTS
    shift_key = jax.random.fold_in(key, 201)
    flip_key = jax.random.fold_in(key, 202)
    shuffle_key = jax.random.fold_in(key, 203)
    rank_order = jnp.arange(TOK_DEV, dtype=jnp.int32)
    first_local = rank_order % group_rows // per_expert
    shifts = jax.random.randint(shift_key, (blocks,), 1, per_group, jnp.int32)
    flips = jax.random.randint(flip_key, (blocks,), 0, GROUPS, jnp.int32)
    group_index = (rank_order[None, :] // group_rows + flips[:, None]) % GROUPS
    second_local = (first_local[None, :] + shifts[:, None]) % per_group
    first_expert = group_index * per_group + first_local[None, :]
    second_expert = group_index * per_group + second_local
    pairing = jnp.stack([first_expert, second_expert], axis=-1).astype(jnp.int32)
    shuffles = jax.vmap(lambda block_key: jax.random.permutation(block_key, TOK_DEV))(jax.random.split(shuffle_key, blocks))

    def place_block(shuffle, block_pairs):
        return jnp.zeros((TOK_DEV, 2), jnp.int32).at[shuffle].set(block_pairs)
    routed = jax.vmap(place_block)(shuffles.astype(jnp.int32), pairing)
    return routed.reshape(TOKENS, 2).astype(jnp.int32)


def shard_levels(key, dims, cuts, smallest, high):
    loudness, own = 1.0, jax.random.fold_in(key, 6)
    for axis_at, shards_of in cuts:
        steps = jnp.exp(jax.random.uniform(jax.random.fold_in(own, axis_at), (shards_of,), jnp.float32, smallest / len(cuts), high / len(cuts)))
        loudness = loudness * jnp.repeat(steps, dims[axis_at] // shards_of).reshape([-1 if axis == axis_at else 1 for axis in range(len(dims))])
    return loudness


def length_profile(count, total, reach, lean):
    portions = [(1 << 20) // math.isqrt(grade ** lean) + 1 for grade in range(2, count + 1)]
    surplus, given = total - reach - (count - 1), [1] * (count - 1)
    while surplus > 0:
        movable = [i for i in range(count - 1) if given[i] < reach]
        mass, budget = sum([portions[i] for i in movable]), surplus
        for i in movable:
            more = min(reach - given[i], max(1, budget * portions[i] // mass), surplus)
            given[i] = given[i] + more
            surplus = surplus - more
    return np.array([reach] + given)


def ragged_sizes(rng, number_of, total, limit, skew):
    if number_of == 2:
        one = jax.random.randint(rng, (), max(1, total - limit), min(limit, total - 1) + 1)
        return jnp.stack([one, total - one])
    tallies = jnp.asarray(length_profile(number_of, total, limit, skew), jnp.int32)
    couples = (number_of - 1) // 2
    donor, taker = tallies[1:1 + 2 * couples:2], tallies[2:2 + 2 * couples:2]
    room = jnp.minimum(donor - 1, limit - taker)
    moved = jax.random.randint(jax.random.fold_in(rng, 1), (couples,), 0, 1 << 20) % (room + 1)
    tallies = tallies.at[1:1 + 2 * couples:2].set(donor - moved).at[2:2 + 2 * couples:2].set(taker + moved)
    return tallies[jax.random.permutation(jax.random.fold_in(rng, 2), number_of)]


def normal_values(key, extent, spread, limit, cuts=(), kind=jnp.bfloat16):
    array = jax.random.normal(key, extent, jnp.float32) * spread
    if len(cuts) > 0:
        array = shard_levels(key, extent, cuts, -0.22, 0.18) * array
    return jnp.clip(array, min=-limit, max=limit).astype(kind)


def setup_inputs(seed: int = 0) -> dict:
    seeds = jax.random.split(jax.random.key(seed), 16)
    return {
        "conv_value": draw_conv_value(jax.random.fold_in(seeds[15], 71), 0),
        "conv_gate": normal_values(seeds[1], (TOKENS, CH), 1.0, 6.0, ((0, 4), (1, 8))),
        "doc_ids": jnp.searchsorted(jnp.cumsum(ragged_sizes(seeds[2], DOCS, TOKENS, DOC_MOST, 0)), jnp.arange(TOKENS), side="right").astype(jnp.int32),
        "conv_kernel": normal_values(seeds[3], (KW, CH), KW ** -0.5, 1.0, ((1, 8),)),
        "norm_gain_conv": jnp.clip(1.0 + 0.18 * jax.random.normal(seeds[4], (CH,), jnp.float32), 0.1, 1.9),
        "norm_bias_conv": normal_values(seeds[5], (CH,), 0.5, 3.0, (), jnp.float32),
        "proj_weight": normal_values(seeds[6], (CH, D), CH ** -0.5, 0.125, ((0, 8),)),
        "residual": normal_values(seeds[7], (TOKENS, D), 1.0, 6.0, ((0, 32),)),
        "norm_gain_moe": jnp.clip(1.0 + 0.18 * jax.random.normal(seeds[8], (D,), jnp.float32), 0.1, 1.9),
        "group_router": normal_values(seeds[9], (D, GROUPS), D ** -0.5, 0.125),
        "expert_router": normal_values(seeds[10], (D, EXPERTS), D ** -0.5, 0.125),
        "routing": draw_routing(jax.random.fold_in(seeds[15], 71), 0),
        "expert_gate_w": normal_values(seeds[12], (EXPERTS, D, FF), D ** -0.5, 0.125, ((0, 4),)),
        "expert_up_w": normal_values(seeds[13], (EXPERTS, D, FF), D ** -0.5, 0.125, ((0, 4),)),
        "expert_down_w": normal_values(seeds[14], (EXPERTS, FF, D), FF ** -0.5, 0.25, ((0, 4),)),
    }


epsilon = 1e-06

def reference(conv_value, conv_gate, doc_ids, conv_kernel, norm_gain_conv, norm_bias_conv, proj_weight, residual, norm_gain_moe, group_router, expert_router, routing, expert_gate_w, expert_up_w, expert_down_w):
    gated_values = (conv_value.astype(jnp.float32) * jax.nn.sigmoid(conv_gate.astype(jnp.float32))).astype(jnp.bfloat16)
    rim_width = KW - 1
    length = gated_values.shape[0]
    padded = jnp.concatenate([jnp.zeros((rim_width, CH), jnp.bfloat16), gated_values], axis=0)
    padded_ids = jnp.concatenate([jnp.zeros((rim_width,), jnp.int32), doc_ids.astype(jnp.int32)], axis=0)
    kernel = conv_kernel.astype(jnp.float32)
    summed = jnp.zeros((length, CH), jnp.float32)
    for tap in range(KW):
        same_doc = padded_ids[tap:tap + length] == doc_ids
        summed = summed + jnp.where(same_doc[:, None], padded[tap:tap + length].astype(jnp.float32) * kernel[tap][None, :], jnp.float32(0.0))
    convolved = summed.astype(jnp.bfloat16)
    values = convolved.astype(jnp.float32)
    average = lax.optimization_barrier(jnp.mean(values, axis=1, keepdims=True))
    centered = values - average
    variance = lax.optimization_barrier(jnp.mean(centered * centered, axis=1, keepdims=True))
    activated = jax.nn.silu(centered * lax.rsqrt(variance + epsilon) * norm_gain_conv + norm_bias_conv).astype(jnp.bfloat16)
    projected = jnp.dot(activated, proj_weight, preferred_element_type=jnp.float32)
    hidden_state = (residual.astype(jnp.float32) + projected).astype(jnp.bfloat16)
    state_values = hidden_state.astype(jnp.float32)
    normed = (state_values * lax.rsqrt(lax.optimization_barrier(jnp.mean(state_values * state_values, axis=1, keepdims=True)) + epsilon) * norm_gain_moe).astype(jnp.bfloat16)
    group_logits = jnp.dot(normed, group_router, preferred_element_type=jnp.float32)
    expert_logits = jnp.dot(normed, expert_router, preferred_element_type=jnp.float32)
    per_group = EXPERTS // GROUPS
    chosen_group = (routing[:, 0] // per_group).astype(jnp.int32)
    group_exp = jnp.exp(group_logits)
    group_prob = jnp.take_along_axis(group_exp, chosen_group[:, None], axis=1)[:, 0] / lax.optimization_barrier(jnp.sum(group_exp, axis=1))
    first_logit = jnp.take_along_axis(expert_logits, routing[:, 0:1], axis=1)[:, 0]
    second_logit = jnp.take_along_axis(expert_logits, routing[:, 1:2], axis=1)[:, 0]
    first_exp = jnp.exp(first_logit)
    second_exp = jnp.exp(second_logit)
    first_weight = group_prob * first_exp / (first_exp + second_exp)
    second_weight = group_prob * second_exp / (first_exp + second_exp)
    per_expert = 2 * length // EXPERTS
    flat_experts = routing.reshape(-1).astype(jnp.int32)
    ordering = jnp.argsort(flat_experts, stable=True).astype(jnp.int32)
    slot_table = ordering.reshape(EXPERTS, per_expert)

    def one_expert(operands):
        assigned, gate_matrix, up_matrix, down_matrix = operands
        token_rows = normed[assigned // 2]
        gate_part = jnp.dot(token_rows, gate_matrix, preferred_element_type=jnp.float32)
        up_part = jnp.dot(token_rows, up_matrix, preferred_element_type=jnp.float32)
        expert_hidden = (jax.nn.silu(gate_part) * up_part).astype(jnp.bfloat16)
        return jnp.dot(expert_hidden, down_matrix, preferred_element_type=jnp.float32).astype(jnp.bfloat16)
    results = lax.map(one_expert, (slot_table, expert_gate_w, expert_up_w, expert_down_w))
    per_assignment = jnp.zeros((2 * length, D), jnp.bfloat16).at[slot_table.reshape(-1)].set(results.reshape(-1, D))
    picked = per_assignment.reshape(length, 2, D).astype(jnp.float32)
    mixture = first_weight[:, None] * picked[:, 0] + second_weight[:, None] * picked[:, 1]
    return (state_values + mixture).astype(jnp.bfloat16)
```

```python
import functools

import jax
import jax.numpy as jnp
from jax import lax
from jax.experimental import pallas as pl
from jax.experimental.pallas import tpu as pltpu
from jax.sharding import PartitionSpec as P

epsilon = 1e-06
MESH = pl.DeviceIdType.MESH
F32 = jnp.float32
BF16 = jnp.bfloat16
HALO = 32


def gate(value, gate_value):
    return (value.astype(F32) * jax.nn.sigmoid(gate_value.astype(F32))).astype(BF16)


def kernel(
    S,
    T,
    G,
    value_hbm,
    gate_hbm,
    ids_row_ref,
    ids_ref,
    kernel_ref,
    gain_conv_ref,
    bias_conv_ref,
    weight_hbm,
    residual_hbm,
    gain_moe_ref,
    group_router_ref,
    expert_router_ref,
    routing_ref,
    gate_w_hbm,
    up_w_hbm,
    down_w_hbm,
    out_ref,
    value,
    gates,
    wfull,
    residual,
    gate_w,
    up_w,
    down_w,
    rim_out,
    rim_in,
    padded,
    taps,
    least_tap,
    conv_out,
    conv_in,
    act,
    hidden,
    normed,
    picks,
    outgoing,
    arrived,
    ffn_hidden,
    results,
    returned,
    local_sem,
    wl_sem,
    rim_sem,
    wz_send,
    wz_recv,
    wx_send,
    wx_recv,
    wp_send,
    wp_recv,
    a2a_send,
    a2a_recv,
    disp_send,
    disp_recv,
    ret_send,
    ret_recv,
):
    s = lax.axis_index("sp")
    t = lax.axis_index("tp")
    Z = T // 2
    z = t // 2
    core = t % 2
    partner = 2 * z + 1 - core
    tokens, width = value.shape
    block = tokens // T
    n_taps = kernel_ref.shape[0]
    piece = wfull.shape[2]
    wrows = wfull.shape[1] // T
    D = S * piece
    square = S == 4
    H = 2
    part_rows = wrows // H

    def remote(src, dst, send, recv, sp_to, tp_to):
        return pltpu.make_async_remote_copy(
            src_ref=src,
            dst_ref=dst,
            send_sem=send,
            recv_sem=recv,
            device_id=(sp_to, tp_to),
            device_id_type=MESH,
        )

    loads = [
        pltpu.make_async_copy(a, b, local_sem.at[i])
        for i, (a, b) in enumerate(
            [
                (value_hbm, value),
                (gate_hbm, gates),
                (residual_hbm, residual),
                (gate_w_hbm, gate_w),
                (up_w_hbm, up_w),
                (down_w_hbm, down_w),
            ]
        )
    ]
    own_rows = pl.ds(pl.multiple_of(t * wrows, wrows), wrows)
    own_w = [
        pltpu.make_async_copy(
            weight_hbm.at[:, pl.ds(j * piece, piece)], wfull.at[j, own_rows, :], wl_sem.at[j]
        )
        for j in range(S)
    ]
    loads[0].start()
    loads[1].start()
    for c in own_w:
        c.start()
    for c in loads[2:]:
        c.start()

    ids_row = jnp.broadcast_to(ids_row_ref[...], (8, tokens))
    position = lax.broadcasted_iota(jnp.int32, (8, tokens), 1)
    low = jnp.int32(-n_taps)
    fresh = (ids_row != pltpu.roll(ids_row, 1, 1)) & (position > 0)
    begin = jnp.where(fresh, position, low)
    shift = 1
    while shift < n_taps:
        moved = jnp.where(position >= shift, pltpu.roll(begin, shift, 1), low)
        begin = jnp.maximum(begin, moved)
        shift *= 2
    least_row = (n_taps - 1 - position + begin).astype(F32)
    lanes = least_tap.shape[1]
    for c in range(tokens // lanes):
        across = jnp.broadcast_to(least_row[0:1, c * lanes : (c + 1) * lanes], (lanes, lanes))
        least_tap[c * lanes : (c + 1) * lanes, :] = across.T

    with jax.named_scope("barrier"):
        barrier = pltpu.get_barrier_semaphore()
        for k in range(1, T):
            pl.semaphore_signal(
                barrier, inc=1, device_id=(s, lax.rem(t + k, T)), device_id_type=MESH
            )
        for k in range(1, S):
            pl.semaphore_signal(
                barrier, inc=1, device_id=(lax.rem(s + k, S), t), device_id_type=MESH
            )
        pl.semaphore_wait(barrier, T + S - 2)

    def w_ref(o, p, h):
        base = pl.multiple_of((2 * o + core) * wrows + h * part_rows, part_rows)
        return wfull.at[p, pl.ds(base, part_rows), :]

    def z_copy(o, h, up, to):
        ref = w_ref(o, s, h)
        return remote(ref, ref, wz_send.at[up, o, h], wz_recv.at[o, h], s, 2 * to + core)

    def x_copy(o, p, h, lane_at, to):
        ref = w_ref(o, p, h)
        return remote(ref, ref, wx_send.at[lane_at, o, h], wx_recv.at[p, o, h], to, t)

    def p_copy(o, p):
        rows_at = pl.ds(pl.multiple_of((2 * o + core) * wrows, wrows), wrows)
        ref = wfull.at[p, rows_at, :]
        return remote(ref, ref, wp_send.at[o, p], wp_recv.at[o, p], s, partner)

    def p_wait(o, p):
        rows_at = pl.ds(pl.multiple_of((2 * o + 1 - core) * wrows, wrows), wrows)
        ref = wfull.at[p, rows_at, :]
        remote(ref, ref, wp_send.at[o, p], wp_recv.at[o, p], s, partner).wait_recv()

    has_up = z + 1 < Z
    has_down = z > 0
    for j in range(S):
        own_w[j].wait()
    for h in range(H):

        @pl.when(has_up)
        def _():
            z_copy(z, h, 0, z + 1).start()

        @pl.when(has_down)
        def _():
            z_copy(z, h, 1, z - 1).start()

    for j in range(S):
        p_copy(z, j).start()

    def sides(k):
        return ((z - k, z - k >= 0, 0), (z + k, z + k < Z, 1))

    def each_slice(k, act_on):
        for o, there, side in sides(k):
            pl.when(there)(functools.partial(act_on, o, side))

    nbr_x = s + 1 - 2 * (s % 2)
    nbr_y = s + 2 - 4 * (s // 2)
    diag = 3 - s

    def z_step(k, h):
        def one(o, side):
            z_copy(o, h, side, z).wait_recv()
            beyond = has_down if side else has_up

            @pl.when(beyond)
            def _():
                z_copy(o, h, side, z - 1 if side else z + 1).start()

            if square:
                x_copy(o, s, h, 0, nbr_x).start()
                x_copy(o, s, h, 1, nbr_y).start()
            else:
                for j in range(1, S):
                    x_copy(o, s, h, j - 1, lax.rem(s + j, S)).start()

        with jax.named_scope(f"z{k}{h}"):
            each_slice(k, one)

    def x_step(k):
        def one(o, side):
            x_copy(o, nbr_x, 0, 2, nbr_y).wait_recv()
            x_copy(o, nbr_x, 0, 2, nbr_y).start()

        if square:
            with jax.named_scope(f"x{k}"):
                each_slice(k, one)

    def y_step(k):
        def one(o, side):
            x_copy(o, nbr_y, 1, 2, nbr_x).wait_recv()
            x_copy(o, nbr_y, 1, 2, nbr_x).start()

        if square:
            with jax.named_scope(f"y{k}"):
                each_slice(k, one)

    def finish_row(k):
        def one(o, side):
            p_copy(o, s).start()
            if square:
                x_copy(o, nbr_x, 1, 0, nbr_x).wait_recv()
                p_copy(o, nbr_x).start()
                x_copy(o, nbr_y, 0, 0, nbr_y).wait_recv()
                p_copy(o, nbr_y).start()
                x_copy(o, diag, 0, 0, diag).wait_recv()
                x_copy(o, diag, 1, 0, diag).wait_recv()
                p_copy(o, diag).start()
            else:
                for j in range(1, S):
                    p = lax.rem(s + S - j, S)
                    for h in range(H):
                        x_copy(o, p, h, j - 1, p).wait_recv()
                    p_copy(o, p).start()

        with jax.named_scope(f"fin{k}"):
            each_slice(k, one)

    loads[0].wait()
    loads[1].wait()
    tail = pl.ds(tokens - HALO, HALO)
    last_reach = jnp.max(least_tap[tokens - 1 : tokens, :], axis=1, keepdims=True)
    row_at = lax.broadcasted_iota(jnp.int32, (HALO, width), 0).astype(F32)
    newer = row_at >= last_reach + (HALO - n_taps)
    rim = jnp.where(newer, gate(value[tail, :], gates[tail, :]).astype(F32), jnp.float32(0.0))
    rim_out[0:HALO, :] = rim.astype(BF16)
    rim_out[HALO : HALO + 16, :] = jnp.full(
        (16, width), ids_ref[tokens - 1].astype(F32), F32
    ).astype(BF16)
    rim_copy = remote(
        rim_out, rim_in, rim_sem.at[0], rim_sem.at[1], lax.rem(s + 1, S), t
    )
    rim_copy.start()

    def gate_rows(i, _):
        rows = pl.ds(pl.multiple_of(i * 64, 64), 64)
        to_rows = pl.ds(pl.multiple_of(HALO + i * 64, 32), 64)
        padded[to_rows, :] = gate(value[rows, :], gates[rows, :]).astype(F32)
        return 0

    with jax.named_scope("gate"):
        lax.fori_loop(0, tokens // 64, gate_rows, 0)
    taps[0:n_taps, :] = kernel_ref[...].astype(F32)

    step_rows = 32 if block % 32 == 0 else 8
    lanes = min(width, 128)

    def conv_block(owner):
        def conv_rows(i, _):
            base = pl.multiple_of(owner * block + i * step_rows, 8)
            least = least_tap[pl.ds(base, step_rows), :]
            window = padded[pl.ds(base, step_rows + HALO), :]
            total = jnp.zeros((step_rows, width), F32)
            for tap in range(n_taps):
                at = tap + HALO + 1 - n_taps
                valid = least <= tap
                product = window[at : at + step_rows, :] * taps[tap : tap + 1, :]
                parts = [
                    jnp.where(valid, product[:, j : j + lanes], jnp.float32(0.0))
                    for j in range(0, width, lanes)
                ]
                total = total + jnp.concatenate(parts, axis=1)
            conv_out[
                owner, pl.ds(pl.multiple_of(i * step_rows, step_rows), step_rows), :
            ] = total.astype(BF16)
            return 0

        lax.fori_loop(0, block // step_rows, conv_rows, 0)

    def conv_some(first, last):
        with jax.named_scope("conv"):

            def one(owner, _):
                conv_block(owner)
                return 0

            lax.fori_loop(first, last, one, 0)

    def conv_copy(to):
        return remote(
            conv_out.at[to], conv_in.at[t], a2a_send.at[to], a2a_recv.at[t], s, to
        )

    def conv_flush(first, last):
        def one(k, _):
            owner = lax.rem(t + k, T)

            @pl.when((owner >= first) & (owner < last))
            def _():
                conv_copy(owner).start()

            return 0

        lax.fori_loop(1, T, one, 0)

    marks = [1 + (T - 1) * i // 7 for i in (3, 5, 7)]
    conv_some(1, marks[0])
    z_step(1, 0)
    conv_some(marks[0], marks[1])
    z_step(1, 1)
    conv_some(marks[1], marks[2])
    z_step(2, 0)
    x_step(1)
    with jax.named_scope("rimwait"):
        rim_copy.wait()
    same = (rim_in[HALO : HALO + 1, :].astype(F32) == ids_ref[0].astype(F32)) & (s > 0)
    padded[0:HALO, :] = jnp.where(same, rim_in[0:HALO, :].astype(F32), jnp.float32(0.0))
    conv_some(0, 1)
    z_step(2, 1)
    conv_flush(0, T)
    y_step(1)
    conv_in[t, :, :] = conv_out[t, :, :]

    rows = block
    E = S
    cap = 2 * rows // E
    lane = lax.broadcasted_iota(jnp.int32, (rows, 128), 1)
    eye = lax.broadcasted_iota(jnp.int32, (rows, rows), 0) == lax.broadcasted_iota(
        jnp.int32, (rows, rows), 1
    )
    named = lax.dot_general(
        eye.astype(F32).astype(BF16),
        routing_ref[...].astype(F32).astype(BF16),
        (((1,), (1,)), ((), ())),
        preferred_element_type=F32,
    )
    first = named[:, 0:1]
    second = named[:, 1:2]
    lane_f = lane.astype(F32)
    chosen = (lane_f == first) | (lane_f == second)
    per_group = E // G
    group_low = lane_f * per_group
    in_group = (first >= group_low) & (first < group_low + per_group)
    row_i = lax.broadcasted_iota(jnp.int32, (rows, rows), 0)
    col_i = lax.broadcasted_iota(jnp.int32, (rows, rows), 1)
    before = jnp.dot(
        (row_i > col_i).astype(F32).astype(BF16),
        chosen.astype(F32).astype(BF16),
        preferred_element_type=F32,
    )
    slot = jnp.where(chosen, before, jnp.float32(-1.0))
    width_e = max(E, 8)
    expert_i = lax.broadcasted_iota(jnp.int32, (width_e, rows), 0)
    chosen_r = (routing_ref[0:1, :] == expert_i) | (routing_ref[1:2, :] == expert_i)
    before_r = jnp.dot(
        chosen_r.astype(F32).astype(BF16),
        (row_i < col_i).astype(F32).astype(BF16),
        preferred_element_type=F32,
    )
    slot_r = jnp.where(chosen_r, before_r, jnp.float32(-1.0))
    cap_i = lax.broadcasted_iota(jnp.int32, (cap, rows), 0).astype(F32)
    for e in range(E):
        picks[e, :, :] = (slot_r[e : e + 1, :] == cap_i).astype(F32).astype(BF16)

    for k in range(3, Z):
        z_step(k, 0)
        x_step(k - 1)
        z_step(k, 1)
        finish_row(k - 2)
        y_step(k - 1)
    finish_row(Z - 2)
    x_step(Z - 1)
    y_step(Z - 1)

    total = jnp.zeros((rows, 1), F32)
    with jax.named_scope("a2await"):
        for k in range(1, T):
            source = lax.rem(t + k, T)
            remote(
                conv_out.at[source],
                conv_in.at[source],
                a2a_send.at[source],
                a2a_recv.at[source],
                s,
                source,
            ).wait_recv()
    with jax.named_scope("act"):
        for j in range(T):
            total = total + jnp.sum(conv_in[j].astype(F32), axis=1, keepdims=True)
        average = total / (T * width)
        total = jnp.zeros((rows, 1), F32)
        for j in range(T):
            centered = conv_in[j].astype(F32) - average
            total = total + jnp.sum(centered * centered, axis=1, keepdims=True)
        scale = lax.rsqrt(total / (T * width) + epsilon)
        for j in range(T):
            cols = slice(j * width, (j + 1) * width)
            v = (conv_in[j].astype(F32) - average) * scale * gain_conv_ref[
                :, cols
            ] + bias_conv_ref[:, cols]
            act[:, cols] = (v / (1.0 + jnp.exp(-v))).astype(BF16)

    finish_row(Z - 1)
    loads[2].wait()
    with jax.named_scope("wpwait"):
        for o in range(Z):
            for j in range(S):
                p_wait(o, j)

    def project(j, squares):
        cols = pl.ds(pl.multiple_of(j * piece, piece), piece)
        acc = residual[:, cols].astype(F32)
        part = jnp.dot(act[...], wfull[j], preferred_element_type=F32)
        state = (acc + part).astype(BF16)
        hidden[:, cols] = state
        state = state.astype(F32)
        return squares + jnp.sum(state * state, axis=1, keepdims=True)

    with jax.named_scope("project"):
        squares = lax.fori_loop(0, S, project, jnp.zeros((rows, 1), F32))
    scale = lax.rsqrt(squares / D + epsilon)

    def norm_cols(j, _):
        cols = pl.ds(pl.multiple_of(j * piece, piece), piece)
        normed[:, cols] = (hidden[:, cols].astype(F32) * scale * gain_moe_ref[:, cols]).astype(BF16)
        return 0

    with jax.named_scope("norm"):
        lax.fori_loop(0, S, norm_cols, 0)

    slot_iota = lax.broadcasted_iota(jnp.int32, (rows, cap), 1).astype(F32)

    def column(array, expert):
        mine = lane[:, : array.shape[1]] == expert
        return jnp.sum(jnp.where(mine, array, jnp.float32(0.0)), axis=1, keepdims=True)

    def gather_rows(expert, target):
        def cols_step(j, _):
            cols = pl.ds(pl.multiple_of(j * piece, piece), piece)
            target[:, cols] = jnp.dot(
                picks[expert], normed[:, cols], preferred_element_type=F32
            ).astype(BF16)
            return 0

        lax.fori_loop(0, S, cols_step, 0)

    with jax.named_scope("dispatch"):
        for k in range(1, S):
            expert = lax.rem(s + k, S)
            gather_rows(expert, outgoing.at[expert])
            remote(
                outgoing.at[expert], arrived.at[s], disp_send.at[expert], disp_recv.at[s], expert, t
            ).start()
        gather_rows(s, arrived.at[s])

    def logits(router):
        return lax.dot_general(
            normed[...], router[...], (((1,), (1,)), ((), ())), preferred_element_type=F32
        )

    group_exp = jnp.exp(logits(group_router_ref))
    expert_exp = jnp.exp(logits(expert_router_ref))
    zero = jnp.float32(0.0)
    group_prob = jnp.sum(
        jnp.where(in_group[:, :G], group_exp, zero), axis=1, keepdims=True
    ) / jnp.sum(group_exp, axis=1, keepdims=True)
    chosen_exp = jnp.where(chosen[:, :E], expert_exp, zero)
    mix = group_prob * chosen_exp / jnp.sum(chosen_exp, axis=1, keepdims=True)

    for c in loads[3:]:
        c.wait()
    ff = gate_w.shape[2]
    ff_step = min(ff, 256)

    def expert_block(sender, target):
        def up_step(j, _):
            cols = pl.ds(pl.multiple_of(j * ff_step, ff_step), ff_step)
            x = arrived[sender]
            g = jnp.dot(x, gate_w[0, :, cols], preferred_element_type=F32)
            u = jnp.dot(x, up_w[0, :, cols], preferred_element_type=F32)
            ffn_hidden[:, cols] = (g / (1.0 + jnp.exp(-g)) * u).astype(BF16)
            return 0

        lax.fori_loop(0, ff // ff_step, up_step, 0)

        def down_step(j, _):
            cols = pl.ds(pl.multiple_of(j * piece, piece), piece)
            target[:, cols] = jnp.dot(
                ffn_hidden[...], down_w[0, :, cols], preferred_element_type=F32
            ).astype(BF16)
            return 0

        lax.fori_loop(0, S, down_step, 0)

    with jax.named_scope("ffnown"):
        expert_block(s, returned.at[s])
    for k in range(1, S):
        sender = lax.rem(s - k + S, S)
        remote(
            outgoing.at[sender], arrived.at[sender], disp_send.at[sender], disp_recv.at[sender], sender, t
        ).wait_recv()
        expert_block(sender, results.at[sender])
        remote(
            results.at[sender], returned.at[s], ret_send.at[sender], ret_recv.at[s], sender, t
        ).start()

    for k in range(1, S):
        expert = lax.rem(s + k, S)
        remote(
            results.at[expert], returned.at[expert], ret_send.at[expert], ret_recv.at[expert], expert, t
        ).wait_recv()
    spreads = [
        jnp.where(column(slot, e) == slot_iota, column(mix, e), zero).astype(BF16)
        for e in range(E)
    ]

    def combine(j, _):
        cols = pl.ds(pl.multiple_of(j * piece, piece), piece)
        acc = jnp.zeros((rows, piece), F32)
        for e in range(E):
            acc = acc + jnp.dot(spreads[e], returned[e, :, cols], preferred_element_type=F32)
        out_ref[:, cols] = (hidden[:, cols].astype(F32) + acc).astype(BF16)
        return 0

    with jax.named_scope("combine"):
        lax.fori_loop(0, S, combine, 0)

    with jax.named_scope("sendwait"):
        for h in range(H):

            @pl.when(has_up)
            def _():
                z_copy(z, h, 0, z + 1).wait_send()

            @pl.when(has_down)
            def _():
                z_copy(z, h, 1, z - 1).wait_send()

        for j in range(S):
            p_copy(z, j).wait_send()
        def sent(o, side):
            beyond = has_down if side else has_up
            for h in range(H):

                @pl.when(beyond)
                def _():
                    z_copy(o, h, side, z - 1 if side else z + 1).wait_send()

                for j in range(3 if square else S - 1):
                    x_copy(o, s, h, j, lax.rem(s + 1, S)).wait_send()
            for j in range(S):
                p_copy(o, j).wait_send()

        for k in range(1, Z):
            each_slice(k, sent)
        for k in range(1, T):
            conv_copy(lax.rem(t + k, T)).wait_send()
        for k in range(1, S):
            to = lax.rem(s + k, S)
            remote(
                outgoing.at[to], arrived.at[s], disp_send.at[to], disp_recv.at[s], to, t
            ).wait_send()
            remote(
                results.at[to], returned.at[s], ret_send.at[to], ret_recv.at[s], to, t
            ).wait_send()


def body(
    S,
    T,
    conv_value,
    conv_gate,
    doc_ids,
    conv_kernel,
    norm_gain_conv,
    norm_bias_conv,
    proj_weight,
    residual,
    norm_gain_moe,
    group_router,
    expert_router,
    routing,
    expert_gate_w,
    expert_up_w,
    expert_down_w,
):
    tokens, width = conv_value.shape
    rows, D = residual.shape
    wrows = proj_weight.shape[0]
    ff = expert_gate_w.shape[2]
    G = group_router.shape[1]
    E = expert_router.shape[1]
    cap = 2 * rows // E
    vmem = pl.BlockSpec(memory_space=pltpu.VMEM)
    hbm = pl.BlockSpec(memory_space=pl.ANY)
    smem = pl.BlockSpec(memory_space=pltpu.SMEM)
    dma = pltpu.SemaphoreType.DMA
    piece = D // S
    Z = T // 2
    return pl.pallas_call(
        functools.partial(kernel, S, T, G),
        out_shape=jax.ShapeDtypeStruct((rows, D), BF16),
        in_specs=[
            hbm, hbm, vmem, smem, vmem, vmem, vmem, hbm, hbm, vmem, vmem, vmem, vmem,
            hbm, hbm, hbm,
        ],
        out_specs=vmem,
        scratch_shapes=[
            pltpu.VMEM((tokens, width), BF16),
            pltpu.VMEM((tokens, width), BF16),
            pltpu.VMEM((S, T * wrows, piece), BF16),
            pltpu.VMEM((rows, D), BF16),
            pltpu.VMEM((1, D, ff), BF16),
            pltpu.VMEM((1, D, ff), BF16),
            pltpu.VMEM((1, ff, D), BF16),
            pltpu.VMEM((HALO + 16, width), BF16),
            pltpu.VMEM((HALO + 16, width), BF16),
            pltpu.VMEM((tokens + HALO, width), F32),
            pltpu.VMEM((32, width), F32),
            pltpu.VMEM((tokens, 128), F32),
            pltpu.VMEM((T, rows, width), BF16),
            pltpu.VMEM((T, rows, width), BF16),
            pltpu.VMEM((rows, T * width), BF16),
            pltpu.VMEM((rows, D), BF16),
            pltpu.VMEM((rows, D), BF16),
            pltpu.VMEM((E, cap, rows), BF16),
            pltpu.VMEM((E, cap, D), BF16),
            pltpu.VMEM((E, cap, D), BF16),
            pltpu.VMEM((cap, ff), BF16),
            pltpu.VMEM((E, cap, D), BF16),
            pltpu.VMEM((E, cap, D), BF16),
            dma((6,)),
            dma((S,)),
            dma((2,)),
            dma((2, Z, 2)),
            dma((Z, 2)),
            dma((max(S - 1, 3), Z, 2)),
            dma((S, Z, 2)),
            dma((Z, S)),
            dma((Z, S)),
            dma((T,)),
            dma((T,)),
            dma((S,)),
            dma((S,)),
            dma((S,)),
            dma((S,)),
        ],
        compiler_params=pltpu.CompilerParams(
            collective_id=0, has_side_effects=True, vmem_limit_bytes=60 * 1024 * 1024
        ),
    )(
        conv_value,
        conv_gate,
        doc_ids[None, :],
        doc_ids,
        conv_kernel,
        norm_gain_conv[None, :],
        norm_bias_conv[None, :],
        proj_weight,
        residual,
        norm_gain_moe[None, :],
        group_router.T,
        expert_router.T,
        routing.T,
        expert_gate_w,
        expert_up_w,
        expert_down_w,
    )


def solution(mesh):
    placed = (
        P("sp", "tp"),
        P("sp", "tp"),
        P("sp"),
        P(None, "tp"),
        P(),
        P(),
        P("tp", None),
        P(("sp", "tp"), None),
        P(),
        P(),
        P(),
        P(("sp", "tp"), None),
        P("sp", None, None),
        P("sp", None, None),
        P("sp", None, None),
    )
    return jax.shard_map(
        functools.partial(body, mesh.shape["sp"], mesh.shape["tp"]),
        mesh=mesh,
        in_specs=placed,
        out_specs=P(("sp", "tp"), None),
        check_vma=False,
    )
```

```python
import functools

import jax
import jax.numpy as jnp
from jax import lax
from jax.experimental import pallas as pl
from jax.experimental.pallas import tpu as pltpu
from jax.sharding import PartitionSpec as P

epsilon = 1e-06
MESH = pl.DeviceIdType.MESH
F32 = jnp.float32
BF16 = jnp.bfloat16
HALO = 32


def gate(value, gate_value):
    return (value.astype(F32) * jax.nn.sigmoid(gate_value.astype(F32))).astype(BF16)


def kernel(
    S,
    T,
    G,
    value_hbm,
    gate_hbm,
    ids_row_ref,
    ids_ref,
    kernel_ref,
    gain_conv_ref,
    bias_conv_ref,
    weight_hbm,
    residual_hbm,
    gain_moe_ref,
    group_router_ref,
    expert_router_ref,
    routing_ref,
    gate_w_hbm,
    up_w_hbm,
    down_w_hbm,
    out_ref,
    value,
    gates,
    wfull,
    residual,
    gate_w,
    up_w,
    down_w,
    rim_out,
    rim_in,
    padded,
    taps,
    least_tap,
    conv_out,
    conv_in,
    act,
    hidden,
    normed,
    normed_in,
    picks,
    spreads,
    outgoing,
    arrived,
    ffn_hidden,
    results,
    returned,
    local_sem,
    wl_sem,
    rim_sem,
    wz_send,
    wz_recv,
    wx_send,
    wx_recv,
    wp_send,
    wp_recv,
    a2a_send,
    a2a_recv,
    disp_send,
    disp_recv,
    ret_send,
    ret_recv,
    out_sem,
):
    s = lax.axis_index("sp")
    t = lax.axis_index("tp")
    Z = T // 2
    z = t // 2
    core = t % 2
    partner = 2 * z + 1 - core
    tokens, width = value.shape
    block = tokens // T
    n_taps = kernel_ref.shape[0]
    piece = wfull.shape[2]
    wrows = wfull.shape[1] // T
    D = S * piece
    square = S == 4
    H = 2
    part_rows = wrows // H

    def remote(src, dst, send, recv, sp_to, tp_to):
        return pltpu.make_async_remote_copy(
            src_ref=src,
            dst_ref=dst,
            send_sem=send,
            recv_sem=recv,
            device_id=(sp_to, tp_to),
            device_id_type=MESH,
        )

    loads = [
        pltpu.make_async_copy(a, b, local_sem.at[i])
        for i, (a, b) in enumerate(
            [
                (value_hbm, value),
                (gate_hbm, gates),
                (residual_hbm, residual),
                (gate_w_hbm, gate_w),
                (up_w_hbm, up_w),
                (down_w_hbm, down_w),
            ]
        )
    ]
    own_rows = pl.ds(pl.multiple_of(t * wrows, wrows), wrows)
    own_w = [
        pltpu.make_async_copy(
            weight_hbm.at[:, pl.ds(j * piece, piece)], wfull.at[j, own_rows, :], wl_sem.at[j]
        )
        for j in range(S)
    ]
    loads[0].start()
    loads[1].start()
    for c in own_w:
        c.start()
    for c in loads[2:]:
        c.start()

    ids_row = jnp.broadcast_to(ids_row_ref[...], (8, tokens))
    position = lax.broadcasted_iota(jnp.int32, (8, tokens), 1)
    low = jnp.int32(-n_taps)
    fresh = (ids_row != pltpu.roll(ids_row, 1, 1)) & (position > 0)
    begin = jnp.where(fresh, position, low)
    shift = 1
    while shift < n_taps:
        moved = jnp.where(position >= shift, pltpu.roll(begin, shift, 1), low)
        begin = jnp.maximum(begin, moved)
        shift *= 2
    least_row = (n_taps - 1 - position + begin).astype(F32)
    lanes = least_tap.shape[1]
    for c in range(tokens // lanes):
        across = jnp.broadcast_to(least_row[0:1, c * lanes : (c + 1) * lanes], (lanes, lanes))
        least_tap[c * lanes : (c + 1) * lanes, :] = across.T

    with jax.named_scope("barrier"):
        barrier = pltpu.get_barrier_semaphore()
        for k in range(1, T):
            pl.semaphore_signal(
                barrier, inc=1, device_id=(s, lax.rem(t + k, T)), device_id_type=MESH
            )
        for k in range(1, S):
            pl.semaphore_signal(
                barrier, inc=1, device_id=(lax.rem(s + k, S), t), device_id_type=MESH
            )
        pl.semaphore_wait(barrier, T + S - 2)

    def w_ref(o, p, h):
        base = pl.multiple_of((2 * o + core) * wrows + h * part_rows, part_rows)
        return wfull.at[p, pl.ds(base, part_rows), :]

    def z_copy(o, h, up, to):
        ref = w_ref(o, s, h)
        return remote(ref, ref, wz_send.at[up, o, h], wz_recv.at[o, h], s, 2 * to + core)

    def x_copy(o, p, h, lane_at, to):
        ref = w_ref(o, p, h)
        return remote(ref, ref, wx_send.at[lane_at, o, h], wx_recv.at[p, o, h], to, t)

    def p_copy(o, p):
        rows_at = pl.ds(pl.multiple_of((2 * o + core) * wrows, wrows), wrows)
        ref = wfull.at[p, rows_at, :]
        return remote(ref, ref, wp_send.at[o, p], wp_recv.at[o, p], s, partner)

    def p_wait(o, p):
        rows_at = pl.ds(pl.multiple_of((2 * o + 1 - core) * wrows, wrows), wrows)
        ref = wfull.at[p, rows_at, :]
        remote(ref, ref, wp_send.at[o, p], wp_recv.at[o, p], s, partner).wait_recv()

    has_up = z + 1 < Z
    has_down = z > 0
    for j in range(S):
        own_w[j].wait()
    for h in range(H):

        @pl.when(has_up)
        def _():
            z_copy(z, h, 0, z + 1).start()

        @pl.when(has_down)
        def _():
            z_copy(z, h, 1, z - 1).start()

    for j in range(S):
        p_copy(z, j).start()

    def sides(k):
        return ((z - k, z - k >= 0, 0), (z + k, z + k < Z, 1))

    def each_slice(k, act_on):
        for o, there, side in sides(k):
            pl.when(there)(functools.partial(act_on, o, side))

    nbr_x = s + 1 - 2 * (s % 2)
    nbr_y = s + 2 - 4 * (s // 2)
    diag = 3 - s

    def z_step(k, h):
        def one(o, side):
            z_copy(o, h, side, z).wait_recv()
            beyond = has_down if side else has_up

            @pl.when(beyond)
            def _():
                z_copy(o, h, side, z - 1 if side else z + 1).start()

            if square:
                x_copy(o, s, h, 0, nbr_x).start()
                x_copy(o, s, h, 1, nbr_y).start()
            else:
                for j in range(1, S):
                    x_copy(o, s, h, j - 1, lax.rem(s + j, S)).start()

        with jax.named_scope(f"z{k}{h}"):
            each_slice(k, one)

    def x_step(k):
        def one(o, side):
            x_copy(o, nbr_x, 0, 2, nbr_y).wait_recv()
            x_copy(o, nbr_x, 0, 2, nbr_y).start()

        if square:
            with jax.named_scope(f"x{k}"):
                each_slice(k, one)

    def y_step(k):
        def one(o, side):
            x_copy(o, nbr_y, 1, 2, nbr_x).wait_recv()
            x_copy(o, nbr_y, 1, 2, nbr_x).start()

        if square:
            with jax.named_scope(f"y{k}"):
                each_slice(k, one)

    def finish_row(k):
        def one(o, side):
            p_copy(o, s).start()
            if square:
                x_copy(o, nbr_x, 1, 0, nbr_x).wait_recv()
                p_copy(o, nbr_x).start()
                x_copy(o, nbr_y, 0, 0, nbr_y).wait_recv()
                p_copy(o, nbr_y).start()
                x_copy(o, diag, 0, 0, diag).wait_recv()
                x_copy(o, diag, 1, 0, diag).wait_recv()
                p_copy(o, diag).start()
            else:
                for j in range(1, S):
                    p = lax.rem(s + S - j, S)
                    for h in range(H):
                        x_copy(o, p, h, j - 1, p).wait_recv()
                    p_copy(o, p).start()

        with jax.named_scope(f"fin{k}"):
            each_slice(k, one)

    loads[0].wait()
    loads[1].wait()
    tail = pl.ds(tokens - HALO, HALO)
    last_reach = jnp.max(least_tap[tokens - 1 : tokens, :], axis=1, keepdims=True)
    row_at = lax.broadcasted_iota(jnp.int32, (HALO, width), 0).astype(F32)
    newer = row_at >= last_reach + (HALO - n_taps)
    rim = jnp.where(newer, gate(value[tail, :], gates[tail, :]).astype(F32), jnp.float32(0.0))
    rim_out[0:HALO, :] = rim.astype(BF16)
    rim_out[HALO : HALO + 16, :] = jnp.full(
        (16, width), ids_ref[tokens - 1].astype(F32), F32
    ).astype(BF16)
    rim_copy = remote(
        rim_out, rim_in, rim_sem.at[0], rim_sem.at[1], lax.rem(s + 1, S), t
    )
    rim_copy.start()

    def gate_rows(i, _):
        rows = pl.ds(pl.multiple_of(i * 64, 64), 64)
        to_rows = pl.ds(pl.multiple_of(HALO + i * 64, 32), 64)
        padded[to_rows, :] = gate(value[rows, :], gates[rows, :]).astype(F32)
        return 0

    with jax.named_scope("gate"):
        lax.fori_loop(0, tokens // 64, gate_rows, 0)
    taps[0:n_taps, :] = kernel_ref[...].astype(F32)

    step_rows = 32 if block % 32 == 0 else 8
    lanes = min(width, 128)

    def conv_block(owner):
        def conv_rows(i, _):
            base = pl.multiple_of(owner * block + i * step_rows, 8)
            least = least_tap[pl.ds(base, step_rows), :]
            window = padded[pl.ds(base, step_rows + HALO), :]
            total = jnp.zeros((step_rows, width), F32)
            for tap in range(n_taps):
                at = tap + HALO + 1 - n_taps
                valid = least <= tap
                product = window[at : at + step_rows, :] * taps[tap : tap + 1, :]
                parts = [
                    jnp.where(valid, product[:, j : j + lanes], jnp.float32(0.0))
                    for j in range(0, width, lanes)
                ]
                total = total + jnp.concatenate(parts, axis=1)
            conv_out[
                owner, pl.ds(pl.multiple_of(i * step_rows, step_rows), step_rows), :
            ] = total.astype(BF16)
            return 0

        lax.fori_loop(0, block // step_rows, conv_rows, 0)

    def conv_some(first, last):
        with jax.named_scope("conv"):

            def one(owner, _):
                conv_block(owner)
                return 0

            lax.fori_loop(first, last, one, 0)

    def conv_copy(to):
        return remote(
            conv_out.at[to], conv_in.at[t], a2a_send.at[to], a2a_recv.at[t], s, to
        )

    def conv_flush():
        conv_copy(partner).start()
        for far in range(1, Z):
            for to, there, _ in sides(far):

                @pl.when(there)
                def _():
                    for c in range(2):
                        conv_copy(2 * to + c).start()

    marks = [1 + (T - 1) * i // 7 for i in (3, 5, 7)]
    conv_some(1, marks[0])
    z_step(1, 0)
    conv_some(marks[0], marks[1])
    z_step(1, 1)
    conv_some(marks[1], marks[2])
    z_step(2, 0)
    x_step(1)
    with jax.named_scope("rimwait"):
        rim_copy.wait()
    same = (rim_in[HALO : HALO + 1, :].astype(F32) == ids_ref[0].astype(F32)) & (s > 0)
    padded[0:HALO, :] = jnp.where(same, rim_in[0:HALO, :].astype(F32), jnp.float32(0.0))
    conv_some(0, 1)
    z_step(2, 1)
    conv_flush()
    y_step(1)
    conv_in[t, :, :] = conv_out[t, :, :]

    rows = block
    E = S
    cap = 2 * rows // E
    lane = lax.broadcasted_iota(jnp.int32, (rows, 128), 1)
    eye = lax.broadcasted_iota(jnp.int32, (rows, rows), 0) == lax.broadcasted_iota(
        jnp.int32, (rows, rows), 1
    )
    named = lax.dot_general(
        eye.astype(F32).astype(BF16),
        routing_ref[...].astype(F32).astype(BF16),
        (((1,), (1,)), ((), ())),
        preferred_element_type=F32,
    )
    first = named[:, 0:1]
    second = named[:, 1:2]
    lane_f = lane.astype(F32)
    chosen = (lane_f == first) | (lane_f == second)
    per_group = E // G
    group_low = lane_f * per_group
    in_group = (first >= group_low) & (first < group_low + per_group)
    row_i = lax.broadcasted_iota(jnp.int32, (rows, rows), 0)
    col_i = lax.broadcasted_iota(jnp.int32, (rows, rows), 1)
    before = jnp.dot(
        (row_i > col_i).astype(F32).astype(BF16),
        chosen.astype(F32).astype(BF16),
        preferred_element_type=F32,
    )
    slot = jnp.where(chosen, before, jnp.float32(-1.0))
    width_e = max(E, 8)
    expert_i = lax.broadcasted_iota(jnp.int32, (width_e, rows), 0)
    chosen_r = (routing_ref[0:1, :] == expert_i) | (routing_ref[1:2, :] == expert_i)
    before_r = jnp.dot(
        chosen_r.astype(F32).astype(BF16),
        (row_i < col_i).astype(F32).astype(BF16),
        preferred_element_type=F32,
    )
    slot_r = jnp.where(chosen_r, before_r, jnp.float32(-1.0))
    cap_i = lax.broadcasted_iota(jnp.int32, (cap, rows), 0).astype(F32)
    for e in range(E):
        picks[e, :, :] = (slot_r[e : e + 1, :] == cap_i).astype(F32).astype(BF16)

    for k in range(3, Z):
        z_step(k, 0)
        x_step(k - 1)
        z_step(k, 1)
        finish_row(k - 2)
        y_step(k - 1)
    finish_row(Z - 2)
    x_step(Z - 1)
    y_step(Z - 1)

    total = jnp.zeros((rows, 1), F32)
    with jax.named_scope("a2await"):
        for k in range(1, T):
            source = lax.rem(t + k, T)
            remote(
                conv_out.at[source],
                conv_in.at[source],
                a2a_send.at[source],
                a2a_recv.at[source],
                s,
                source,
            ).wait_recv()
    with jax.named_scope("act"):
        for j in range(T):
            total = total + jnp.sum(conv_in[j].astype(F32), axis=1, keepdims=True)
        average = total / (T * width)
        total = jnp.zeros((rows, 1), F32)
        for j in range(T):
            centered = conv_in[j].astype(F32) - average
            total = total + jnp.sum(centered * centered, axis=1, keepdims=True)
        scale = lax.rsqrt(total / (T * width) + epsilon)
        for j in range(T):
            cols = slice(j * width, (j + 1) * width)
            v = (conv_in[j].astype(F32) - average) * scale * gain_conv_ref[
                :, cols
            ] + bias_conv_ref[:, cols]
            act[:, cols] = (v / (1.0 + jnp.exp(-v))).astype(BF16)

    finish_row(Z - 1)
    loads[2].wait()
    with jax.named_scope("wpwait"):
        for o in range(Z):
            for j in range(S):
                p_wait(o, j)

    others = [nbr_x, nbr_y, diag] if square else [lax.rem(s + S - k, S) for k in range(1, S)]
    prompt = others[:2] if square else others
    late = others[2:] if square else []

    def disp_copy(expert, j):
        return remote(
            outgoing.at[expert, j],
            arrived.at[s, j],
            disp_send.at[expert, j],
            disp_recv.at[s, j],
            expert,
            t,
        )

    def disp_wait(sender, j):
        remote(
            outgoing.at[sender, j],
            arrived.at[sender, j],
            disp_send.at[sender, j],
            disp_recv.at[sender, j],
            sender,
            t,
        ).wait_recv()

    def ret_copy(sender, j):
        return remote(
            results.at[sender, j],
            returned.at[s, j],
            ret_send.at[sender, j],
            ret_recv.at[s, j],
            sender,
            t,
        )

    def ret_wait(expert, j):
        remote(
            results.at[expert, j],
            returned.at[expert, j],
            ret_send.at[expert, j],
            ret_recv.at[expert, j],
            expert,
            t,
        ).wait_recv()

    def piece_cols(j):
        return pl.ds(pl.multiple_of(j * piece, piece), piece)

    def project(j, squares):
        cols = piece_cols(j)
        acc = residual[:, cols].astype(F32)
        part = jnp.dot(act[...], wfull[j], preferred_element_type=F32)
        state = (acc + part).astype(BF16)
        hidden[:, cols] = state
        for expert in others:
            outgoing[expert, j, :, :] = jnp.dot(
                picks[expert], state, preferred_element_type=F32
            ).astype(BF16)
        for expert in prompt:
            disp_copy(expert, j).start()
        arrived[s, j, :, :] = jnp.dot(picks[s], state, preferred_element_type=F32).astype(BF16)
        state = state.astype(F32)
        return squares + jnp.sum(state * state, axis=1, keepdims=True)

    with jax.named_scope("project"):
        squares = lax.fori_loop(0, S, project, jnp.zeros((rows, 1), F32))
        for expert in late:
            for j in range(S):
                disp_copy(expert, j).start()

    for c in loads[3:]:
        c.wait()
    ff = gate_w.shape[2]
    ff_step = min(ff, 256)

    def expert_block(sender, target, send):
        def square_step(j, squares):
            x = arrived[sender, j].astype(F32)
            return squares + jnp.sum(x * x, axis=1, keepdims=True)

        total = lax.fori_loop(0, S, square_step, jnp.zeros((cap, 1), F32))
        row_scale = lax.rsqrt(total / D + epsilon)

        def norm_step(j, _):
            cols = piece_cols(j)
            x = arrived[sender, j].astype(F32)
            normed_in[:, cols] = (x * row_scale * gain_moe_ref[:, cols]).astype(BF16)
            return 0

        lax.fori_loop(0, S, norm_step, 0)

        def up_step(j, _):
            cols = pl.ds(pl.multiple_of(j * ff_step, ff_step), ff_step)
            x = normed_in[...]
            g = jnp.dot(x, gate_w[0, :, cols], preferred_element_type=F32)
            u = jnp.dot(x, up_w[0, :, cols], preferred_element_type=F32)
            ffn_hidden[:, cols] = (g / (1.0 + jnp.exp(-g)) * u).astype(BF16)
            return 0

        lax.fori_loop(0, ff // ff_step, up_step, 0)

        def down_step(j, _):
            target[j, :, :] = jnp.dot(
                ffn_hidden[...], down_w[0, :, piece_cols(j)], preferred_element_type=F32
            ).astype(BF16)
            if send:
                ret_copy(sender, j).start()
            return 0

        lax.fori_loop(0, S, down_step, 0)

    with jax.named_scope("ffnown"):
        expert_block(s, returned.at[s], False)

    scale = lax.rsqrt(squares / D + epsilon)

    def norm_cols(j, _):
        cols = piece_cols(j)
        normed[:, cols] = (hidden[:, cols].astype(F32) * scale * gain_moe_ref[:, cols]).astype(BF16)
        return 0

    def logits(router):
        return lax.dot_general(
            normed[...], router[...], (((1,), (1,)), ((), ())), preferred_element_type=F32
        )

    def column(array, expert):
        mine = lane[:, : array.shape[1]] == expert
        return jnp.sum(jnp.where(mine, array, jnp.float32(0.0)), axis=1, keepdims=True)

    zero = jnp.float32(0.0)
    with jax.named_scope("router"):
        lax.fori_loop(0, S, norm_cols, 0)
        group_exp = jnp.exp(logits(group_router_ref))
        expert_exp = jnp.exp(logits(expert_router_ref))
        group_prob = jnp.sum(
            jnp.where(in_group[:, :G], group_exp, zero), axis=1, keepdims=True
        ) / jnp.sum(group_exp, axis=1, keepdims=True)
        chosen_exp = jnp.where(chosen[:, :E], expert_exp, zero)
        mix = group_prob * chosen_exp / jnp.sum(chosen_exp, axis=1, keepdims=True)
        slot_iota = lax.broadcasted_iota(jnp.int32, (rows, cap), 1).astype(F32)
        for e in range(E):
            spreads[e, :, :] = jnp.where(
                column(slot, e) == slot_iota, column(mix, e), zero
            ).astype(BF16)

    for i, sender in enumerate(others):
        with jax.named_scope(f"dispwait{i}"):
            for j in range(S):
                disp_wait(sender, j)
        with jax.named_scope(f"ffn{i}"):
            expert_block(sender, results.at[sender], True)

    def combine(j, _):
        cols = piece_cols(j)
        for expert in others:
            ret_wait(expert, j)
        acc = hidden[:, cols].astype(F32)
        for e in range(E):
            acc = acc + jnp.dot(spreads[e], returned[e, j], preferred_element_type=F32)
        hidden[:, cols] = acc.astype(BF16)
        pltpu.make_async_copy(hidden.at[:, cols], out_ref.at[:, cols], out_sem.at[j]).start()
        return 0

    with jax.named_scope("combine"):
        lax.fori_loop(0, S, combine, 0)

    with jax.named_scope("sendwait"):
        for h in range(H):

            @pl.when(has_up)
            def _():
                z_copy(z, h, 0, z + 1).wait_send()

            @pl.when(has_down)
            def _():
                z_copy(z, h, 1, z - 1).wait_send()

        for j in range(S):
            p_copy(z, j).wait_send()
        def sent(o, side):
            beyond = has_down if side else has_up
            for h in range(H):

                @pl.when(beyond)
                def _():
                    z_copy(o, h, side, z - 1 if side else z + 1).wait_send()

                for j in range(3 if square else S - 1):
                    x_copy(o, s, h, j, lax.rem(s + 1, S)).wait_send()
            for j in range(S):
                p_copy(o, j).wait_send()

        for k in range(1, Z):
            each_slice(k, sent)
        for k in range(1, T):
            conv_copy(lax.rem(t + k, T)).wait_send()
        for expert in others:
            for j in range(S):
                disp_copy(expert, j).wait_send()
                ret_copy(expert, j).wait_send()
        for j in range(S):
            cols = piece_cols(j)
            pltpu.make_async_copy(hidden.at[:, cols], out_ref.at[:, cols], out_sem.at[j]).wait()


def body(
    S,
    T,
    conv_value,
    conv_gate,
    doc_ids,
    conv_kernel,
    norm_gain_conv,
    norm_bias_conv,
    proj_weight,
    residual,
    norm_gain_moe,
    group_router,
    expert_router,
    routing,
    expert_gate_w,
    expert_up_w,
    expert_down_w,
):
    tokens, width = conv_value.shape
    rows, D = residual.shape
    wrows = proj_weight.shape[0]
    ff = expert_gate_w.shape[2]
    G = group_router.shape[1]
    E = expert_router.shape[1]
    cap = 2 * rows // E
    vmem = pl.BlockSpec(memory_space=pltpu.VMEM)
    hbm = pl.BlockSpec(memory_space=pl.ANY)
    smem = pl.BlockSpec(memory_space=pltpu.SMEM)
    dma = pltpu.SemaphoreType.DMA
    piece = D // S
    Z = T // 2
    return pl.pallas_call(
        functools.partial(kernel, S, T, G),
        out_shape=jax.ShapeDtypeStruct((rows, D), BF16),
        in_specs=[
            hbm, hbm, vmem, smem, vmem, vmem, vmem, hbm, hbm, vmem, vmem, vmem, vmem,
            hbm, hbm, hbm,
        ],
        out_specs=hbm,
        scratch_shapes=[
            pltpu.VMEM((tokens, width), BF16),
            pltpu.VMEM((tokens, width), BF16),
            pltpu.VMEM((S, T * wrows, piece), BF16),
            pltpu.VMEM((rows, D), BF16),
            pltpu.VMEM((1, D, ff), BF16),
            pltpu.VMEM((1, D, ff), BF16),
            pltpu.VMEM((1, ff, D), BF16),
            pltpu.VMEM((HALO + 16, width), BF16),
            pltpu.VMEM((HALO + 16, width), BF16),
            pltpu.VMEM((tokens + HALO, width), F32),
            pltpu.VMEM((32, width), F32),
            pltpu.VMEM((tokens, 128), F32),
            pltpu.VMEM((T, rows, width), BF16),
            pltpu.VMEM((T, rows, width), BF16),
            pltpu.VMEM((rows, T * width), BF16),
            pltpu.VMEM((rows, D), BF16),
            pltpu.VMEM((rows, D), BF16),
            pltpu.VMEM((cap, D), BF16),
            pltpu.VMEM((E, cap, rows), BF16),
            pltpu.VMEM((E, rows, cap), BF16),
            pltpu.VMEM((E, S, cap, piece), BF16),
            pltpu.VMEM((E, S, cap, piece), BF16),
            pltpu.VMEM((cap, ff), BF16),
            pltpu.VMEM((E, S, cap, piece), BF16),
            pltpu.VMEM((E, S, cap, piece), BF16),
            dma((6,)),
            dma((S,)),
            dma((2,)),
            dma((2, Z, 2)),
            dma((Z, 2)),
            dma((max(S - 1, 3), Z, 2)),
            dma((S, Z, 2)),
            dma((Z, S)),
            dma((Z, S)),
            dma((T,)),
            dma((T,)),
            dma((S, S)),
            dma((S, S)),
            dma((S, S)),
            dma((S, S)),
            dma((S,)),
        ],
        compiler_params=pltpu.CompilerParams(
            collective_id=0, has_side_effects=True, vmem_limit_bytes=60 * 1024 * 1024
        ),
    )(
        conv_value,
        conv_gate,
        doc_ids[None, :],
        doc_ids,
        conv_kernel,
        norm_gain_conv[None, :],
        norm_bias_conv[None, :],
        proj_weight,
        residual,
        norm_gain_moe[None, :],
        group_router.T,
        expert_router.T,
        routing.T,
        expert_gate_w,
        expert_up_w,
        expert_down_w,
    )


def solution(mesh):
    placed = (
        P("sp", "tp"),
        P("sp", "tp"),
        P("sp"),
        P(None, "tp"),
        P(),
        P(),
        P("tp", None),
        P(("sp", "tp"), None),
        P(),
        P(),
        P(),
        P(("sp", "tp"), None),
        P("sp", None, None),
        P("sp", None, None),
        P("sp", None, None),
    )
    return jax.shard_map(
        functools.partial(body, mesh.shape["sp"], mesh.shape["tp"]),
        mesh=mesh,
        in_specs=placed,
        out_specs=P(("sp", "tp"), None),
        check_vma=False,
    )
```

```python
import functools

import jax
import jax.numpy as jnp
from jax import lax
from jax.experimental import pallas as pl
from jax.experimental.pallas import tpu as pltpu
from jax.sharding import PartitionSpec as P

epsilon = 1e-06
MESH = pl.DeviceIdType.MESH
F32 = jnp.float32
BF16 = jnp.bfloat16
HALO = 32


def gate(value, gate_value):
    return (value.astype(F32) * jax.nn.sigmoid(gate_value.astype(F32))).astype(BF16)


def kernel(
    S,
    T,
    G,
    value_hbm,
    gate_hbm,
    ids_hbm,
    kernel_hbm,
    gain_conv_hbm,
    bias_conv_hbm,
    weight_hbm,
    residual_hbm,
    gain_moe_hbm,
    group_router_hbm,
    expert_router_hbm,
    routing_hbm,
    gate_w_hbm,
    up_w_hbm,
    down_w_hbm,
    out_ref,
    ids_row_ref,
    kernel_ref,
    gain_conv_ref,
    bias_conv_ref,
    gain_moe_ref,
    group_router_ref,
    expert_router_ref,
    routing_ref,
    value,
    gates,
    wfull,
    residual,
    gate_w,
    up_w,
    down_w,
    rim_out,
    rim_in,
    padded,
    taps,
    least_tap,
    conv_out,
    conv_in,
    act,
    hidden,
    normed,
    normed_in,
    picks,
    spreads,
    outgoing,
    arrived,
    ffn_hidden,
    results,
    returned,
    local_sem,
    wl_sem,
    rim_sem,
    wz_send,
    wz_recv,
    wx_send,
    wx_recv,
    wp_send,
    wp_recv,
    a2a_send,
    a2a_recv,
    disp_send,
    disp_recv,
    ret_send,
    ret_recv,
):
    s = lax.axis_index("sp")
    t = lax.axis_index("tp")
    Z = T // 2
    z = t // 2
    core = t % 2
    partner = 2 * z + 1 - core
    tokens, width = value.shape
    block = tokens // T
    n_taps = kernel_ref.shape[0]
    piece = wfull.shape[2]
    wrows = wfull.shape[1] // T
    D = S * piece
    square = S == 4
    H = 2
    part_rows = wrows // H

    def remote(src, dst, send, recv, sp_to, tp_to):
        return pltpu.make_async_remote_copy(
            src_ref=src,
            dst_ref=dst,
            send_sem=send,
            recv_sem=recv,
            device_id=(sp_to, tp_to),
            device_id_type=MESH,
        )

    barrier = pltpu.get_barrier_semaphore()
    for k in range(1, T):
        pl.semaphore_signal(
            barrier, inc=1, device_id=(s, lax.rem(t + k, T)), device_id_type=MESH
        )
    for k in range(1, S):
        pl.semaphore_signal(
            barrier, inc=1, device_id=(lax.rem(s + k, S), t), device_id_type=MESH
        )

    loads = [
        pltpu.make_async_copy(a, b, local_sem.at[i])
        for i, (a, b) in enumerate(
            [
                (ids_hbm, ids_row_ref),
                (value_hbm, value),
                (gate_hbm, gates),
                (kernel_hbm, kernel_ref),
                (routing_hbm, routing_ref),
                (gain_conv_hbm, gain_conv_ref),
                (bias_conv_hbm, bias_conv_ref),
                (residual_hbm, residual),
                (gain_moe_hbm, gain_moe_ref),
                (group_router_hbm, group_router_ref),
                (expert_router_hbm, expert_router_ref),
                (gate_w_hbm, gate_w),
                (up_w_hbm, up_w),
                (down_w_hbm, down_w),
            ]
        )
    ]
    own_rows = pl.ds(pl.multiple_of(t * wrows, wrows), wrows)
    own_w = [
        pltpu.make_async_copy(
            weight_hbm.at[:, pl.ds(j * piece, piece)], wfull.at[j, own_rows, :], wl_sem.at[j]
        )
        for j in range(S)
    ]
    loads[0].start()
    for c in own_w:
        c.start()
    for c in loads[1:]:
        c.start()

    loads[0].wait()
    ids_row = jnp.broadcast_to(ids_row_ref[...], (8, tokens))
    position = lax.broadcasted_iota(jnp.int32, (8, tokens), 1)
    low = jnp.int32(-n_taps)
    fresh = (ids_row != pltpu.roll(ids_row, 1, 1)) & (position > 0)
    begin = jnp.where(fresh, position, low)
    shift = 1
    while shift < n_taps:
        moved = jnp.where(position >= shift, pltpu.roll(begin, shift, 1), low)
        begin = jnp.maximum(begin, moved)
        shift *= 2
    least_row = (n_taps - 1 - position + begin).astype(F32)
    lanes = least_tap.shape[1]
    for c in range(tokens // lanes):
        across = jnp.broadcast_to(least_row[0:1, c * lanes : (c + 1) * lanes], (lanes, lanes))
        least_tap[c * lanes : (c + 1) * lanes, :] = across.T

    with jax.named_scope("barrier"):
        pl.semaphore_wait(barrier, T + S - 2)

    def w_ref(o, p, h):
        base = pl.multiple_of((2 * o + core) * wrows + h * part_rows, part_rows)
        return wfull.at[p, pl.ds(base, part_rows), :]

    def z_copy(o, h, up, to):
        ref = w_ref(o, s, h)
        return remote(ref, ref, wz_send.at[up, o, h], wz_recv.at[o, h], s, 2 * to + core)

    def x_copy(o, p, h, lane_at, to):
        ref = w_ref(o, p, h)
        return remote(ref, ref, wx_send.at[lane_at, o, h], wx_recv.at[p, o, h], to, t)

    def p_copy(o, p):
        rows_at = pl.ds(pl.multiple_of((2 * o + core) * wrows, wrows), wrows)
        ref = wfull.at[p, rows_at, :]
        return remote(ref, ref, wp_send.at[o, p], wp_recv.at[o, p], s, partner)

    def p_wait(o, p):
        rows_at = pl.ds(pl.multiple_of((2 * o + 1 - core) * wrows, wrows), wrows)
        ref = wfull.at[p, rows_at, :]
        remote(ref, ref, wp_send.at[o, p], wp_recv.at[o, p], s, partner).wait_recv()

    has_up = z + 1 < Z
    has_down = z > 0
    for j in range(S):
        own_w[j].wait()
    for h in range(H):

        @pl.when(has_up)
        def _():
            z_copy(z, h, 0, z + 1).start()

        @pl.when(has_down)
        def _():
            z_copy(z, h, 1, z - 1).start()

    for j in range(S):
        p_copy(z, j).start()

    def sides(k):
        return ((z - k, z - k >= 0, 0), (z + k, z + k < Z, 1))

    def each_slice(k, act_on):
        for o, there, side in sides(k):
            pl.when(there)(functools.partial(act_on, o, side))

    nbr_x = s + 1 - 2 * (s % 2)
    nbr_y = s + 2 - 4 * (s // 2)
    diag = 3 - s
    order = [s, nbr_x, nbr_y, diag] if square else [lax.rem(s + S - j, S) for j in range(S)]

    def z_step(k, h):
        def one(o, side):
            z_copy(o, h, side, z).wait_recv()
            beyond = has_down if side else has_up

            @pl.when(beyond)
            def _():
                z_copy(o, h, side, z - 1 if side else z + 1).start()

            if square:
                x_copy(o, s, h, 0, nbr_x).start()
                x_copy(o, s, h, 1, nbr_y).start()
            else:
                for j in range(1, S):
                    x_copy(o, s, h, j - 1, lax.rem(s + j, S)).start()

        with jax.named_scope(f"z{k}{h}"):
            each_slice(k, one)

    def x_step(k):
        def one(o, side):
            x_copy(o, nbr_x, 0, 2, nbr_y).wait_recv()
            x_copy(o, nbr_x, 0, 2, nbr_y).start()

        if square:
            with jax.named_scope(f"x{k}"):
                each_slice(k, one)

    def y_step(k):
        def one(o, side):
            x_copy(o, nbr_y, 1, 2, nbr_x).wait_recv()
            x_copy(o, nbr_y, 1, 2, nbr_x).start()

        if square:
            with jax.named_scope(f"y{k}"):
                each_slice(k, one)

    def finish_row(k, parts):
        def one(o, side):
            for i in parts:
                p = order[i]
                if i > 0 and square:
                    for h in ((1,), (0,), (0, 1))[i - 1]:
                        x_copy(o, p, h, 0, p).wait_recv()
                elif i > 0:
                    for h in range(H):
                        x_copy(o, p, h, i - 1, p).wait_recv()
                p_copy(o, p).start()

        with jax.named_scope(f"fin{k}{parts[0]}"):
            each_slice(k, one)

    for c in loads[1:4]:
        c.wait()
    tail = pl.ds(tokens - HALO, HALO)
    last_reach = jnp.max(least_tap[tokens - 1 : tokens, :], axis=1, keepdims=True)
    row_at = lax.broadcasted_iota(jnp.int32, (HALO, width), 0).astype(F32)
    newer = row_at >= last_reach + (HALO - n_taps)
    rim = jnp.where(newer, gate(value[tail, :], gates[tail, :]).astype(F32), jnp.float32(0.0))
    rim_out[0:HALO, :] = rim.astype(BF16)
    last_id = ids_row_ref[0:1, tokens - 1 : tokens].astype(F32)
    rim_out[HALO : HALO + 16, :] = jnp.broadcast_to(last_id, (16, width)).astype(BF16)
    rim_copy = remote(
        rim_out, rim_in, rim_sem.at[0], rim_sem.at[1], lax.rem(s + 1, S), t
    )
    rim_copy.start()

    def gate_rows(i, _):
        rows = pl.ds(pl.multiple_of(i * 64, 64), 64)
        to_rows = pl.ds(pl.multiple_of(HALO + i * 64, 32), 64)
        padded[to_rows, :] = gate(value[rows, :], gates[rows, :]).astype(F32)
        return 0

    with jax.named_scope("gate"):
        lax.fori_loop(0, tokens // 64, gate_rows, 0)
    taps[0:n_taps, :] = kernel_ref[...].astype(F32)

    step_rows = 32 if block % 32 == 0 else 8
    lanes = min(width, 128)

    def conv_block(owner):
        def conv_rows(i, _):
            base = pl.multiple_of(owner * block + i * step_rows, 8)
            least = least_tap[pl.ds(base, step_rows), :]
            window = padded[pl.ds(base, step_rows + HALO), :]
            total = jnp.zeros((step_rows, width), F32)
            for tap in range(n_taps):
                at = tap + HALO + 1 - n_taps
                valid = least <= tap
                product = window[at : at + step_rows, :] * taps[tap : tap + 1, :]
                parts = [
                    jnp.where(valid, product[:, j : j + lanes], jnp.float32(0.0))
                    for j in range(0, width, lanes)
                ]
                total = total + jnp.concatenate(parts, axis=1)
            conv_out[
                owner, pl.ds(pl.multiple_of(i * step_rows, step_rows), step_rows), :
            ] = total.astype(BF16)
            return 0

        lax.fori_loop(0, block // step_rows, conv_rows, 0)

    def conv_some(first, last):
        with jax.named_scope("conv"):

            def one(owner, _):
                conv_block(owner)
                return 0

            lax.fori_loop(first, last, one, 0)

    def conv_copy(to):
        return remote(
            conv_out.at[to], conv_in.at[t], a2a_send.at[to], a2a_recv.at[t], s, to
        )

    def conv_flush(inner):
        if not inner:
            conv_copy(partner).start()
        for far in range(1, Z):
            for to, there, _ in sides(far):
                middle = (to > 0) & (to < Z - 1)

                @pl.when(there & (middle if inner else jnp.logical_not(middle)))
                def _():
                    for c in range(2):
                        conv_copy(2 * to + c).start()

    marks = [1 + (T - 1) * i // 7 for i in (3, 5, 7)]
    conv_some(1, marks[0])
    z_step(1, 0)
    conv_some(marks[0], marks[1])
    z_step(1, 1)
    conv_some(marks[1], marks[2])
    z_step(2, 0)
    conv_flush(True)
    with jax.named_scope("rimwait"):
        rim_copy.wait()
    same = (rim_in[HALO : HALO + 1, :].astype(F32) == ids_row_ref[0:1, 0:1].astype(F32)) & (s > 0)
    padded[0:HALO, :] = jnp.where(same, rim_in[0:HALO, :].astype(F32), jnp.float32(0.0))
    conv_some(0, 1)
    x_step(1)
    z_step(2, 1)
    conv_flush(False)
    y_step(1)
    conv_in[t, :, :] = conv_out[t, :, :]

    rows = block
    E = S
    for c in loads[4:7]:
        c.wait()
    cap = 2 * rows // E
    lane = lax.broadcasted_iota(jnp.int32, (rows, 128), 1)
    eye = lax.broadcasted_iota(jnp.int32, (rows, rows), 0) == lax.broadcasted_iota(
        jnp.int32, (rows, rows), 1
    )
    named = lax.dot_general(
        eye.astype(F32).astype(BF16),
        routing_ref[...].astype(F32).astype(BF16),
        (((1,), (1,)), ((), ())),
        preferred_element_type=F32,
    )
    first = named[:, 0:1]
    second = named[:, 1:2]
    lane_f = lane.astype(F32)
    chosen = (lane_f == first) | (lane_f == second)
    per_group = E // G
    group_low = lane_f * per_group
    in_group = (first >= group_low) & (first < group_low + per_group)
    row_i = lax.broadcasted_iota(jnp.int32, (rows, rows), 0)
    col_i = lax.broadcasted_iota(jnp.int32, (rows, rows), 1)
    before = jnp.dot(
        (row_i > col_i).astype(F32).astype(BF16),
        chosen.astype(F32).astype(BF16),
        preferred_element_type=F32,
    )
    slot = jnp.where(chosen, before, jnp.float32(-1.0))
    width_e = max(E, 8)
    expert_i = lax.broadcasted_iota(jnp.int32, (width_e, rows), 0)
    chosen_r = (routing_ref[0:1, :] == expert_i) | (routing_ref[1:2, :] == expert_i)
    before_r = jnp.dot(
        chosen_r.astype(F32).astype(BF16),
        (row_i < col_i).astype(F32).astype(BF16),
        preferred_element_type=F32,
    )
    slot_r = jnp.where(chosen_r, before_r, jnp.float32(-1.0))
    cap_i = lax.broadcasted_iota(jnp.int32, (cap, rows), 0).astype(F32)
    for e in range(E):
        picks[e, :, :] = (slot_r[e : e + 1, :] == cap_i).astype(F32).astype(BF16)

    all_parts = tuple(range(S))
    for k in range(3, Z):
        z_step(k, 0)
        x_step(k - 1)
        z_step(k, 1)
        finish_row(k - 2, all_parts)
        y_step(k - 1)
    finish_row(Z - 1, all_parts[:1])
    finish_row(Z - 2, all_parts[:-1])
    x_step(Z - 1)
    y_step(Z - 1)
    finish_row(Z - 1, all_parts[1:-1])

    with jax.named_scope("a2await"):
        total = jnp.sum(conv_in[t].astype(F32), axis=1, keepdims=True)
        for k in range(1, T):
            source = lax.rem(t + k, T)
            remote(
                conv_out.at[source],
                conv_in.at[source],
                a2a_send.at[source],
                a2a_recv.at[source],
                s,
                source,
            ).wait_recv()
            total = total + jnp.sum(conv_in[source].astype(F32), axis=1, keepdims=True)
    with jax.named_scope("act"):
        average = total / (T * width)
        total = jnp.zeros((rows, 1), F32)
        for j in range(T):
            centered = conv_in[j].astype(F32) - average
            total = total + jnp.sum(centered * centered, axis=1, keepdims=True)
        scale = lax.rsqrt(total / (T * width) + epsilon)
        for j in range(T):
            cols = slice(j * width, (j + 1) * width)
            v = (conv_in[j].astype(F32) - average) * scale * gain_conv_ref[
                :, cols
            ] + bias_conv_ref[:, cols]
            act[:, cols] = (v / (1.0 + jnp.exp(-v))).astype(BF16)

    loads[7].wait()

    others = order[1:]
    prompt = others[:2] if square else others
    late = others[2:] if square else []

    def disp_copy(expert, j):
        return remote(
            outgoing.at[expert, j],
            arrived.at[s, j],
            disp_send.at[expert, j],
            disp_recv.at[s, j],
            expert,
            t,
        )

    def disp_wait(sender, j):
        remote(
            outgoing.at[sender, j],
            arrived.at[sender, j],
            disp_send.at[sender, j],
            disp_recv.at[sender, j],
            sender,
            t,
        ).wait_recv()

    def ret_copy(sender, j):
        return remote(
            results.at[sender, j],
            returned.at[s, j],
            ret_send.at[sender, j],
            ret_recv.at[s, j],
            sender,
            t,
        )

    def ret_wait(expert, j):
        remote(
            results.at[expert, j],
            returned.at[expert, j],
            ret_send.at[expert, j],
            ret_recv.at[expert, j],
            expert,
            t,
        ).wait_recv()

    def piece_cols(j):
        return pl.ds(pl.multiple_of(j * piece, piece), piece)

    def project(j, squares):
        with jax.named_scope("wpwait"):
            for o in range(Z):
                p_wait(o, j)
        cols = piece_cols(j)
        acc = residual[:, cols].astype(F32)
        part = jnp.dot(act[...], wfull[j], preferred_element_type=F32)
        state = (acc + part).astype(BF16)
        hidden[:, cols] = state
        for expert in others:
            outgoing[expert, j, :, :] = jnp.dot(
                picks[expert], state, preferred_element_type=F32
            ).astype(BF16)
        for expert in prompt:
            disp_copy(expert, j).start()
        arrived[s, j, :, :] = jnp.dot(picks[s], state, preferred_element_type=F32).astype(BF16)
        state = state.astype(F32)
        return squares + jnp.sum(state * state, axis=1, keepdims=True)

    def finish_last():
        for k in (Z - 2, Z - 1):
            finish_row(k, all_parts[-1:])

    squares = jnp.zeros((rows, 1), F32)
    if square:
        for i, j in enumerate(order):
            with jax.named_scope(f"project{i}"):
                squares = project(j, squares)
            if i == 0:
                finish_last()
    else:
        finish_last()
        squares = lax.fori_loop(0, S, project, squares)
    for expert in late:
        for j in order:
            disp_copy(expert, j).start()

    for c in loads[8:]:
        c.wait()
    ff = gate_w.shape[2]
    ff_step = min(ff, 256)

    def expert_block(sender, target, send):
        def square_step(j, squares):
            x = arrived[sender, j].astype(F32)
            return squares + jnp.sum(x * x, axis=1, keepdims=True)

        total = lax.fori_loop(0, S, square_step, jnp.zeros((cap, 1), F32))
        row_scale = lax.rsqrt(total / D + epsilon)

        def norm_step(j, _):
            cols = piece_cols(j)
            x = arrived[sender, j].astype(F32)
            normed_in[:, cols] = (x * row_scale * gain_moe_ref[:, cols]).astype(BF16)
            return 0

        lax.fori_loop(0, S, norm_step, 0)

        def up_step(j, _):
            cols = pl.ds(pl.multiple_of(j * ff_step, ff_step), ff_step)
            x = normed_in[...]
            g = jnp.dot(x, gate_w[0, :, cols], preferred_element_type=F32)
            u = jnp.dot(x, up_w[0, :, cols], preferred_element_type=F32)
            ffn_hidden[:, cols] = (g / (1.0 + jnp.exp(-g)) * u).astype(BF16)
            return 0

        lax.fori_loop(0, ff // ff_step, up_step, 0)

        def down_step(j, _):
            target[j, :, :] = jnp.dot(
                ffn_hidden[...], down_w[0, :, piece_cols(j)], preferred_element_type=F32
            ).astype(BF16)
            if send:
                ret_copy(sender, j).start()
            return 0

        lax.fori_loop(0, S, down_step, 0)

    with jax.named_scope("ffnown"):
        expert_block(s, returned.at[s], False)

    scale = lax.rsqrt(squares / D + epsilon)

    def norm_cols(j, _):
        cols = piece_cols(j)
        normed[:, cols] = (hidden[:, cols].astype(F32) * scale * gain_moe_ref[:, cols]).astype(BF16)
        return 0

    def logits(router):
        return lax.dot_general(
            normed[...], router[...], (((1,), (1,)), ((), ())), preferred_element_type=F32
        )

    def column(array, expert):
        mine = lane[:, : array.shape[1]] == expert
        return jnp.sum(jnp.where(mine, array, jnp.float32(0.0)), axis=1, keepdims=True)

    zero = jnp.float32(0.0)
    with jax.named_scope("router"):
        lax.fori_loop(0, S, norm_cols, 0)
        group_exp = jnp.exp(logits(group_router_ref))
        expert_exp = jnp.exp(logits(expert_router_ref))
        group_prob = jnp.sum(
            jnp.where(in_group[:, :G], group_exp, zero), axis=1, keepdims=True
        ) / jnp.sum(group_exp, axis=1, keepdims=True)
        chosen_exp = jnp.where(chosen[:, :E], expert_exp, zero)
        mix = group_prob * chosen_exp / jnp.sum(chosen_exp, axis=1, keepdims=True)
        slot_iota = lax.broadcasted_iota(jnp.int32, (rows, cap), 1).astype(F32)
        for e in range(E):
            spreads[e, :, :] = jnp.where(
                column(slot, e) == slot_iota, column(mix, e), zero
            ).astype(BF16)

    for i, sender in enumerate(others):
        with jax.named_scope(f"dispwait{i}"):
            for j in range(S):
                disp_wait(sender, j)
        with jax.named_scope(f"ffn{i}"):
            expert_block(sender, results.at[sender], True)

    def combine(j, _):
        cols = piece_cols(j)
        for expert in others:
            ret_wait(expert, j)
        acc = hidden[:, cols].astype(F32)
        for e in range(E):
            acc = acc + jnp.dot(spreads[e], returned[e, j], preferred_element_type=F32)
        out_ref[:, cols] = acc.astype(BF16)
        return 0

    with jax.named_scope("combine"):
        lax.fori_loop(0, S, combine, 0)

    with jax.named_scope("sendwait"):
        for h in range(H):

            @pl.when(has_up)
            def _():
                z_copy(z, h, 0, z + 1).wait_send()

            @pl.when(has_down)
            def _():
                z_copy(z, h, 1, z - 1).wait_send()

        for j in range(S):
            p_copy(z, j).wait_send()
        def sent(o, side):
            beyond = has_down if side else has_up
            for h in range(H):

                @pl.when(beyond)
                def _():
                    z_copy(o, h, side, z - 1 if side else z + 1).wait_send()

                for j in range(3 if square else S - 1):
                    x_copy(o, s, h, j, lax.rem(s + 1, S)).wait_send()
            for j in range(S):
                p_copy(o, j).wait_send()

        for k in range(1, Z):
            each_slice(k, sent)
        for k in range(1, T):
            conv_copy(lax.rem(t + k, T)).wait_send()
        for expert in others:
            for j in range(S):
                disp_copy(expert, j).wait_send()
                ret_copy(expert, j).wait_send()


def body(
    S,
    T,
    conv_value,
    conv_gate,
    doc_ids,
    conv_kernel,
    norm_gain_conv,
    norm_bias_conv,
    proj_weight,
    residual,
    norm_gain_moe,
    group_router,
    expert_router,
    routing,
    expert_gate_w,
    expert_up_w,
    expert_down_w,
):
    tokens, width = conv_value.shape
    rows, D = residual.shape
    wrows = proj_weight.shape[0]
    ff = expert_gate_w.shape[2]
    G = group_router.shape[1]
    E = expert_router.shape[1]
    cap = 2 * rows // E
    hbm = pl.BlockSpec(memory_space=pl.ANY)
    dma = pltpu.SemaphoreType.DMA
    piece = D // S
    Z = T // 2
    return pl.pallas_call(
        functools.partial(kernel, S, T, G),
        out_shape=pltpu.VMEM((rows, D), BF16),
        in_specs=[hbm] * 15,
        out_specs=pl.BlockSpec(memory_space=pltpu.VMEM),
        scratch_shapes=[
            pltpu.VMEM((1, tokens), jnp.int32),
            pltpu.VMEM(conv_kernel.shape, BF16),
            pltpu.VMEM((1, T * width), F32),
            pltpu.VMEM((1, T * width), F32),
            pltpu.VMEM((1, D), F32),
            pltpu.VMEM((G, D), BF16),
            pltpu.VMEM((E, D), BF16),
            pltpu.VMEM((2, rows), jnp.int32),
            pltpu.VMEM((tokens, width), BF16),
            pltpu.VMEM((tokens, width), BF16),
            pltpu.VMEM((S, T * wrows, piece), BF16),
            pltpu.VMEM((rows, D), BF16),
            pltpu.VMEM((1, D, ff), BF16),
            pltpu.VMEM((1, D, ff), BF16),
            pltpu.VMEM((1, ff, D), BF16),
            pltpu.VMEM((HALO + 16, width), BF16),
            pltpu.VMEM((HALO + 16, width), BF16),
            pltpu.VMEM((tokens + HALO, width), F32),
            pltpu.VMEM((32, width), F32),
            pltpu.VMEM((tokens, 128), F32),
            pltpu.VMEM((T, rows, width), BF16),
            pltpu.VMEM((T, rows, width), BF16),
            pltpu.VMEM((rows, T * width), BF16),
            pltpu.VMEM((rows, D), BF16),
            pltpu.VMEM((rows, D), BF16),
            pltpu.VMEM((cap, D), BF16),
            pltpu.VMEM((E, cap, rows), BF16),
            pltpu.VMEM((E, rows, cap), BF16),
            pltpu.VMEM((E, S, cap, piece), BF16),
            pltpu.VMEM((E, S, cap, piece), BF16),
            pltpu.VMEM((cap, ff), BF16),
            pltpu.VMEM((E, S, cap, piece), BF16),
            pltpu.VMEM((E, S, cap, piece), BF16),
            dma((14,)),
            dma((S,)),
            dma((2,)),
            dma((2, Z, 2)),
            dma((Z, 2)),
            dma((max(S - 1, 3), Z, 2)),
            dma((S, Z, 2)),
            dma((Z, S)),
            dma((Z, S)),
            dma((T,)),
            dma((T,)),
            dma((S, S)),
            dma((S, S)),
            dma((S, S)),
            dma((S, S)),
        ],
        compiler_params=pltpu.CompilerParams(
            collective_id=0, has_side_effects=True, vmem_limit_bytes=60 * 1024 * 1024
        ),
    )(
        conv_value,
        conv_gate,
        doc_ids[None, :],
        conv_kernel,
        norm_gain_conv[None, :],
        norm_bias_conv[None, :],
        proj_weight,
        residual,
        norm_gain_moe[None, :],
        group_router.T,
        expert_router.T,
        routing.T,
        expert_gate_w,
        expert_up_w,
        expert_down_w,
    )


def solution(mesh):
    placed = (
        P("sp", "tp"),
        P("sp", "tp"),
        P("sp"),
        P(None, "tp"),
        P(),
        P(),
        P("tp", None),
        P(("sp", "tp"), None),
        P(),
        P(),
        P(),
        P(("sp", "tp"), None),
        P("sp", None, None),
        P("sp", None, None),
        P("sp", None, None),
    )
    return jax.shard_map(
        functools.partial(body, mesh.shape["sp"], mesh.shape["tp"]),
        mesh=mesh,
        in_specs=placed,
        out_specs=P(("sp", "tp"), None),
        check_vma=False,
    )
```

```python
import functools

import jax
import jax.numpy as jnp
from jax import lax
from jax.experimental import pallas as pl
from jax.experimental.pallas import tpu as pltpu
from jax.sharding import PartitionSpec as P

epsilon = 1e-06
MESH = pl.DeviceIdType.MESH
F32 = jnp.float32
BF16 = jnp.bfloat16
HALO = 32
CHUNKS = 2


def gate(value, gate_value):
    return (value.astype(F32) * jax.nn.sigmoid(gate_value.astype(F32))).astype(BF16)


def kernel(
    S,
    T,
    G,
    value_hbm,
    gate_hbm,
    ids_hbm,
    kernel_hbm,
    gain_conv_hbm,
    bias_conv_hbm,
    weight_hbm,
    residual_hbm,
    gain_moe_hbm,
    group_router_hbm,
    expert_router_hbm,
    routing_hbm,
    gate_w_hbm,
    up_w_hbm,
    down_w_hbm,
    out_ref,
    ids_row_ref,
    kernel_ref,
    gain_conv_ref,
    bias_conv_ref,
    gain_moe_ref,
    group_router_ref,
    expert_router_ref,
    routing_ref,
    value,
    gates,
    wfull,
    residual,
    gate_w,
    up_w,
    down_w,
    rim_out,
    rim_in,
    padded,
    taps,
    least_tap,
    conv_out,
    conv_in,
    act,
    hidden,
    normed,
    normed_in,
    picks,
    spreads,
    outgoing,
    arrived,
    ffn_hidden,
    results,
    returned,
    router_all,
    down_stage,
    down_x,
    h_own,
    h_out,
    h_in,
    back_out,
    back_in,
    local_sem,
    wl_sem,
    rim_sem,
    wz_send,
    wz_recv,
    wx_send,
    wx_recv,
    wp_send,
    wp_recv,
    a2a_send,
    a2a_recv,
    disp_send,
    disp_recv,
    ret_send,
    ret_recv,
    ex_send,
    ex_recv,
    hx_send,
    hx_recv,
    rt_send,
    rt_recv,
    zd_send,
    zd_recv,
    dp_send,
    dp_recv,
    dx_sem,
):
    s = lax.axis_index("sp")
    t = lax.axis_index("tp")
    Z = T // 2
    z = t // 2
    core = t % 2
    partner = 2 * z + 1 - core
    tokens, width = value.shape
    block = tokens // T
    n_taps = kernel_ref.shape[0]
    piece = wfull.shape[2]
    wrows = wfull.shape[1] // T
    D = S * piece
    square = S == 4
    E = S
    paired = square and E == 2 * G
    wide = D // T
    H = 2
    part_rows = wrows // H

    def remote(src, dst, send, recv, sp_to, tp_to):
        return pltpu.make_async_remote_copy(
            src_ref=src,
            dst_ref=dst,
            send_sem=send,
            recv_sem=recv,
            device_id=(sp_to, tp_to),
            device_id_type=MESH,
        )

    barrier = pltpu.get_barrier_semaphore()
    for k in range(1, T):
        pl.semaphore_signal(
            barrier, inc=1, device_id=(s, lax.rem(t + k, T)), device_id_type=MESH
        )
    for k in range(1, S):
        pl.semaphore_signal(
            barrier, inc=1, device_id=(lax.rem(s + k, S), t), device_id_type=MESH
        )

    loads = [
        pltpu.make_async_copy(a, b, local_sem.at[i])
        for i, (a, b) in enumerate(
            [
                (ids_hbm, ids_row_ref),
                (value_hbm, value),
                (gate_hbm, gates),
                (kernel_hbm, kernel_ref),
                (routing_hbm, routing_ref),
                (gain_conv_hbm, gain_conv_ref),
                (bias_conv_hbm, bias_conv_ref),
                (residual_hbm, residual),
                (gain_moe_hbm, gain_moe_ref),
                (group_router_hbm, group_router_ref),
                (expert_router_hbm, expert_router_ref),
                (gate_w_hbm, gate_w),
                (up_w_hbm, up_w),
                (down_w_hbm, down_w),
            ]
        )
    ]
    own_rows = pl.ds(pl.multiple_of(t * wrows, wrows), wrows)
    own_w = [
        pltpu.make_async_copy(
            weight_hbm.at[:, pl.ds(j * piece, piece)], wfull.at[j, own_rows, :], wl_sem.at[j]
        )
        for j in range(S)
    ]
    stage = pltpu.make_async_copy(
        down_w_hbm.at[0, :, pl.ds(pl.multiple_of(t * wide, wide), wide)],
        down_stage,
        local_sem.at[14],
    )
    loads[0].start()
    for c in own_w:
        c.start()
    if paired:
        stage.start()
    for c in loads[1:]:
        c.start()

    loads[0].wait()
    ids_row = jnp.broadcast_to(ids_row_ref[...], (8, tokens))
    position = lax.broadcasted_iota(jnp.int32, (8, tokens), 1)
    low = jnp.int32(-n_taps)
    fresh = (ids_row != pltpu.roll(ids_row, 1, 1)) & (position > 0)
    begin = jnp.where(fresh, position, low)
    shift = 1
    while shift < n_taps:
        moved = jnp.where(position >= shift, pltpu.roll(begin, shift, 1), low)
        begin = jnp.maximum(begin, moved)
        shift *= 2
    least_row = (n_taps - 1 - position + begin).astype(F32)
    lanes = least_tap.shape[1]
    for c in range(tokens // lanes):
        across = jnp.broadcast_to(least_row[0:1, c * lanes : (c + 1) * lanes], (lanes, lanes))
        least_tap[c * lanes : (c + 1) * lanes, :] = across.T

    with jax.named_scope("barrier"):
        pl.semaphore_wait(barrier, T + S - 2)

    def w_ref(o, p, h):
        base = pl.multiple_of((2 * o + core) * wrows + h * part_rows, part_rows)
        return wfull.at[p, pl.ds(base, part_rows), :]

    def z_copy(o, h, up, to):
        ref = w_ref(o, s, h)
        return remote(ref, ref, wz_send.at[up, o, h], wz_recv.at[o, h], s, 2 * to + core)

    def x_copy(o, p, h, lane_at, to):
        ref = w_ref(o, p, h)
        return remote(ref, ref, wx_send.at[lane_at, o, h], wx_recv.at[p, o, h], to, t)

    def p_copy(o, p):
        rows_at = pl.ds(pl.multiple_of((2 * o + core) * wrows, wrows), wrows)
        ref = wfull.at[p, rows_at, :]
        return remote(ref, ref, wp_send.at[o, p], wp_recv.at[o, p], s, partner)

    def p_wait(o, p):
        rows_at = pl.ds(pl.multiple_of((2 * o + 1 - core) * wrows, wrows), wrows)
        ref = wfull.at[p, rows_at, :]
        remote(ref, ref, wp_send.at[o, p], wp_recv.at[o, p], s, partner).wait_recv()

    has_up = z + 1 < Z
    has_down = z > 0
    for j in range(S):
        own_w[j].wait()
    for h in range(H):

        @pl.when(has_up)
        def _():
            z_copy(z, h, 0, z + 1).start()

        @pl.when(has_down)
        def _():
            z_copy(z, h, 1, z - 1).start()

    for j in range(S):
        p_copy(z, j).start()
    dx_copy = remote(
        down_stage, down_x.at[t], dx_sem.at[0], dx_sem.at[1], s + 1 - 2 * (s % 2), t
    )
    if paired:
        stage.wait()
        dx_copy.start()

    def sides(k):
        return ((z - k, z - k >= 0, 0), (z + k, z + k < Z, 1))

    def each_slice(k, act_on):
        for o, there, side in sides(k):
            pl.when(there)(functools.partial(act_on, o, side))

    nbr_x = s + 1 - 2 * (s % 2)
    nbr_y = s + 2 - 4 * (s // 2)
    diag = 3 - s
    order = [s, nbr_x, nbr_y, diag] if square else [lax.rem(s + S - j, S) for j in range(S)]

    def z_step(k, h):
        def one(o, side):
            z_copy(o, h, side, z).wait_recv()
            beyond = has_down if side else has_up

            @pl.when(beyond)
            def _():
                z_copy(o, h, side, z - 1 if side else z + 1).start()

            if square:
                x_copy(o, s, h, 0, nbr_x).start()
                x_copy(o, s, h, 1, nbr_y).start()
            else:
                for j in range(1, S):
                    x_copy(o, s, h, j - 1, lax.rem(s + j, S)).start()

        with jax.named_scope(f"z{k}{h}"):
            each_slice(k, one)

    def x_step(k):
        def one(o, side):
            x_copy(o, nbr_x, 0, 2, nbr_y).wait_recv()
            x_copy(o, nbr_x, 0, 2, nbr_y).start()

        if square:
            with jax.named_scope(f"x{k}"):
                each_slice(k, one)

    def y_step(k):
        def one(o, side):
            x_copy(o, nbr_y, 1, 2, nbr_x).wait_recv()
            x_copy(o, nbr_y, 1, 2, nbr_x).start()

        if square:
            with jax.named_scope(f"y{k}"):
                each_slice(k, one)

    def zd_copy(o, side, to):
        ref = down_x.at[2 * o + core]
        return remote(ref, ref, zd_send.at[side, o], zd_recv.at[o], s, 2 * to + core)

    def dp_copy(o):
        ref = down_x.at[2 * o + core]
        return remote(ref, ref, dp_send.at[o], dp_recv.at[o], s, partner)

    def dp_wait(o):
        ref = down_x.at[2 * o + 1 - core]
        remote(ref, ref, dp_send.at[o], dp_recv.at[o], s, partner).wait_recv()

    def d_start():
        dx_copy.wait_recv()

        @pl.when(has_up)
        def _():
            zd_copy(z, 0, z + 1).start()

        @pl.when(has_down)
        def _():
            zd_copy(z, 1, z - 1).start()

        dp_copy(z).start()

    def d_step(k):
        def one(o, side):
            zd_copy(o, side, z).wait_recv()

            @pl.when(has_down if side else has_up)
            def _():
                zd_copy(o, side, z - 1 if side else z + 1).start()

            dp_copy(o).start()

        with jax.named_scope(f"d{k}"):
            each_slice(k, one)

    def finish_row(k, parts):
        def one(o, side):
            for i in parts:
                p = order[i]
                if i > 0 and square:
                    for h in ((1,), (0,), (0, 1))[i - 1]:
                        x_copy(o, p, h, 0, p).wait_recv()
                elif i > 0:
                    for h in range(H):
                        x_copy(o, p, h, i - 1, p).wait_recv()
                p_copy(o, p).start()

        with jax.named_scope(f"fin{k}{parts[0]}"):
            each_slice(k, one)

    for c in loads[1:4]:
        c.wait()
    tail = pl.ds(tokens - HALO, HALO)
    last_reach = jnp.max(least_tap[tokens - 1 : tokens, :], axis=1, keepdims=True)
    row_at = lax.broadcasted_iota(jnp.int32, (HALO, width), 0).astype(F32)
    newer = row_at >= last_reach + (HALO - n_taps)
    rim = jnp.where(newer, gate(value[tail, :], gates[tail, :]).astype(F32), jnp.float32(0.0))
    rim_out[0:HALO, :] = rim.astype(BF16)
    last_id = ids_row_ref[0:1, tokens - 1 : tokens].astype(F32)
    rim_out[HALO : HALO + 16, :] = jnp.broadcast_to(last_id, (16, width)).astype(BF16)
    rim_copy = remote(
        rim_out, rim_in, rim_sem.at[0], rim_sem.at[1], lax.rem(s + 1, S), t
    )
    rim_copy.start()

    def gate_rows(i, _):
        rows = pl.ds(pl.multiple_of(i * 64, 64), 64)
        to_rows = pl.ds(pl.multiple_of(HALO + i * 64, 32), 64)
        padded[to_rows, :] = gate(value[rows, :], gates[rows, :]).astype(F32)
        return 0

    with jax.named_scope("gate"):
        lax.fori_loop(0, tokens // 64, gate_rows, 0)
    taps[0:n_taps, :] = kernel_ref[...].astype(F32)

    step_rows = 32 if block % 32 == 0 else 8
    lanes = min(width, 128)

    def conv_block(owner):
        def conv_rows(i, _):
            base = pl.multiple_of(owner * block + i * step_rows, 8)
            least = least_tap[pl.ds(base, step_rows), :]
            window = padded[pl.ds(base, step_rows + HALO), :]
            total = jnp.zeros((step_rows, width), F32)
            for tap in range(n_taps):
                at = tap + HALO + 1 - n_taps
                valid = least <= tap
                product = window[at : at + step_rows, :] * taps[tap : tap + 1, :]
                parts = [
                    jnp.where(valid, product[:, j : j + lanes], jnp.float32(0.0))
                    for j in range(0, width, lanes)
                ]
                total = total + jnp.concatenate(parts, axis=1)
            conv_out[
                owner, pl.ds(pl.multiple_of(i * step_rows, step_rows), step_rows), :
            ] = total.astype(BF16)
            return 0

        lax.fori_loop(0, block // step_rows, conv_rows, 0)

    def conv_some(first, last):
        with jax.named_scope("conv"):

            def one(owner, _):
                conv_block(owner)
                return 0

            lax.fori_loop(first, last, one, 0)

    def conv_copy(to):
        return remote(
            conv_out.at[to], conv_in.at[t], a2a_send.at[to], a2a_recv.at[t], s, to
        )

    def conv_flush(inner):
        if not inner:
            conv_copy(partner).start()
        for far in range(1, Z):
            for to, there, _ in sides(far):
                middle = (to > 0) & (to < Z - 1)

                @pl.when(there & (middle if inner else jnp.logical_not(middle)))
                def _():
                    for c in range(2):
                        conv_copy(2 * to + c).start()

    marks = [1 + (T - 1) * i // 7 for i in (3, 5, 7)]
    conv_some(1, marks[0])
    z_step(1, 0)
    conv_some(marks[0], marks[1])
    z_step(1, 1)
    conv_some(marks[1], marks[2])
    z_step(2, 0)
    conv_flush(True)
    with jax.named_scope("rimwait"):
        rim_copy.wait()
    same = (rim_in[HALO : HALO + 1, :].astype(F32) == ids_row_ref[0:1, 0:1].astype(F32)) & (s > 0)
    padded[0:HALO, :] = jnp.where(same, rim_in[0:HALO, :].astype(F32), jnp.float32(0.0))
    conv_some(0, 1)
    x_step(1)
    z_step(2, 1)
    conv_flush(False)
    y_step(1)
    conv_in[t, :, :] = conv_out[t, :, :]

    rows = block
    for c in loads[4:7]:
        c.wait()
    cap = 2 * rows // E
    lane = lax.broadcasted_iota(jnp.int32, (rows, 128), 1)
    eye = lax.broadcasted_iota(jnp.int32, (rows, rows), 0) == lax.broadcasted_iota(
        jnp.int32, (rows, rows), 1
    )
    named = lax.dot_general(
        eye.astype(F32).astype(BF16),
        routing_ref[...].astype(F32).astype(BF16),
        (((1,), (1,)), ((), ())),
        preferred_element_type=F32,
    )
    first = named[:, 0:1]
    second = named[:, 1:2]
    lane_f = lane.astype(F32)
    chosen = (lane_f == first) | (lane_f == second)
    per_group = E // G
    group_low = lane_f * per_group
    in_group = (first >= group_low) & (first < group_low + per_group)
    row_i = lax.broadcasted_iota(jnp.int32, (rows, rows), 0)
    col_i = lax.broadcasted_iota(jnp.int32, (rows, rows), 1)
    before = jnp.dot(
        (row_i > col_i).astype(F32).astype(BF16),
        chosen.astype(F32).astype(BF16),
        preferred_element_type=F32,
    )
    slot = jnp.where(chosen, before, jnp.float32(-1.0))
    width_e = max(E, 8)
    expert_i = lax.broadcasted_iota(jnp.int32, (width_e, rows), 0)
    chosen_r = (routing_ref[0:1, :] == expert_i) | (routing_ref[1:2, :] == expert_i)
    before_r = jnp.dot(
        chosen_r.astype(F32).astype(BF16),
        (row_i < col_i).astype(F32).astype(BF16),
        preferred_element_type=F32,
    )
    slot_r = jnp.where(chosen_r, before_r, jnp.float32(-1.0))
    cap_i = lax.broadcasted_iota(jnp.int32, (cap, rows), 0).astype(F32)
    for e in range(E):
        picks[e, :, :] = (slot_r[e : e + 1, :] == cap_i).astype(F32).astype(BF16)

    all_parts = tuple(range(S))
    for k in range(3, Z):
        z_step(k, 0)
        x_step(k - 1)
        z_step(k, 1)
        finish_row(k - 2, all_parts)
        y_step(k - 1)
    finish_row(Z - 1, all_parts[:1])
    finish_row(Z - 2, all_parts[:-1])
    x_step(Z - 1)
    y_step(Z - 1)
    finish_row(Z - 1, all_parts[1:-1])

    with jax.named_scope("a2await"):
        total = jnp.sum(conv_in[t].astype(F32), axis=1, keepdims=True)
        for k in range(1, T):
            source = lax.rem(t + k, T)
            remote(
                conv_out.at[source],
                conv_in.at[source],
                a2a_send.at[source],
                a2a_recv.at[source],
                s,
                source,
            ).wait_recv()
            total = total + jnp.sum(conv_in[source].astype(F32), axis=1, keepdims=True)
    if paired:
        with jax.named_scope("d0"):
            d_start()
    with jax.named_scope("act"):
        average = total / (T * width)
        total = jnp.zeros((rows, 1), F32)
        for j in range(T):
            centered = conv_in[j].astype(F32) - average
            total = total + jnp.sum(centered * centered, axis=1, keepdims=True)
        scale = lax.rsqrt(total / (T * width) + epsilon)
        for j in range(T):
            cols = slice(j * width, (j + 1) * width)
            v = (conv_in[j].astype(F32) - average) * scale * gain_conv_ref[
                :, cols
            ] + bias_conv_ref[:, cols]
            act[:, cols] = (v / (1.0 + jnp.exp(-v))).astype(BF16)

    loads[7].wait()

    others = order[1:]
    prompt = others[:2] if square else others
    late = others[2:] if square else []

    def piece_cols(j):
        return pl.ds(pl.multiple_of(j * piece, piece), piece)

    def finish_last():
        for k in (Z - 2, Z - 1):
            finish_row(k, all_parts[-1:])

    def column(array, expert):
        mine = lane[:, : array.shape[1]] == expert
        return jnp.sum(jnp.where(mine, array, jnp.float32(0.0)), axis=1, keepdims=True)

    zero = jnp.float32(0.0)
    slot_iota = lax.broadcasted_iota(jnp.int32, (rows, cap), 1).astype(F32)
    ff = gate_w.shape[2]
    ff_step = min(ff, 256)


    if paired:
        C = CHUNKS
        part = cap // C
        mates = (s, nbr_x)

        def chunk(c):
            return pl.ds(c * part, part)

        def a_copy(j):
            return remote(
                outgoing.at[0, j], arrived.at[0, j], ex_send.at[0, j], ex_recv.at[0, j], nbr_x, t
            )

        def b_copy(j, c):
            return remote(
                outgoing.at[1, j, chunk(c), :],
                arrived.at[1, j, chunk(c), :],
                ex_send.at[1 + c, j],
                ex_recv.at[1 + c, j],
                nbr_y,
                t,
            )

        def f_copy(j, c):
            return remote(
                arrived.at[1, j, chunk(c), :],
                arrived.at[2, j, chunk(c), :],
                ex_send.at[1 + C + c, j],
                ex_recv.at[1 + C + c, j],
                nbr_x,
                t,
            )

        def h_rows(kind, c):
            return pl.ds(0, cap) if kind == 0 else chunk(c)

        def hx_copy(kind, c):
            at = h_rows(kind, c)
            return remote(
                h_out.at[kind, at, :],
                h_in.at[kind, at, :],
                hx_send.at[kind, c],
                hx_recv.at[kind, c],
                nbr_x,
                t,
            )

        def rt_copy(q, c):
            return remote(
                back_out.at[q, chunk(c), :],
                back_in.at[q, chunk(c), :],
                rt_send.at[q, c],
                rt_recv.at[q, c],
                nbr_y,
                t,
            )

        y_order = [nbr_y, diag, s, nbr_x]

        def project(i, j):
            with jax.named_scope("wpwait"):
                for o in range(Z):
                    p_wait(o, j)
            cols = piece_cols(j)
            acc = residual[:, cols].astype(F32)
            acc = acc + jnp.dot(act[...], wfull[j], preferred_element_type=F32)
            state = acc.astype(BF16)
            hidden[:, cols] = state
            outgoing[1, j, :, :] = jnp.dot(
                picks[nbr_y], state, preferred_element_type=F32
            ).astype(BF16)
            b_copy(j, 0).start()
            outgoing[0, j, :, :] = jnp.dot(
                picks[s], state, preferred_element_type=F32
            ).astype(BF16)
            if i < 2:
                a_copy(j).start()

        def forward(c, first, last):
            with jax.named_scope(f"fwd{c}{first}"):
                for j in y_order[first:last]:
                    b_copy(j, c).wait_recv()
                    f_copy(j, c).start()

        router_lane = lax.broadcasted_iota(jnp.int32, (1, router_all.shape[0]), 1)
        group_lane = router_lane < G
        own_group_lane = router_lane == s // 2
        own_lane = router_lane == s + G
        mate_lane = (router_lane == s + G) | (router_lane == nbr_x + G)

        def gate_up(source, at, count, target):
            def square_step(j, squares):
                x = source[j, at, :].astype(F32)
                return squares + jnp.sum(x * x, axis=1, keepdims=True)

            total = lax.fori_loop(0, S, square_step, jnp.zeros((count, 1), F32))
            row_scale = lax.rsqrt(total / D + epsilon)

            def norm_step(j, _):
                cols = piece_cols(j)
                x = source[j, at, :].astype(F32)
                normed_in[0:count, cols] = (x * row_scale * gain_moe_ref[:, cols]).astype(BF16)
                return 0

            lax.fori_loop(0, S, norm_step, 0)
            logits = lax.dot_general(
                normed_in[0:count, :],
                router_all[...],
                (((1,), (1,)), ((), ())),
                preferred_element_type=F32,
            )
            exps = jnp.exp(logits)

            def over(mask):
                return jnp.sum(jnp.where(mask, exps, zero), axis=1, keepdims=True)

            weight = over(own_group_lane) / over(group_lane) * over(own_lane) / over(mate_lane)

            def up_step(j, _):
                cols = pl.ds(pl.multiple_of(j * ff_step, ff_step), ff_step)
                x = normed_in[0:count, :]
                g = jnp.dot(x, gate_w[0, :, cols], preferred_element_type=F32)
                u = jnp.dot(x, up_w[0, :, cols], preferred_element_type=F32)
                target[at, cols] = (g / (1.0 + jnp.exp(-g)) * u * weight).astype(BF16)
                return 0

            lax.fori_loop(0, ff // ff_step, up_step, 0)

        def each_block(k, act_on):
            def pair(o, side):
                def one(c2, _):
                    act_on(2 * o + c2)
                    return 0

                lax.fori_loop(0, 2, one, 0)

            if k == 0:
                pair(z, 0)
            else:
                each_slice(k, pair)

        def wide_cols(q):
            return pl.ds(pl.multiple_of(q * wide, wide), wide)

        def both(kind, at, q):
            acc = jnp.dot(
                h_own[kind, at, :], down_w[0, :, wide_cols(q)], preferred_element_type=F32
            )
            acc = acc + jnp.dot(h_in[kind, at, :], down_x[q], preferred_element_type=F32)
            return acc.astype(BF16)

        def down_b(k, c):
            def block_of(q):
                back_out[q, chunk(c), :] = both(1, chunk(c), q)
                rt_copy(q, c).start()

            with jax.named_scope(f"down{k}{c}"):
                if c == 0:
                    if k == 0:
                        dp_wait(z)
                    else:
                        each_slice(k, lambda o, side: dp_wait(o))
                each_block(k, block_of)

        for i, j in enumerate(order):
            with jax.named_scope(f"project{i}"):
                project(i, j)
            if i == 0:
                finish_last()
        for c in range(1, C):
            for j in order:
                b_copy(j, c).start()
        forward(0, 0, S // 2)
        for c in loads[8:]:
            c.wait()
        blank = jnp.zeros((router_all.shape[0] - G - E, D), F32)
        router_all[...] = jnp.concatenate(
            [group_router_ref[...].astype(F32), expert_router_ref[...].astype(F32), blank], axis=0
        ).astype(BF16)
        forward(0, S // 2, S)
        everyone = pl.ds(0, cap)
        with jax.named_scope("guB0"):
            gate_up(arrived.at[1], chunk(0), part, h_own.at[1])
        forward(1, 0, S // 2)
        with jax.named_scope("guA"):
            gate_up(outgoing.at[0], everyone, cap, h_own.at[0])
        forward(1, S // 2, S)
        d_step(1)
        with jax.named_scope("fw0"):
            for j in y_order:
                f_copy(j, 0).wait_recv()
        with jax.named_scope("guF0"):
            gate_up(arrived.at[2], chunk(0), part, h_out.at[1])
        hx_copy(1, 0).start()
        a_copy(order[2]).start()
        with jax.named_scope("guB1"):
            gate_up(arrived.at[1], chunk(1), part, h_own.at[1])
        with jax.named_scope("fw1"):
            for j in y_order:
                f_copy(j, 1).wait_recv()
        with jax.named_scope("guF1"):
            gate_up(arrived.at[2], chunk(1), part, h_out.at[1])
        hx_copy(1, 1).start()
        a_copy(order[3]).start()
        d_step(2)
        for e, at in enumerate((s, nbr_y)):
            spreads[e, :, :] = jnp.where(
                column(slot, at) == slot_iota, jnp.float32(1.0), zero
            ).astype(BF16)
        with jax.named_scope("hw0"):
            hx_copy(1, 0).wait_recv()
        down_b(0, 0)
        down_b(1, 0)
        with jax.named_scope("hw1"):
            hx_copy(1, 1).wait_recv()
        down_b(0, 1)
        down_b(1, 1)
        with jax.named_scope("aw"):
            for j in order:
                a_copy(j).wait_recv()
        with jax.named_scope("guX"):
            gate_up(arrived.at[0], everyone, cap, h_out.at[0])
        hx_copy(0, 0).start()
        for k in range(2, Z):
            if k > 2:
                d_step(k)
            for c in range(C):
                down_b(k, c)
        with jax.named_scope("hwA"):
            hx_copy(0, 0).wait_recv()

        def combine(q):
            for c in range(C):
                rt_copy(q, c).wait_recv()
            cols = wide_cols(q)
            acc = hidden[:, cols].astype(F32)
            acc = acc + jnp.dot(spreads[0], both(0, everyone, q), preferred_element_type=F32)
            acc = acc + jnp.dot(spreads[1], back_in[q], preferred_element_type=F32)
            out_ref[:, cols] = acc.astype(BF16)

        for k in range(Z):
            with jax.named_scope(f"combine{k}"):
                each_block(k, combine)

        with jax.named_scope("sendwait"):
            dx_copy.wait_send()
            for i in range(S):
                a_copy(i).wait_send()
                for c in range(C):
                    b_copy(i, c).wait_send()
                    f_copy(i, c).wait_send()
            hx_copy(0, 0).wait_send()
            for c in range(C):
                hx_copy(1, c).wait_send()
                for q in range(T):
                    rt_copy(q, c).wait_send()

            @pl.when(has_up)
            def _():
                zd_copy(z, 0, z + 1).wait_send()

            @pl.when(has_down)
            def _():
                zd_copy(z, 1, z - 1).wait_send()

            dp_copy(z).wait_send()

            def d_sent(o, side):
                @pl.when(has_down if side else has_up)
                def _():
                    zd_copy(o, side, z - 1 if side else z + 1).wait_send()

                dp_copy(o).wait_send()

            for k in range(1, Z):
                each_slice(k, d_sent)

    else:
        def disp_copy(expert, j):
            return remote(
                outgoing.at[expert, j],
                arrived.at[s, j],
                disp_send.at[expert, j],
                disp_recv.at[s, j],
                expert,
                t,
            )

        def disp_wait(sender, j):
            remote(
                outgoing.at[sender, j],
                arrived.at[sender, j],
                disp_send.at[sender, j],
                disp_recv.at[sender, j],
                sender,
                t,
            ).wait_recv()

        def ret_copy(sender, j):
            return remote(
                results.at[sender, j],
                returned.at[s, j],
                ret_send.at[sender, j],
                ret_recv.at[s, j],
                sender,
                t,
            )

        def ret_wait(expert, j):
            remote(
                results.at[expert, j],
                returned.at[expert, j],
                ret_send.at[expert, j],
                ret_recv.at[expert, j],
                expert,
                t,
            ).wait_recv()

        def project(j, squares):
            with jax.named_scope("wpwait"):
                for o in range(Z):
                    p_wait(o, j)
            cols = piece_cols(j)
            acc = residual[:, cols].astype(F32)
            part = jnp.dot(act[...], wfull[j], preferred_element_type=F32)
            state = (acc + part).astype(BF16)
            hidden[:, cols] = state
            for expert in others:
                outgoing[expert, j, :, :] = jnp.dot(
                    picks[expert], state, preferred_element_type=F32
                ).astype(BF16)
            for expert in prompt:
                disp_copy(expert, j).start()
            arrived[s, j, :, :] = jnp.dot(picks[s], state, preferred_element_type=F32).astype(BF16)
            state = state.astype(F32)
            return squares + jnp.sum(state * state, axis=1, keepdims=True)

        squares = jnp.zeros((rows, 1), F32)
        if square:
            for i, j in enumerate(order):
                with jax.named_scope(f"project{i}"):
                    squares = project(j, squares)
                if i == 0:
                    finish_last()
        else:
            finish_last()
            squares = lax.fori_loop(0, S, project, squares)
        for expert in late:
            for j in order:
                disp_copy(expert, j).start()

        for c in loads[8:]:
            c.wait()

        def expert_block(sender, target, send):
            def square_step(j, squares):
                x = arrived[sender, j].astype(F32)
                return squares + jnp.sum(x * x, axis=1, keepdims=True)

            total = lax.fori_loop(0, S, square_step, jnp.zeros((cap, 1), F32))
            row_scale = lax.rsqrt(total / D + epsilon)

            def norm_step(j, _):
                cols = piece_cols(j)
                x = arrived[sender, j].astype(F32)
                normed_in[:, cols] = (x * row_scale * gain_moe_ref[:, cols]).astype(BF16)
                return 0

            lax.fori_loop(0, S, norm_step, 0)

            def up_step(j, _):
                cols = pl.ds(pl.multiple_of(j * ff_step, ff_step), ff_step)
                x = normed_in[...]
                g = jnp.dot(x, gate_w[0, :, cols], preferred_element_type=F32)
                u = jnp.dot(x, up_w[0, :, cols], preferred_element_type=F32)
                ffn_hidden[:, cols] = (g / (1.0 + jnp.exp(-g)) * u).astype(BF16)
                return 0

            lax.fori_loop(0, ff // ff_step, up_step, 0)

            def down_step(j, _):
                target[j, :, :] = jnp.dot(
                    ffn_hidden[...], down_w[0, :, piece_cols(j)], preferred_element_type=F32
                ).astype(BF16)
                if send:
                    ret_copy(sender, j).start()
                return 0

            lax.fori_loop(0, S, down_step, 0)

        with jax.named_scope("ffnown"):
            expert_block(s, returned.at[s], False)

        scale = lax.rsqrt(squares / D + epsilon)

        def norm_cols(j, _):
            cols = piece_cols(j)
            normed[:, cols] = (hidden[:, cols].astype(F32) * scale * gain_moe_ref[:, cols]).astype(BF16)
            return 0

        def logits(router):
            return lax.dot_general(
                normed[...], router[...], (((1,), (1,)), ((), ())), preferred_element_type=F32
            )

        with jax.named_scope("router"):
            lax.fori_loop(0, S, norm_cols, 0)
            group_exp = jnp.exp(logits(group_router_ref))
            expert_exp = jnp.exp(logits(expert_router_ref))
            group_prob = jnp.sum(
                jnp.where(in_group[:, :G], group_exp, zero), axis=1, keepdims=True
            ) / jnp.sum(group_exp, axis=1, keepdims=True)
            chosen_exp = jnp.where(chosen[:, :E], expert_exp, zero)
            mix = group_prob * chosen_exp / jnp.sum(chosen_exp, axis=1, keepdims=True)
            for e in range(E):
                spreads[e, :, :] = jnp.where(
                    column(slot, e) == slot_iota, column(mix, e), zero
                ).astype(BF16)

        for i, sender in enumerate(others):
            with jax.named_scope(f"dispwait{i}"):
                for j in range(S):
                    disp_wait(sender, j)
            with jax.named_scope(f"ffn{i}"):
                expert_block(sender, results.at[sender], True)

        def combine(j, _):
            cols = piece_cols(j)
            for expert in others:
                ret_wait(expert, j)
            acc = hidden[:, cols].astype(F32)
            for e in range(E):
                acc = acc + jnp.dot(spreads[e], returned[e, j], preferred_element_type=F32)
            out_ref[:, cols] = acc.astype(BF16)
            return 0

        with jax.named_scope("combine"):
            lax.fori_loop(0, S, combine, 0)


        for expert in others:
            for j in range(S):
                disp_copy(expert, j).wait_send()
                ret_copy(expert, j).wait_send()

    with jax.named_scope("sendwait"):
        for h in range(H):

            @pl.when(has_up)
            def _():
                z_copy(z, h, 0, z + 1).wait_send()

            @pl.when(has_down)
            def _():
                z_copy(z, h, 1, z - 1).wait_send()

        for j in range(S):
            p_copy(z, j).wait_send()
        def sent(o, side):
            beyond = has_down if side else has_up
            for h in range(H):

                @pl.when(beyond)
                def _():
                    z_copy(o, h, side, z - 1 if side else z + 1).wait_send()

                for j in range(3 if square else S - 1):
                    x_copy(o, s, h, j, lax.rem(s + 1, S)).wait_send()
            for j in range(S):
                p_copy(o, j).wait_send()

        for k in range(1, Z):
            each_slice(k, sent)
        for k in range(1, T):
            conv_copy(lax.rem(t + k, T)).wait_send()


def body(
    S,
    T,
    conv_value,
    conv_gate,
    doc_ids,
    conv_kernel,
    norm_gain_conv,
    norm_bias_conv,
    proj_weight,
    residual,
    norm_gain_moe,
    group_router,
    expert_router,
    routing,
    expert_gate_w,
    expert_up_w,
    expert_down_w,
):
    tokens, width = conv_value.shape
    rows, D = residual.shape
    wrows = proj_weight.shape[0]
    ff = expert_gate_w.shape[2]
    G = group_router.shape[1]
    E = expert_router.shape[1]
    cap = 2 * rows // E
    hbm = pl.BlockSpec(memory_space=pl.ANY)
    dma = pltpu.SemaphoreType.DMA
    piece = D // S
    Z = T // 2
    return pl.pallas_call(
        functools.partial(kernel, S, T, G),
        out_shape=pltpu.VMEM((rows, D), BF16),
        in_specs=[hbm] * 15,
        out_specs=pl.BlockSpec(memory_space=pltpu.VMEM),
        scratch_shapes=[
            pltpu.VMEM((1, tokens), jnp.int32),
            pltpu.VMEM(conv_kernel.shape, BF16),
            pltpu.VMEM((1, T * width), F32),
            pltpu.VMEM((1, T * width), F32),
            pltpu.VMEM((1, D), F32),
            pltpu.VMEM((G, D), BF16),
            pltpu.VMEM((E, D), BF16),
            pltpu.VMEM((2, rows), jnp.int32),
            pltpu.VMEM((tokens, width), BF16),
            pltpu.VMEM((tokens, width), BF16),
            pltpu.VMEM((S, T * wrows, piece), BF16),
            pltpu.VMEM((rows, D), BF16),
            pltpu.VMEM((1, D, ff), BF16),
            pltpu.VMEM((1, D, ff), BF16),
            pltpu.VMEM((1, ff, D), BF16),
            pltpu.VMEM((HALO + 16, width), BF16),
            pltpu.VMEM((HALO + 16, width), BF16),
            pltpu.VMEM((tokens + HALO, width), F32),
            pltpu.VMEM((32, width), F32),
            pltpu.VMEM((tokens, 128), F32),
            pltpu.VMEM((T, rows, width), BF16),
            pltpu.VMEM((T, rows, width), BF16),
            pltpu.VMEM((rows, T * width), BF16),
            pltpu.VMEM((rows, D), BF16),
            pltpu.VMEM((rows, D), BF16),
            pltpu.VMEM((cap, D), BF16),
            pltpu.VMEM((E, cap, rows), BF16),
            pltpu.VMEM((E, rows, cap), BF16),
            pltpu.VMEM((E, S, cap, piece), BF16),
            pltpu.VMEM((E, S, cap, piece), BF16),
            pltpu.VMEM((cap, ff), BF16),
            pltpu.VMEM((E, S, cap, piece), BF16),
            pltpu.VMEM((E, S, cap, piece), BF16),
            pltpu.VMEM((G + E + (-G - E) % 8, D), BF16),
            pltpu.VMEM((ff, D // T), BF16),
            pltpu.VMEM((T, ff, D // T), BF16),
            pltpu.VMEM((2, cap, ff), BF16),
            pltpu.VMEM((2, cap, ff), BF16),
            pltpu.VMEM((2, cap, ff), BF16),
            pltpu.VMEM((T, cap, D // T), BF16),
            pltpu.VMEM((T, cap, D // T), BF16),
            dma((15,)),
            dma((S,)),
            dma((2,)),
            dma((2, Z, 2)),
            dma((Z, 2)),
            dma((max(S - 1, 3), Z, 2)),
            dma((S, Z, 2)),
            dma((Z, S)),
            dma((Z, S)),
            dma((T,)),
            dma((T,)),
            dma((S, S)),
            dma((S, S)),
            dma((S, S)),
            dma((S, S)),
            dma((1 + 2 * CHUNKS, S)),
            dma((1 + 2 * CHUNKS, S)),
            dma((2, CHUNKS)),
            dma((2, CHUNKS)),
            dma((T, CHUNKS)),
            dma((T, CHUNKS)),
            dma((2, Z)),
            dma((Z,)),
            dma((Z,)),
            dma((Z,)),
            dma((2,)),
        ],
        compiler_params=pltpu.CompilerParams(
            collective_id=0, has_side_effects=True, vmem_limit_bytes=60 * 1024 * 1024
        ),
    )(
        conv_value,
        conv_gate,
        doc_ids[None, :],
        conv_kernel,
        norm_gain_conv[None, :],
        norm_bias_conv[None, :],
        proj_weight,
        residual,
        norm_gain_moe[None, :],
        group_router.T,
        expert_router.T,
        routing.T,
        expert_gate_w,
        expert_up_w,
        expert_down_w,
    )


def solution(mesh):
    placed = (
        P("sp", "tp"),
        P("sp", "tp"),
        P("sp"),
        P(None, "tp"),
        P(),
        P(),
        P("tp", None),
        P(("sp", "tp"), None),
        P(),
        P(),
        P(),
        P(("sp", "tp"), None),
        P("sp", None, None),
        P("sp", None, None),
        P("sp", None, None),
    )
    return jax.shard_map(
        functools.partial(body, mesh.shape["sp"], mesh.shape["tp"]),
        mesh=mesh,
        in_specs=placed,
        out_specs=P(("sp", "tp"), None),
        check_vma=False,
    )
```

```python
import functools

import jax
import jax.numpy as jnp
from jax import lax
from jax.experimental import pallas as pl
from jax.experimental.pallas import tpu as pltpu
from jax.sharding import PartitionSpec as P

epsilon = 1e-06
MESH = pl.DeviceIdType.MESH
F32 = jnp.float32
BF16 = jnp.bfloat16
HALO = 32
CHUNKS = 2


def gate(value, gate_value):
    return (value.astype(F32) * jax.nn.sigmoid(gate_value.astype(F32))).astype(BF16)


def kernel(
    S,
    T,
    G,
    value_hbm,
    gate_hbm,
    ids_hbm,
    kernel_hbm,
    gain_conv_hbm,
    bias_conv_hbm,
    weight_hbm,
    residual_hbm,
    gain_moe_hbm,
    group_router_hbm,
    expert_router_hbm,
    routing_hbm,
    gate_w_hbm,
    up_w_hbm,
    down_w_hbm,
    out_ref,
    ids_row_ref,
    kernel_ref,
    gain_conv_ref,
    bias_conv_ref,
    gain_moe_ref,
    group_router_ref,
    expert_router_ref,
    routing_ref,
    value,
    gates,
    wfull,
    residual,
    gate_w,
    up_w,
    down_w,
    rim_out,
    rim_in,
    padded,
    taps,
    least_tap,
    conv_out,
    conv_in,
    act,
    hidden,
    normed,
    normed_in,
    picks,
    spreads,
    outgoing,
    arrived,
    ffn_hidden,
    results,
    returned,
    router_all,
    down_stage,
    down_x,
    h_own,
    h_out,
    h_in,
    back_out,
    back_in,
    own_down,
    spread_all,
    base_out,
    local_sem,
    wl_sem,
    rim_sem,
    wz_send,
    wz_recv,
    wx_send,
    wx_recv,
    wp_send,
    wp_recv,
    a2a_send,
    a2a_recv,
    disp_send,
    disp_recv,
    ret_send,
    ret_recv,
    ex_send,
    ex_recv,
    hx_send,
    hx_recv,
    rt_send,
    rt_recv,
    zd_send,
    zd_recv,
    dp_send,
    dp_recv,
    dx_sem,
):
    s = lax.axis_index("sp")
    t = lax.axis_index("tp")
    Z = T // 2
    z = t // 2
    core = t % 2
    partner = 2 * z + 1 - core
    tokens, width = value.shape
    block = tokens // T
    n_taps = kernel_ref.shape[0]
    piece = wfull.shape[2]
    wrows = wfull.shape[1] // T
    D = S * piece
    square = S == 4
    E = S
    paired = square and expert_router_ref.shape[0] == S and E == 2 * G
    wide = D // T
    H = 2
    part_rows = wrows // H

    def remote(src, dst, send, recv, sp_to, tp_to):
        return pltpu.make_async_remote_copy(
            src_ref=src,
            dst_ref=dst,
            send_sem=send,
            recv_sem=recv,
            device_id=(sp_to, tp_to),
            device_id_type=MESH,
        )

    barrier = pltpu.get_barrier_semaphore()
    for k in range(1, T):
        pl.semaphore_signal(
            barrier, inc=1, device_id=(s, lax.rem(t + k, T)), device_id_type=MESH
        )
    for k in range(1, S):
        pl.semaphore_signal(
            barrier, inc=1, device_id=(lax.rem(s + k, S), t), device_id_type=MESH
        )

    loads = [
        pltpu.make_async_copy(a, b, local_sem.at[i])
        for i, (a, b) in enumerate(
            [
                (ids_hbm, ids_row_ref),
                (value_hbm, value),
                (gate_hbm, gates),
                (kernel_hbm, kernel_ref),
                (routing_hbm, routing_ref),
                (gain_conv_hbm, gain_conv_ref),
                (bias_conv_hbm, bias_conv_ref),
                (residual_hbm, residual),
                (gain_moe_hbm, gain_moe_ref),
                (group_router_hbm, group_router_ref),
                (expert_router_hbm, expert_router_ref),
                (gate_w_hbm, gate_w),
                (up_w_hbm, up_w),
                (down_w_hbm, down_w),
            ]
        )
    ]
    nbr_x = s + 1 - 2 * (s % 2)
    nbr_y = s + 2 - 4 * (s // 2)
    diag = 3 - s
    order = [s, nbr_x, nbr_y, diag] if square else [lax.rem(s + S - j, S) for j in range(S)]
    own_rows = pl.ds(pl.multiple_of(t * wrows, wrows), wrows)
    own_w = [
        pltpu.make_async_copy(
            weight_hbm.at[:, pl.ds(pl.multiple_of(j * piece, piece), piece)],
            wfull.at[j, own_rows, :],
            wl_sem.at[i],
        )
        for i, j in enumerate(order)
    ]
    stage = pltpu.make_async_copy(
        down_w_hbm.at[0, :, pl.ds(pl.multiple_of(t * wide, wide), wide)],
        down_stage,
        local_sem.at[14],
    )
    loads[0].start()
    own_w[0].start()
    if paired:
        stage.start()
    for c in loads[1:4]:
        c.start()

    loads[0].wait()
    ids_row = jnp.broadcast_to(ids_row_ref[...], (8, tokens))
    position = lax.broadcasted_iota(jnp.int32, (8, tokens), 1)
    low = jnp.int32(-n_taps)
    fresh = (ids_row != pltpu.roll(ids_row, 1, 1)) & (position > 0)
    begin = jnp.where(fresh, position, low)
    shift = 1
    while shift < n_taps:
        moved = jnp.where(position >= shift, pltpu.roll(begin, shift, 1), low)
        begin = jnp.maximum(begin, moved)
        shift *= 2
    least_row = (n_taps - 1 - position + begin).astype(F32)
    lanes = least_tap.shape[1]
    for c in range(tokens // lanes):
        across = jnp.broadcast_to(least_row[0:1, c * lanes : (c + 1) * lanes], (lanes, lanes))
        least_tap[c * lanes : (c + 1) * lanes, :] = across.T

    with jax.named_scope("barrier"):
        pl.semaphore_wait(barrier, T + S - 2)

    def w_ref(o, p, h):
        base = pl.multiple_of((2 * o + core) * wrows + h * part_rows, part_rows)
        return wfull.at[p, pl.ds(base, part_rows), :]

    def z_copy(o, h, up, to):
        ref = w_ref(o, s, h)
        return remote(ref, ref, wz_send.at[up, o, h], wz_recv.at[o, h], s, 2 * to + core)

    def x_copy(o, p, h, role, to):
        ref = w_ref(o, p, h)
        return remote(ref, ref, wx_send.at[0], wx_recv.at[role, o, h], to, t)

    def p_copy(o, p):
        rows_at = pl.ds(pl.multiple_of((2 * o + core) * wrows, wrows), wrows)
        ref = wfull.at[p, rows_at, :]
        return remote(ref, ref, wp_send.at[0], wp_recv.at[p], s, partner)

    def p_wait(p):
        ref = wfull.at[p, pl.ds(0, Z * wrows), :]
        remote(ref, ref, wp_send.at[0], wp_recv.at[p], s, partner).wait_recv()

    has_up = z + 1 < Z
    has_down = z > 0
    own_w[0].wait()
    for h in range(H):

        @pl.when(has_up)
        def _():
            z_copy(z, h, 0, z + 1).start()

        @pl.when(has_down)
        def _():
            z_copy(z, h, 1, z - 1).start()

    for c in own_w[1:]:
        c.start()
    for c in loads[4:]:
        c.start()
    dx_copy = remote(down_stage, down_x.at[t], dx_sem.at[0], dx_sem.at[1], nbr_x, t)
    if paired:
        stage.wait()
        dx_copy.start()
    p_copy(z, s).start()

    def sides(k):
        return ((z - k, z - k >= 0, 0), (z + k, z + k < Z, 1))

    def each_slice(k, act_on):
        for o, there, side in sides(k):
            pl.when(there)(functools.partial(act_on, o, side))

    def z_step(k, h):
        def one(o, side):
            z_copy(o, h, side, z).wait_recv()
            beyond = has_down if side else has_up

            @pl.when(beyond)
            def _():
                z_copy(o, h, side, z - 1 if side else z + 1).start()

            if square:
                x_copy(o, s, h, 0, nbr_x).start()
                x_copy(o, s, h, 1, nbr_y).start()
            else:
                for j in range(1, S):
                    x_copy(o, s, h, j - 1, lax.rem(s + j, S)).start()

        with jax.named_scope(f"z{k}{h}"):
            each_slice(k, one)

    def x_step(k):
        def one(o, side):
            x_copy(o, nbr_x, 0, 0, nbr_y).wait_recv()
            x_copy(o, nbr_x, 0, 2, nbr_y).start()

        if square:
            with jax.named_scope(f"x{k}"):
                each_slice(k, one)

    def y_step(k):
        def one(o, side):
            x_copy(o, nbr_y, 1, 1, nbr_x).wait_recv()
            x_copy(o, nbr_y, 1, 2, nbr_x).start()

        if square:
            with jax.named_scope(f"y{k}"):
                each_slice(k, one)

    def zd_copy(o, side, to):
        ref = down_x.at[2 * o + core]
        return remote(ref, ref, zd_send.at[side, o], zd_recv.at[o], s, 2 * to + core)

    def dp_copy(o):
        ref = down_x.at[2 * o + core]
        return remote(ref, ref, dp_send.at[0], dp_recv.at[o], s, partner)

    def dp_wait(o):
        ref = down_x.at[2 * o + 1 - core]
        remote(ref, ref, dp_send.at[0], dp_recv.at[o], s, partner).wait_recv()

    def at_edge(o):
        return (o == 0) | (o == Z - 1)

    def d_start(edges):
        if edges:
            dx_copy.wait_recv()
            dp_copy(z).start()
        mine = at_edge(z) if edges else jnp.logical_not(at_edge(z))

        @pl.when(mine & has_up)
        def _():
            zd_copy(z, 0, z + 1).start()

        @pl.when(mine & has_down)
        def _():
            zd_copy(z, 1, z - 1).start()

    def d_step(k, edges=None):
        def one(o, side):
            zd_copy(o, side, z).wait_recv()

            @pl.when(has_down if side else has_up)
            def _():
                zd_copy(o, side, z - 1 if side else z + 1).start()

            dp_copy(o).start()

        def some(o, side):
            pl.when(at_edge(o) if edges else jnp.logical_not(at_edge(o)))(
                functools.partial(one, o, side)
            )

        with jax.named_scope(f"d{k}"):
            each_slice(k, one if edges is None else some)

    def finish_row(k, parts):
        def one(o, side):
            for i in parts:
                p = order[i]
                if i > 0 and square:
                    for h in ((1,), (0,), (0, 1))[i - 1]:
                        x_copy(o, p, h, i - 1, p).wait_recv()
                elif i > 0:
                    for h in range(H):
                        x_copy(o, p, h, i - 1, p).wait_recv()
                p_copy(o, p).start()

        with jax.named_scope(f"fin{k}{parts[0]}"):
            each_slice(k, one)

    for c in loads[1:4]:
        c.wait()
    tail = pl.ds(tokens - HALO, HALO)
    last_reach = jnp.max(least_tap[tokens - 1 : tokens, :], axis=1, keepdims=True)
    row_at = lax.broadcasted_iota(jnp.int32, (HALO, width), 0).astype(F32)
    newer = row_at >= last_reach + (HALO - n_taps)
    rim = jnp.where(newer, gate(value[tail, :], gates[tail, :]).astype(F32), jnp.float32(0.0))
    rim_out[0:HALO, :] = rim.astype(BF16)
    last_id = ids_row_ref[0:1, tokens - 1 : tokens].astype(F32)
    rim_out[HALO : HALO + 16, :] = jnp.broadcast_to(last_id, (16, width)).astype(BF16)
    rim_copy = remote(
        rim_out, rim_in, rim_sem.at[0], rim_sem.at[1], lax.rem(s + 1, S), t
    )
    rim_copy.start()

    def gate_rows(i, _):
        rows = pl.ds(pl.multiple_of(i * 64, 64), 64)
        to_rows = pl.ds(pl.multiple_of(HALO + i * 64, 32), 64)
        padded[to_rows, :] = gate(value[rows, :], gates[rows, :]).astype(F32)
        return 0

    with jax.named_scope("gate"):
        lax.fori_loop(0, tokens // 64, gate_rows, 0)
    taps[0:n_taps, :] = kernel_ref[...].astype(F32)

    step_rows = 32 if block % 32 == 0 else 8
    lanes = min(width, 128)

    def conv_block(owner):
        def conv_rows(i, _):
            base = pl.multiple_of(owner * block + i * step_rows, 8)
            least = least_tap[pl.ds(base, step_rows), :]
            window = padded[pl.ds(base, step_rows + HALO), :]
            total = jnp.zeros((step_rows, width), F32)
            for tap in range(n_taps):
                at = tap + HALO + 1 - n_taps
                valid = least <= tap
                product = window[at : at + step_rows, :] * taps[tap : tap + 1, :]
                parts = [
                    jnp.where(valid, product[:, j : j + lanes], jnp.float32(0.0))
                    for j in range(0, width, lanes)
                ]
                total = total + jnp.concatenate(parts, axis=1)
            conv_out[
                owner, pl.ds(pl.multiple_of(i * step_rows, step_rows), step_rows), :
            ] = total.astype(BF16)
            return 0

        lax.fori_loop(0, block // step_rows, conv_rows, 0)

    def conv_some(first, last):
        with jax.named_scope("conv"):

            def one(owner, _):
                conv_block(owner)
                return 0

            lax.fori_loop(first, last, one, 0)

    def conv_copy(to):
        return remote(
            conv_out.at[to], conv_in.at[t], a2a_send.at[0], a2a_recv.at[t], s, to
        )

    def conv_flush(inner):
        if not inner:
            conv_copy(partner).start()
        for far in range(1, Z):
            for to, there, _ in sides(far):
                middle = (to > 0) & (to < Z - 1)

                @pl.when(there & (middle if inner else jnp.logical_not(middle)))
                def _():
                    for c in range(2):
                        conv_copy(2 * to + c).start()

    marks = [1 + (T - 2) * i // 6 for i in (1, 2, 4, 6)]
    conv_some(1, marks[0])
    for i in range(1, S):
        own_w[i].wait()
        p_copy(z, order[i]).start()
    conv_some(marks[0], marks[1])
    z_step(1, 0)
    conv_some(marks[1], marks[2])
    z_step(1, 1)
    conv_some(marks[2], marks[3])
    z_step(2, 0)
    conv_flush(True)
    conv_some(marks[3], T)
    with jax.named_scope("rimwait"):
        rim_copy.wait()
    same = (rim_in[HALO : HALO + 1, :].astype(F32) == ids_row_ref[0:1, 0:1].astype(F32)) & (s > 0)
    padded[0:HALO, :] = jnp.where(same, rim_in[0:HALO, :].astype(F32), jnp.float32(0.0))
    conv_some(0, 1)
    x_step(1)
    z_step(2, 1)
    conv_flush(False)
    if paired:
        d_start(True)
    y_step(1)
    conv_in[t, :, :] = conv_out[t, :, :]

    rows = block
    for c in loads[4:7]:
        c.wait()
    cap = 2 * rows // E
    lane = lax.broadcasted_iota(jnp.int32, (rows, 128), 1)
    eye = lax.broadcasted_iota(jnp.int32, (rows, rows), 0) == lax.broadcasted_iota(
        jnp.int32, (rows, rows), 1
    )
    named = lax.dot_general(
        eye.astype(F32).astype(BF16),
        routing_ref[...].astype(F32).astype(BF16),
        (((1,), (1,)), ((), ())),
        preferred_element_type=F32,
    )
    first = named[:, 0:1]
    second = named[:, 1:2]
    lane_f = lane.astype(F32)
    chosen = (lane_f == first) | (lane_f == second)
    per_group = E // G
    group_low = lane_f * per_group
    in_group = (first >= group_low) & (first < group_low + per_group)
    row_i = lax.broadcasted_iota(jnp.int32, (rows, rows), 0)
    col_i = lax.broadcasted_iota(jnp.int32, (rows, rows), 1)
    before = jnp.dot(
        (row_i > col_i).astype(F32).astype(BF16),
        chosen.astype(F32).astype(BF16),
        preferred_element_type=F32,
    )
    slot = jnp.where(chosen, before, jnp.float32(-1.0))
    width_e = max(E, 8)
    expert_i = lax.broadcasted_iota(jnp.int32, (width_e, rows), 0)
    chosen_r = (routing_ref[0:1, :] == expert_i) | (routing_ref[1:2, :] == expert_i)
    before_r = jnp.dot(
        chosen_r.astype(F32).astype(BF16),
        (row_i < col_i).astype(F32).astype(BF16),
        preferred_element_type=F32,
    )
    slot_r = jnp.where(chosen_r, before_r, jnp.float32(-1.0))
    cap_i = lax.broadcasted_iota(jnp.int32, (cap, rows), 0).astype(F32)
    for e in range(E):
        picks[e, :, :] = (slot_r[e : e + 1, :] == cap_i).astype(F32).astype(BF16)

    def piece_cols(j):
        return pl.ds(pl.multiple_of(j * piece, piece), piece)

    def finish_last():
        for k in (Z - 2, Z - 1):
            finish_row(k, all_parts[-1:])

    def column(array, expert):
        mine = lane[:, : array.shape[1]] == expert
        return jnp.sum(jnp.where(mine, array, jnp.float32(0.0)), axis=1, keepdims=True)

    zero = jnp.float32(0.0)
    slot_iota = lax.broadcasted_iota(jnp.int32, (rows, cap), 1).astype(F32)
    ff = gate_w.shape[2]
    ff_step = min(ff, 256)


    if paired:
        for c in loads[8:]:
            c.wait()
        blank = jnp.zeros((router_all.shape[0] - G - E, D), F32)
        router_all[...] = jnp.concatenate(
            [group_router_ref[...].astype(F32), expert_router_ref[...].astype(F32), blank], axis=0
        ).astype(BF16)
        for e, at in enumerate((s, nbr_y)):
            spread_all[e, :, :] = jnp.where(
                column(slot, at) == slot_iota, jnp.float32(1.0), zero
            ).astype(BF16)
    all_parts = tuple(range(S))
    for k in range(3, Z):
        z_step(k, 0)
        x_step(k - 1)
        z_step(k, 1)
        finish_row(k - 2, all_parts)
        y_step(k - 1)
    finish_row(Z - 1, all_parts[:1])
    finish_row(Z - 2, all_parts[:-1])
    x_step(Z - 1)
    y_step(Z - 1)
    finish_row(Z - 1, all_parts[1:-1])

    with jax.named_scope("a2await"):
        total = jnp.sum(conv_in[t].astype(F32), axis=1, keepdims=True)
        for k in range(1, T):
            source = lax.rem(t + k, T)
            remote(
                conv_out.at[source],
                conv_in.at[source],
                a2a_send.at[0],
                a2a_recv.at[source],
                s,
                source,
            ).wait_recv()
            total = total + jnp.sum(conv_in[source].astype(F32), axis=1, keepdims=True)
    if paired:
        with jax.named_scope("d0"):
            d_start(False)
            d_step(1, True)
    with jax.named_scope("act"):
        average = total / (T * width)
        total = jnp.zeros((rows, 1), F32)
        for j in range(T):
            centered = conv_in[j].astype(F32) - average
            total = total + jnp.sum(centered * centered, axis=1, keepdims=True)
        scale = lax.rsqrt(total / (T * width) + epsilon)
        for j in range(T):
            cols = slice(j * width, (j + 1) * width)
            v = (conv_in[j].astype(F32) - average) * scale * gain_conv_ref[
                :, cols
            ] + bias_conv_ref[:, cols]
            act[:, cols] = (v / (1.0 + jnp.exp(-v))).astype(BF16)

    loads[7].wait()

    others = order[1:]
    prompt = others[:2] if square else others
    late = others[2:] if square else []

    if paired:
        C = CHUNKS
        part = cap // C
        mates = (s, nbr_x)

        def chunk(c):
            return pl.ds(c * part, part)

        def a_copy(j):
            return remote(
                outgoing.at[0, j], arrived.at[0, j], ex_send.at[0], ex_recv.at[0], nbr_x, t
            )

        def b_copy(j, c):
            return remote(
                outgoing.at[1, j, chunk(c), :],
                arrived.at[1, j, chunk(c), :],
                ex_send.at[0],
                ex_recv.at[1 + c * S + j],
                nbr_y,
                t,
            )

        def f_copy(j, c):
            return remote(
                arrived.at[1, j, chunk(c), :],
                arrived.at[2, j, chunk(c), :],
                ex_send.at[0],
                ex_recv.at[1 + C * S + c],
                nbr_x,
                t,
            )

        def h_rows(kind, c):
            return pl.ds(0, cap) if kind == 0 else chunk(c)

        def hx_copy(kind, c):
            at = h_rows(kind, c)
            return remote(
                h_out.at[kind, at, :],
                h_in.at[kind, at, :],
                hx_send.at[0],
                hx_recv.at[kind, c],
                nbr_x,
                t,
            )

        def rt_copy(q, c):
            return remote(
                back_out.at[q, chunk(c), :],
                back_in.at[q, pl.ds(cap + c * part, part), :],
                rt_send.at[0],
                rt_recv.at[q],
                nbr_y,
                t,
            )

        def a_wait():
            ref = arrived.at[0]
            remote(ref, ref, ex_send.at[0], ex_recv.at[0], nbr_x, t).wait_recv()

        def f_wait(c):
            ref = arrived.at[2, :, chunk(c), :]
            remote(ref, ref, ex_send.at[0], ex_recv.at[1 + C * S + c], nbr_x, t).wait_recv()

        def rt_wait(q):
            ref = back_in.at[q, pl.ds(cap, cap), :]
            remote(ref, ref, rt_send.at[0], rt_recv.at[q], nbr_y, t).wait_recv()

        y_order = [nbr_y, diag, s, nbr_x]

        def project(i, j):
            with jax.named_scope("wpwait"):
                p_wait(j)
            cols = piece_cols(j)
            acc = residual[:, cols].astype(F32)
            acc = acc + jnp.dot(act[...], wfull[j], preferred_element_type=F32)
            state = acc.astype(BF16)
            hidden[:, cols] = state
            outgoing[1, j, :, :] = jnp.dot(
                picks[nbr_y], state, preferred_element_type=F32
            ).astype(BF16)
            b_copy(j, 0).start()
            if i == 0:
                for c in range(1, C):
                    b_copy(j, c).start()
            outgoing[0, j, :, :] = jnp.dot(
                picks[s], state, preferred_element_type=F32
            ).astype(BF16)
            if i < 2:
                a_copy(j).start()

        def forward(c, first, last):
            with jax.named_scope(f"fwd{c}{first}"):
                for j in y_order[first:last]:
                    b_copy(j, c).wait_recv()
                    f_copy(j, c).start()

        router_lane = lax.broadcasted_iota(jnp.int32, (1, router_all.shape[0]), 1)
        group_lane = router_lane < G
        own_group_lane = router_lane == s // 2
        own_lane = router_lane == s + G
        mate_lane = (router_lane == s + G) | (router_lane == nbr_x + G)

        def gate_up(source, at, count, target):
            total = jnp.zeros((count, 1), F32)
            for j in range(S):
                x = source[j, at, :].astype(F32)
                total = total + jnp.sum(x * x, axis=1, keepdims=True)
            row_scale = lax.rsqrt(total / D + epsilon)
            for j in range(S):
                cols = slice(j * piece, (j + 1) * piece)
                x = source[j, at, :].astype(F32)
                normed_in[0:count, cols] = (x * row_scale * gain_moe_ref[:, cols]).astype(BF16)
            logits = lax.dot_general(
                normed_in[0:count, :],
                router_all[...],
                (((1,), (1,)), ((), ())),
                preferred_element_type=F32,
            )
            exps = jnp.exp(logits)

            def over(mask):
                return jnp.sum(jnp.where(mask, exps, zero), axis=1, keepdims=True)

            weight = over(own_group_lane) / over(group_lane) * over(own_lane) / over(mate_lane)

            for j in range(ff // ff_step):
                cols = slice(j * ff_step, (j + 1) * ff_step)
                x = normed_in[0:count, :]
                g = jnp.dot(x, gate_w[0, :, cols], preferred_element_type=F32)
                u = jnp.dot(x, up_w[0, :, cols], preferred_element_type=F32)
                target[at, cols] = (g / (1.0 + jnp.exp(-g)) * u * weight).astype(BF16)

        def each_block(k, act_on):
            def pair(o, side):
                for c2 in range(2):
                    act_on(2 * o + c2)

            if k == 0:
                pair(z, 0)
            else:
                each_slice(k, pair)

        def wide_cols(q):
            return pl.ds(pl.multiple_of(q * wide, wide), wide)

        def both(kind, at, q):
            acc = jnp.dot(
                h_own[kind, at, :], down_w[0, :, wide_cols(q)], preferred_element_type=F32
            )
            acc = acc + jnp.dot(h_in[kind, at, :], down_x[q], preferred_element_type=F32)
            return acc.astype(BF16)

        def down_b(k, c):
            def block_of(q):
                back_out[q, chunk(c), :] = both(1, chunk(c), q)
                rt_copy(q, c).start()

            with jax.named_scope(f"down{k}{c}"):
                if c == 0:
                    if k == 0:
                        dp_wait(z)
                    else:
                        each_slice(k, lambda o, side: dp_wait(o))
                each_block(k, block_of)

        everyone = pl.ds(0, cap)
        for i, j in enumerate(order):
            with jax.named_scope(f"project{i}"):
                project(i, j)
            if i == 0:
                finish_last()
            if i == 2:
                forward(0, 0, 1)
        for c in range(1, C):
            for j in order[1:]:
                b_copy(j, c).start()
        with jax.named_scope("guA"):
            gate_up(outgoing.at[0], everyone, cap, h_own.at[0])
        forward(0, 1, 3)
        d_step(1, False)
        forward(0, 3, 4)
        with jax.named_scope("guB0"):
            gate_up(arrived.at[1], chunk(0), part, h_own.at[1])
        forward(1, 0, 4)
        with jax.named_scope("fw0"):
            f_wait(0)
        with jax.named_scope("guF0"):
            gate_up(arrived.at[2], chunk(0), part, h_out.at[1])
        hx_copy(1, 0).start()
        a_copy(order[2]).start()
        with jax.named_scope("guB1"):
            gate_up(arrived.at[1], chunk(1), part, h_own.at[1])
        d_step(2)
        with jax.named_scope("fw1"):
            f_wait(1)
        with jax.named_scope("guF1"):
            gate_up(arrived.at[2], chunk(1), part, h_out.at[1])
        hx_copy(1, 1).start()
        a_copy(order[3]).start()
        with jax.named_scope("hw0"):
            hx_copy(1, 0).wait_recv()
        down_b(0, 0)
        down_b(1, 0)
        with jax.named_scope("hw1"):
            hx_copy(1, 1).wait_recv()
        down_b(0, 1)
        down_b(1, 1)
        with jax.named_scope("aw"):
            a_wait()
        with jax.named_scope("guX"):
            gate_up(arrived.at[0], everyone, cap, h_out.at[0])
        hx_copy(0, 0).start()
        for k in range(3, Z):
            d_step(k)
        for k in range(2, Z):
            for c in range(C):
                down_b(k, c)
        with jax.named_scope("own_down"):
            for q in range(T):
                own_down[q, :, :] = jnp.dot(
                    h_own[0], down_w[0, :, q * wide : (q + 1) * wide], preferred_element_type=F32
                )

        def combine_b(q):
            rt_wait(q)
            mixed = jnp.dot(
                spread_all[1], back_in[q, cap : 2 * cap, :], preferred_element_type=F32
            )
            base_out[q, :, :] = hidden[:, wide_cols(q)].astype(F32) + mixed

        def combine_a(q):
            acc = own_down[q] + jnp.dot(h_in[0], down_x[q], preferred_element_type=F32)
            mixed = jnp.dot(spread_all[0], acc.astype(BF16), preferred_element_type=F32)
            out_ref[:, wide_cols(q)] = (base_out[q] + mixed).astype(BF16)

        def combine(q):
            combine_b(q)
            combine_a(q)

        ahead = min(2, Z)
        for k in range(ahead):
            with jax.named_scope(f"comb_b{k}"):
                each_block(k, combine_b)
        with jax.named_scope("hwA"):
            hx_copy(0, 0).wait_recv()

        for k in range(Z):
            with jax.named_scope(f"combine{k}"):
                each_block(k, combine_a if k < ahead else combine)

        with jax.named_scope("sendwait"):
            dx_copy.wait_send()
            sets = outgoing.at[0:3]
            remote(sets, sets, ex_send.at[0], ex_recv.at[0], nbr_x, t).wait_send()
            remote(h_out, h_out, hx_send.at[0], hx_recv.at[0, 0], nbr_x, t).wait_send()
            remote(back_out, back_out, rt_send.at[0], rt_recv.at[0], nbr_y, t).wait_send()
            ref = down_x.at[0:Z]
            remote(ref, ref, dp_send.at[0], dp_recv.at[0], s, partner).wait_send()

            @pl.when(has_up)
            def _():
                zd_copy(z, 0, z + 1).wait_send()

            @pl.when(has_down)
            def _():
                zd_copy(z, 1, z - 1).wait_send()

            def d_sent(o, side):
                @pl.when(has_down if side else has_up)
                def _():
                    zd_copy(o, side, z - 1 if side else z + 1).wait_send()

            for k in range(1, Z):
                each_slice(k, d_sent)

    else:
        def disp_copy(expert, j):
            return remote(
                outgoing.at[expert, j],
                arrived.at[s, j],
                disp_send.at[expert, j],
                disp_recv.at[s, j],
                expert,
                t,
            )

        def disp_wait(sender, j):
            remote(
                outgoing.at[sender, j],
                arrived.at[sender, j],
                disp_send.at[sender, j],
                disp_recv.at[sender, j],
                sender,
                t,
            ).wait_recv()

        def ret_copy(sender, j):
            return remote(
                results.at[sender, j],
                returned.at[s, j],
                ret_send.at[sender, j],
                ret_recv.at[s, j],
                sender,
                t,
            )

        def ret_wait(expert, j):
            remote(
                results.at[expert, j],
                returned.at[expert, j],
                ret_send.at[expert, j],
                ret_recv.at[expert, j],
                expert,
                t,
            ).wait_recv()

        def project(j, squares):
            with jax.named_scope("wpwait"):
                p_wait(j)
            cols = piece_cols(j)
            acc = residual[:, cols].astype(F32)
            part = jnp.dot(act[...], wfull[j], preferred_element_type=F32)
            state = (acc + part).astype(BF16)
            hidden[:, cols] = state
            for expert in others:
                outgoing[expert, j, :, :] = jnp.dot(
                    picks[expert], state, preferred_element_type=F32
                ).astype(BF16)
            for expert in prompt:
                disp_copy(expert, j).start()
            arrived[s, j, :, :] = jnp.dot(picks[s], state, preferred_element_type=F32).astype(BF16)
            state = state.astype(F32)
            return squares + jnp.sum(state * state, axis=1, keepdims=True)

        squares = jnp.zeros((rows, 1), F32)
        if square:
            for i, j in enumerate(order):
                with jax.named_scope(f"project{i}"):
                    squares = project(j, squares)
                if i == 0:
                    finish_last()
        else:
            finish_last()
            squares = lax.fori_loop(0, S, project, squares)
        for expert in late:
            for j in order:
                disp_copy(expert, j).start()

        for c in loads[8:]:
            c.wait()

        def expert_block(sender, target, send):
            def square_step(j, squares):
                x = arrived[sender, j].astype(F32)
                return squares + jnp.sum(x * x, axis=1, keepdims=True)

            total = lax.fori_loop(0, S, square_step, jnp.zeros((cap, 1), F32))
            row_scale = lax.rsqrt(total / D + epsilon)

            def norm_step(j, _):
                cols = piece_cols(j)
                x = arrived[sender, j].astype(F32)
                normed_in[:, cols] = (x * row_scale * gain_moe_ref[:, cols]).astype(BF16)
                return 0

            lax.fori_loop(0, S, norm_step, 0)

            def up_step(j, _):
                cols = pl.ds(pl.multiple_of(j * ff_step, ff_step), ff_step)
                x = normed_in[...]
                g = jnp.dot(x, gate_w[0, :, cols], preferred_element_type=F32)
                u = jnp.dot(x, up_w[0, :, cols], preferred_element_type=F32)
                ffn_hidden[:, cols] = (g / (1.0 + jnp.exp(-g)) * u).astype(BF16)
                return 0

            lax.fori_loop(0, ff // ff_step, up_step, 0)

            def down_step(j, _):
                target[j, :, :] = jnp.dot(
                    ffn_hidden[...], down_w[0, :, piece_cols(j)], preferred_element_type=F32
                ).astype(BF16)
                if send:
                    ret_copy(sender, j).start()
                return 0

            lax.fori_loop(0, S, down_step, 0)

        with jax.named_scope("ffnown"):
            expert_block(s, returned.at[s], False)

        scale = lax.rsqrt(squares / D + epsilon)

        def norm_cols(j, _):
            cols = piece_cols(j)
            normed[:, cols] = (hidden[:, cols].astype(F32) * scale * gain_moe_ref[:, cols]).astype(BF16)
            return 0

        def logits(router):
            return lax.dot_general(
                normed[...], router[...], (((1,), (1,)), ((), ())), preferred_element_type=F32
            )

        with jax.named_scope("router"):
            lax.fori_loop(0, S, norm_cols, 0)
            group_exp = jnp.exp(logits(group_router_ref))
            expert_exp = jnp.exp(logits(expert_router_ref))
            group_prob = jnp.sum(
                jnp.where(in_group[:, :G], group_exp, zero), axis=1, keepdims=True
            ) / jnp.sum(group_exp, axis=1, keepdims=True)
            chosen_exp = jnp.where(chosen[:, :E], expert_exp, zero)
            mix = group_prob * chosen_exp / jnp.sum(chosen_exp, axis=1, keepdims=True)
            for e in range(E):
                spreads[e, :, :] = jnp.where(
                    column(slot, e) == slot_iota, column(mix, e), zero
                ).astype(BF16)

        for i, sender in enumerate(others):
            with jax.named_scope(f"dispwait{i}"):
                for j in range(S):
                    disp_wait(sender, j)
            with jax.named_scope(f"ffn{i}"):
                expert_block(sender, results.at[sender], True)

        def combine(j, _):
            cols = piece_cols(j)
            for expert in others:
                ret_wait(expert, j)
            acc = hidden[:, cols].astype(F32)
            for e in range(E):
                acc = acc + jnp.dot(spreads[e], returned[e, j], preferred_element_type=F32)
            out_ref[:, cols] = acc.astype(BF16)
            return 0

        with jax.named_scope("combine"):
            lax.fori_loop(0, S, combine, 0)


        for expert in others:
            for j in range(S):
                disp_copy(expert, j).wait_send()
                ret_copy(expert, j).wait_send()

    with jax.named_scope("sendwait"):
        for h in range(H):

            @pl.when(has_up)
            def _():
                z_copy(z, h, 0, z + 1).wait_send()

            @pl.when(has_down)
            def _():
                z_copy(z, h, 1, z - 1).wait_send()

        def sent(o, side):
            for h in range(H):

                @pl.when(has_down if side else has_up)
                def _():
                    z_copy(o, h, side, z - 1 if side else z + 1).wait_send()

        for k in range(1, Z):
            each_slice(k, sent)
        ref = wfull.at[0 : S - 1, pl.ds(0, (Z - 1) * wrows), :]
        remote(ref, ref, wx_send.at[0], wx_recv.at[0, 0, 0], order[1], t).wait_send()
        ref = wfull.at[:, pl.ds(0, Z * wrows), :]
        remote(ref, ref, wp_send.at[0], wp_recv.at[0], s, partner).wait_send()
        ref = conv_out.at[0 : T - 1]
        remote(ref, ref, a2a_send.at[0], a2a_recv.at[0], s, partner).wait_send()


def body(
    S,
    T,
    conv_value,
    conv_gate,
    doc_ids,
    conv_kernel,
    norm_gain_conv,
    norm_bias_conv,
    proj_weight,
    residual,
    norm_gain_moe,
    group_router,
    expert_router,
    routing,
    expert_gate_w,
    expert_up_w,
    expert_down_w,
):
    tokens, width = conv_value.shape
    rows, D = residual.shape
    wrows = proj_weight.shape[0]
    ff = expert_gate_w.shape[2]
    G = group_router.shape[1]
    E = expert_router.shape[1]
    cap = 2 * rows // E
    hbm = pl.BlockSpec(memory_space=pl.ANY)
    dma = pltpu.SemaphoreType.DMA
    piece = D // S
    Z = T // 2
    paired = S == 4 and E == S and E == 2 * G
    return pl.pallas_call(
        functools.partial(kernel, S, T, G),
        out_shape=pltpu.VMEM((rows, D), BF16),
        in_specs=[hbm] * 15,
        out_specs=pl.BlockSpec(memory_space=pltpu.VMEM),
        scratch_shapes=[
            pltpu.VMEM((1, tokens), jnp.int32),
            pltpu.VMEM(conv_kernel.shape, BF16),
            pltpu.VMEM((1, T * width), F32),
            pltpu.VMEM((1, T * width), F32),
            pltpu.VMEM((1, D), F32),
            pltpu.VMEM((G, D), BF16),
            pltpu.VMEM((E, D), BF16),
            pltpu.VMEM((2, rows), jnp.int32),
            pltpu.VMEM((tokens, width), BF16),
            pltpu.VMEM((tokens, width), BF16),
            pltpu.VMEM((S, T * wrows, piece), BF16),
            pltpu.VMEM((rows, D), BF16),
            pltpu.VMEM((1, D, ff), BF16),
            pltpu.VMEM((1, D, ff), BF16),
            pltpu.VMEM((1, ff, D), BF16),
            pltpu.VMEM((HALO + 16, width), BF16),
            pltpu.VMEM((HALO + 16, width), BF16),
            pltpu.VMEM((tokens + HALO, width), F32),
            pltpu.VMEM((32, width), F32),
            pltpu.VMEM((tokens, 128), F32),
            pltpu.VMEM((T, rows, width), BF16),
            pltpu.VMEM((T, rows, width), BF16),
            pltpu.VMEM((rows, T * width), BF16),
            pltpu.VMEM((rows, D), BF16),
            pltpu.VMEM((rows, D), BF16),
            pltpu.VMEM((cap, D), BF16),
            pltpu.VMEM((E, cap, rows), BF16),
            pltpu.VMEM((E, rows, cap), BF16),
            pltpu.VMEM((E, S, cap, piece), BF16),
            pltpu.VMEM((E, S, cap, piece), BF16),
            pltpu.VMEM((cap, ff), BF16),
            pltpu.VMEM((E, S, cap, piece), BF16),
            pltpu.VMEM((E, S, cap, piece), BF16),
            pltpu.VMEM((G + E + (-G - E) % 8, D), BF16),
            pltpu.VMEM((ff, D // T), BF16),
            pltpu.VMEM((T, ff, D // T), BF16),
            pltpu.VMEM((2, cap, ff), BF16),
            pltpu.VMEM((2, cap, ff), BF16),
            pltpu.VMEM((2, cap, ff), BF16),
            pltpu.VMEM((T, cap, D // T), BF16),
            pltpu.VMEM((T, 2 * cap, D // T), BF16),
            pltpu.VMEM((T, cap, D // T), F32),
            pltpu.VMEM((2, rows, cap), BF16),
            pltpu.VMEM((T, rows, D // T), F32),
            dma((15,)),
            dma((S,)),
            dma((2,)),
            dma((2, Z, 2)),
            dma((Z, 2)),
            dma((1,)),
            dma((S - 1, Z, 2)),
            dma((1,)),
            dma((S,)),
            dma((1,)),
            dma((T,)),
            dma((1, 1) if paired else (S, S)),
            dma((1, 1) if paired else (S, S)),
            dma((1, 1) if paired else (S, S)),
            dma((1, 1) if paired else (S, S)),
            dma((1,)),
            dma((1 + CHUNKS * (S + 1),)),
            dma((1,)),
            dma((2, CHUNKS)),
            dma((1,)),
            dma((T,)),
            dma((2, Z)),
            dma((Z,)),
            dma((1,)),
            dma((Z,)),
            dma((2,)),
        ],
        compiler_params=pltpu.CompilerParams(
            collective_id=0, has_side_effects=True, vmem_limit_bytes=60 * 1024 * 1024
        ),
    )(
        conv_value,
        conv_gate,
        doc_ids[None, :],
        conv_kernel,
        norm_gain_conv[None, :],
        norm_bias_conv[None, :],
        proj_weight,
        residual,
        norm_gain_moe[None, :],
        group_router.T,
        expert_router.T,
        routing.T,
        expert_gate_w,
        expert_up_w,
        expert_down_w,
    )


def solution(mesh):
    placed = (
        P("sp", "tp"),
        P("sp", "tp"),
        P("sp"),
        P(None, "tp"),
        P(),
        P(),
        P("tp", None),
        P(("sp", "tp"), None),
        P(),
        P(),
        P(),
        P(("sp", "tp"), None),
        P("sp", None, None),
        P("sp", None, None),
        P("sp", None, None),
    )
    return jax.shard_map(
        functools.partial(body, mesh.shape["sp"], mesh.shape["tp"]),
        mesh=mesh,
        in_specs=placed,
        out_specs=P(("sp", "tp"), None),
        check_vma=False,
    )
```

```python
import functools

import jax
import jax.numpy as jnp
from jax import lax
from jax.experimental import pallas as pl
from jax.experimental.pallas import tpu as pltpu
from jax.sharding import PartitionSpec as P

epsilon = 1e-06
MESH = pl.DeviceIdType.MESH
F32 = jnp.float32
BF16 = jnp.bfloat16
HALO = 32
CHUNKS = 2


def gate(value, gate_value):
    return (value.astype(F32) * jax.nn.sigmoid(gate_value.astype(F32))).astype(BF16)


def kernel(
    S,
    T,
    G,
    value_hbm,
    gate_hbm,
    ids_hbm,
    kernel_hbm,
    gain_conv_hbm,
    bias_conv_hbm,
    weight_hbm,
    residual_hbm,
    gain_moe_hbm,
    group_router_hbm,
    expert_router_hbm,
    routing_hbm,
    gate_w_hbm,
    up_w_hbm,
    down_w_hbm,
    out_ref,
    ids_row_ref,
    kernel_ref,
    gain_conv_ref,
    bias_conv_ref,
    gain_moe_ref,
    group_router_ref,
    expert_router_ref,
    routing_ref,
    value,
    gates,
    wfull,
    residual,
    gate_w,
    up_w,
    down_w,
    rim_out,
    rim_in,
    padded,
    taps,
    least_tap,
    conv_out,
    conv_in,
    act,
    hidden,
    normed,
    normed_in,
    picks,
    spreads,
    outgoing,
    arrived,
    ffn_hidden,
    results,
    returned,
    router_all,
    down_stage,
    down_x,
    h_own,
    h_out,
    h_in,
    back_out,
    back_in,
    h_rows,
    spread_all,
    base_out,
    local_sem,
    wl_sem,
    rim_sem,
    wz_send,
    wz_recv,
    wx_send,
    wx_recv,
    wp_send,
    wp_recv,
    a2a_send,
    a2a_recv,
    disp_send,
    disp_recv,
    ret_send,
    ret_recv,
    ex_send,
    ex_recv,
    hx_send,
    hx_recv,
    rt_send,
    rt_recv,
    zd_send,
    zd_recv,
    dp_send,
    dp_recv,
    dx_sem,
):
    s = lax.axis_index("sp")
    t = lax.axis_index("tp")
    Z = T // 2
    z = t // 2
    core = t % 2
    partner = 2 * z + 1 - core
    tokens, width = value.shape
    block = tokens // T
    n_taps = kernel_ref.shape[0]
    piece = wfull.shape[2]
    wrows = wfull.shape[1] // T
    D = S * piece
    square = S == 4
    E = S
    paired = square and expert_router_ref.shape[0] == S and E == 2 * G
    wide = D // T
    H = 2
    part_rows = wrows // H

    def remote(src, dst, send, recv, sp_to, tp_to):
        return pltpu.make_async_remote_copy(
            src_ref=src,
            dst_ref=dst,
            send_sem=send,
            recv_sem=recv,
            device_id=(sp_to, tp_to),
            device_id_type=MESH,
        )

    barrier = pltpu.get_barrier_semaphore()
    for k in range(1, T):
        pl.semaphore_signal(
            barrier, inc=1, device_id=(s, lax.rem(t + k, T)), device_id_type=MESH
        )
    for k in range(1, S):
        pl.semaphore_signal(
            barrier, inc=1, device_id=(lax.rem(s + k, S), t), device_id_type=MESH
        )

    loads = [
        pltpu.make_async_copy(a, b, local_sem.at[i])
        for i, (a, b) in enumerate(
            [
                (ids_hbm, ids_row_ref),
                (value_hbm, value),
                (gate_hbm, gates),
                (kernel_hbm, kernel_ref),
                (routing_hbm, routing_ref),
                (gain_conv_hbm, gain_conv_ref),
                (bias_conv_hbm, bias_conv_ref),
                (residual_hbm, residual),
                (gain_moe_hbm, gain_moe_ref),
                (group_router_hbm, group_router_ref),
                (expert_router_hbm, expert_router_ref),
                (gate_w_hbm, gate_w),
                (up_w_hbm, up_w),
                (down_w_hbm, down_w),
            ]
        )
    ]
    nbr_x = s + 1 - 2 * (s % 2)
    nbr_y = s + 2 - 4 * (s // 2)
    diag = 3 - s
    order = [s, nbr_x, nbr_y, diag] if square else [lax.rem(s + S - j, S) for j in range(S)]
    own_rows = pl.ds(pl.multiple_of(t * wrows, wrows), wrows)
    own_w = [
        pltpu.make_async_copy(
            weight_hbm.at[:, pl.ds(pl.multiple_of(j * piece, piece), piece)],
            wfull.at[j, own_rows, :],
            wl_sem.at[i],
        )
        for i, j in enumerate(order)
    ]
    stage = pltpu.make_async_copy(
        down_w_hbm.at[0, :, pl.ds(pl.multiple_of(t * wide, wide), wide)],
        down_stage,
        local_sem.at[14],
    )
    loads[0].start()
    own_w[0].start()
    if paired:
        stage.start()
    for c in loads[1:4]:
        c.start()

    with jax.named_scope("barrier"):
        pl.semaphore_wait(barrier, T + S - 2)

    def w_ref(o, p, h):
        base = pl.multiple_of((2 * o + core) * wrows + h * part_rows, part_rows)
        return wfull.at[p, pl.ds(base, part_rows), :]

    def z_copy(o, h, up, to):
        ref = w_ref(o, s, h)
        return remote(ref, ref, wz_send.at[up], wz_recv.at[o, h], s, 2 * to + core)

    def x_copy(o, p, h, role, to):
        ref = w_ref(o, p, h)
        return remote(ref, ref, wx_send.at[0], wx_recv.at[role, o, h], to, t)

    def p_copy(o, p):
        rows_at = pl.ds(pl.multiple_of((2 * o + core) * wrows, wrows), wrows)
        ref = wfull.at[p, rows_at, :]
        return remote(ref, ref, wp_send.at[0], wp_recv.at[p], s, partner)

    def p_wait(p):
        ref = wfull.at[p, pl.ds(0, Z * wrows), :]
        remote(ref, ref, wp_send.at[0], wp_recv.at[p], s, partner).wait_recv()

    has_up = z + 1 < Z
    has_down = z > 0
    own_w[0].wait()
    for h in range(H):

        @pl.when(has_up)
        def _():
            z_copy(z, h, 0, z + 1).start()

        @pl.when(has_down)
        def _():
            z_copy(z, h, 1, z - 1).start()

    for c in own_w[1:]:
        c.start()
    for c in loads[4:]:
        c.start()
    dx_copy = remote(down_stage, down_x.at[t], dx_sem.at[0], dx_sem.at[1], nbr_x, t)
    if paired:
        stage.wait()
        dx_copy.start()
    p_copy(z, s).start()

    def sides(k):
        return ((z - k, z - k >= 0, 0), (z + k, z + k < Z, 1))

    def each_slice(k, act_on):
        for o, there, side in sides(k):
            pl.when(there)(functools.partial(act_on, o, side))

    def z_step(k, h):
        def one(o, side):
            z_copy(o, h, side, z).wait_recv()
            beyond = has_down if side else has_up

            @pl.when(beyond)
            def _():
                z_copy(o, h, side, z - 1 if side else z + 1).start()

            if square:
                x_copy(o, s, h, 0, nbr_x).start()
                x_copy(o, s, h, 1, nbr_y).start()
            else:
                for j in range(1, S):
                    x_copy(o, s, h, j - 1, lax.rem(s + j, S)).start()
            if h == H - 1:
                p_copy(o, s).start()

        with jax.named_scope(f"z{k}{h}"):
            each_slice(k, one)

    def x_step(k):
        def one(o, side):
            x_copy(o, nbr_x, 0, 0, nbr_y).wait_recv()
            x_copy(o, nbr_x, 0, 2, nbr_y).start()

        if square:
            with jax.named_scope(f"x{k}"):
                each_slice(k, one)

    def y_step(k):
        def one(o, side):
            x_copy(o, nbr_y, 1, 1, nbr_x).wait_recv()
            x_copy(o, nbr_y, 1, 2, nbr_x).start()

        if square:
            with jax.named_scope(f"y{k}"):
                each_slice(k, one)

    def zd_copy(o, side, to):
        ref = down_x.at[2 * o + core]
        return remote(ref, ref, zd_send.at[side], zd_recv.at[o], s, 2 * to + core)

    def dp_copy(o):
        ref = down_x.at[2 * o + core]
        return remote(ref, ref, dp_send.at[0], dp_recv.at[o], s, partner)

    def dp_wait(o):
        ref = down_x.at[2 * o + 1 - core]
        remote(ref, ref, dp_send.at[0], dp_recv.at[o], s, partner).wait_recv()

    def at_edge(o):
        return (o == 0) | (o == Z - 1)

    def d_start(edges):
        if edges:
            dx_copy.wait_recv()
            dp_copy(z).start()
        mine = at_edge(z) if edges else jnp.logical_not(at_edge(z))

        @pl.when(mine & has_up)
        def _():
            zd_copy(z, 0, z + 1).start()

        @pl.when(mine & has_down)
        def _():
            zd_copy(z, 1, z - 1).start()

    def d_step(k, edges=None):
        def one(o, side):
            zd_copy(o, side, z).wait_recv()

            @pl.when(has_down if side else has_up)
            def _():
                zd_copy(o, side, z - 1 if side else z + 1).start()

            dp_copy(o).start()

        def some(o, side):
            pl.when(at_edge(o) if edges else jnp.logical_not(at_edge(o)))(
                functools.partial(one, o, side)
            )

        with jax.named_scope(f"d{k}"):
            each_slice(k, one if edges is None else some)

    def finish_row(k, parts):
        def one(o, side):
            for i in parts:
                p = order[i]
                if square:
                    for h in ((1,), (0,), (0, 1))[i - 1]:
                        x_copy(o, p, h, i - 1, p).wait_recv()
                else:
                    for h in range(H):
                        x_copy(o, p, h, i - 1, p).wait_recv()
                p_copy(o, p).start()

        with jax.named_scope(f"fin{k}{parts[0]}"):
            each_slice(k, one)

    loads[0].wait()
    ids_row = jnp.broadcast_to(ids_row_ref[...], (8, tokens))
    position = lax.broadcasted_iota(jnp.int32, (8, tokens), 1)
    low = jnp.int32(-n_taps)
    fresh = (ids_row != pltpu.roll(ids_row, 1, 1)) & (position > 0)
    begin = jnp.where(fresh, position, low)
    shift = 1
    while shift < n_taps:
        moved = jnp.where(position >= shift, pltpu.roll(begin, shift, 1), low)
        begin = jnp.maximum(begin, moved)
        shift *= 2
    least_row = (n_taps - 1 - position + begin).astype(F32)
    lanes = least_tap.shape[1]
    for c in range(tokens // lanes):
        across = jnp.broadcast_to(least_row[0:1, c * lanes : (c + 1) * lanes], (lanes, lanes))
        least_tap[c * lanes : (c + 1) * lanes, :] = across.T

    for c in loads[1:4]:
        c.wait()
    tail = pl.ds(tokens - HALO, HALO)
    last_reach = jnp.max(least_tap[tokens - 1 : tokens, :], axis=1, keepdims=True)
    row_at = lax.broadcasted_iota(jnp.int32, (HALO, width), 0).astype(F32)
    newer = row_at >= last_reach + (HALO - n_taps)
    rim = jnp.where(newer, gate(value[tail, :], gates[tail, :]).astype(F32), jnp.float32(0.0))
    rim_out[0:HALO, :] = rim.astype(BF16)
    last_id = ids_row_ref[0:1, tokens - 1 : tokens].astype(F32)
    rim_out[HALO : HALO + 16, :] = jnp.broadcast_to(last_id, (16, width)).astype(BF16)
    rim_copy = remote(
        rim_out, rim_in, rim_sem.at[0], rim_sem.at[1], lax.rem(s + 1, S), t
    )
    rim_copy.start()

    def gate_rows(i, _):
        rows = pl.ds(pl.multiple_of(i * 64, 64), 64)
        to_rows = pl.ds(pl.multiple_of(HALO + i * 64, 32), 64)
        padded[to_rows, :] = gate(value[rows, :], gates[rows, :]).astype(F32)
        return 0

    with jax.named_scope("gate"):
        lax.fori_loop(0, tokens // 64, gate_rows, 0)
    taps[0:n_taps, :] = kernel_ref[...].astype(F32)

    step_rows = 32 if block % 32 == 0 else 8
    lanes = min(width, 128)

    def conv_block(owner):
        def conv_rows(i, _):
            base = pl.multiple_of(owner * block + i * step_rows, 8)
            least = least_tap[pl.ds(base, step_rows), :]
            window = padded[pl.ds(base, step_rows + HALO), :]
            total = jnp.zeros((step_rows, width), F32)
            for tap in range(n_taps):
                at = tap + HALO + 1 - n_taps
                valid = least <= tap
                product = window[at : at + step_rows, :] * taps[tap : tap + 1, :]
                parts = [
                    jnp.where(valid, product[:, j : j + lanes], jnp.float32(0.0))
                    for j in range(0, width, lanes)
                ]
                total = total + jnp.concatenate(parts, axis=1)
            conv_out[
                owner, pl.ds(pl.multiple_of(i * step_rows, step_rows), step_rows), :
            ] = total.astype(BF16)
            return 0

        lax.fori_loop(0, block // step_rows, conv_rows, 0)

    def conv_some(first, last):
        with jax.named_scope("conv"):

            def one(owner, _):
                conv_block(owner)
                return 0

            lax.fori_loop(first, last, one, 0)

    def conv_copy(to):
        return remote(
            conv_out.at[to], conv_in.at[t], a2a_send.at[0], a2a_recv.at[0], s, to
        )

    def conv_flush(inner):
        if not inner:
            conv_copy(partner).start()
        for far in range(1, Z):
            for to, there, _ in sides(far):
                middle = (to > 0) & (to < Z - 1)

                @pl.when(there & (middle if inner else jnp.logical_not(middle)))
                def _():
                    for c in range(2):
                        conv_copy(2 * to + c).start()

    marks = [1 + (T - 2) * i // 6 for i in (1, 2, 4, 6)]
    conv_some(1, marks[0])
    for i in range(1, S):
        own_w[i].wait()
        p_copy(z, order[i]).start()
    conv_some(marks[0], marks[1])
    z_step(1, 0)
    conv_some(marks[1], marks[2])
    z_step(1, 1)
    conv_some(marks[2], marks[3])
    z_step(2, 0)
    conv_flush(True)
    conv_some(marks[3], T)
    with jax.named_scope("rimwait"):
        rim_copy.wait()
    same = (rim_in[HALO : HALO + 1, :].astype(F32) == ids_row_ref[0:1, 0:1].astype(F32)) & (s > 0)
    padded[0:HALO, :] = jnp.where(same, rim_in[0:HALO, :].astype(F32), jnp.float32(0.0))
    conv_some(0, 1)
    x_step(1)
    z_step(2, 1)
    conv_flush(False)
    if paired:
        d_start(True)
    y_step(1)
    conv_in[t, :, :] = conv_out[t, :, :]

    rows = block
    for c in loads[4:7]:
        c.wait()
    cap = 2 * rows // E
    lane = lax.broadcasted_iota(jnp.int32, (rows, 128), 1)
    eye = lax.broadcasted_iota(jnp.int32, (rows, rows), 0) == lax.broadcasted_iota(
        jnp.int32, (rows, rows), 1
    )
    named = lax.dot_general(
        eye.astype(F32).astype(BF16),
        routing_ref[...].astype(F32).astype(BF16),
        (((1,), (1,)), ((), ())),
        preferred_element_type=F32,
    )
    first = named[:, 0:1]
    second = named[:, 1:2]
    lane_f = lane.astype(F32)
    chosen = (lane_f == first) | (lane_f == second)
    per_group = E // G
    group_low = lane_f * per_group
    in_group = (first >= group_low) & (first < group_low + per_group)
    row_i = lax.broadcasted_iota(jnp.int32, (rows, rows), 0)
    col_i = lax.broadcasted_iota(jnp.int32, (rows, rows), 1)
    before = jnp.dot(
        (row_i > col_i).astype(F32).astype(BF16),
        chosen.astype(F32).astype(BF16),
        preferred_element_type=F32,
    )
    slot = jnp.where(chosen, before, jnp.float32(-1.0))
    width_e = max(E, 8)
    expert_i = lax.broadcasted_iota(jnp.int32, (width_e, rows), 0)
    chosen_r = (routing_ref[0:1, :] == expert_i) | (routing_ref[1:2, :] == expert_i)
    before_r = jnp.dot(
        chosen_r.astype(F32).astype(BF16),
        (row_i < col_i).astype(F32).astype(BF16),
        preferred_element_type=F32,
    )
    slot_r = jnp.where(chosen_r, before_r, jnp.float32(-1.0))
    cap_i = lax.broadcasted_iota(jnp.int32, (cap, rows), 0).astype(F32)
    for e in range(E):
        picks[e, :, :] = (slot_r[e : e + 1, :] == cap_i).astype(F32).astype(BF16)

    def piece_cols(j):
        return pl.ds(pl.multiple_of(j * piece, piece), piece)

    def finish_last():
        for k in (Z - 2, Z - 1):
            finish_row(k, all_parts[-1:])

    def column(array, expert):
        mine = lane[:, : array.shape[1]] == expert
        return jnp.sum(jnp.where(mine, array, jnp.float32(0.0)), axis=1, keepdims=True)

    zero = jnp.float32(0.0)
    slot_iota = lax.broadcasted_iota(jnp.int32, (rows, cap), 1).astype(F32)
    ff = gate_w.shape[2]
    ff_step = min(ff, 256)


    if paired:
        for c in loads[8:]:
            c.wait()
        blank = jnp.zeros((router_all.shape[0] - G - E, D), F32)
        router_all[...] = jnp.concatenate(
            [group_router_ref[...].astype(F32), expert_router_ref[...].astype(F32), blank], axis=0
        ).astype(BF16)
        for e, at in enumerate((s, nbr_y)):
            spread_all[e, :, :] = jnp.where(
                column(slot, at) == slot_iota, jnp.float32(1.0), zero
            ).astype(BF16)
    all_parts = tuple(range(1, S))
    for k in range(3, Z):
        z_step(k, 0)
        x_step(k - 1)
        z_step(k, 1)
        finish_row(k - 2, all_parts)
        y_step(k - 1)
    finish_row(Z - 2, all_parts[:-1])
    x_step(Z - 1)
    y_step(Z - 1)
    finish_row(Z - 1, all_parts[:-1])

    with jax.named_scope("a2await"):
        ref = conv_in.at[0 : T - 1]
        remote(ref, ref, a2a_send.at[0], a2a_recv.at[0], s, partner).wait_recv()
    if paired:
        with jax.named_scope("d0"):
            d_start(False)
            d_step(1, True)
    with jax.named_scope("act"):
        total = jnp.zeros((rows, 1), F32)
        for j in range(T):
            total = total + jnp.sum(conv_in[j].astype(F32), axis=1, keepdims=True)
        average = total / (T * width)
        total = jnp.zeros((rows, 1), F32)
        for j in range(T):
            centered = conv_in[j].astype(F32) - average
            total = total + jnp.sum(centered * centered, axis=1, keepdims=True)
        scale = lax.rsqrt(total / (T * width) + epsilon)
        for j in range(T):
            cols = slice(j * width, (j + 1) * width)
            v = (conv_in[j].astype(F32) - average) * scale * gain_conv_ref[
                :, cols
            ] + bias_conv_ref[:, cols]
            act[:, cols] = (v / (1.0 + jnp.exp(-v))).astype(BF16)

    loads[7].wait()

    others = order[1:]
    prompt = others[:2] if square else others
    late = others[2:] if square else []

    if paired:
        C = CHUNKS
        part = cap // C
        mates = (s, nbr_x)

        def chunk(c):
            return pl.ds(c * part, part)

        def a_copy(j, c):
            return remote(
                outgoing.at[0, j, chunk(c), :],
                arrived.at[0, j, chunk(c), :],
                ex_send.at[0],
                ex_recv.at[C * (S + 1) + c],
                nbr_x,
                t,
            )

        def b_copy(j, c):
            return remote(
                outgoing.at[1, j, chunk(c), :],
                arrived.at[1, j, chunk(c), :],
                ex_send.at[0],
                ex_recv.at[c * S + j],
                nbr_y,
                t,
            )

        def f_copy(j, c):
            return remote(
                arrived.at[1, j, chunk(c), :],
                arrived.at[2, j, chunk(c), :],
                ex_send.at[0],
                ex_recv.at[C * S + c],
                nbr_x,
                t,
            )

        def hx_copy(kind, c):
            at = chunk(c)
            return remote(
                h_out.at[kind, at, :],
                h_in.at[kind, at, :],
                hx_send.at[0],
                hx_recv.at[kind, c],
                nbr_x,
                t,
            )

        def rt_copy(q, c):
            return remote(
                back_out.at[q, chunk(c), :],
                back_in.at[q, chunk(c), :],
                rt_send.at[0],
                rt_recv.at[q],
                nbr_y,
                t,
            )

        def a_wait(c):
            ref = arrived.at[0, :, chunk(c), :]
            remote(ref, ref, ex_send.at[0], ex_recv.at[C * (S + 1) + c], nbr_x, t).wait_recv()

        def f_wait(c):
            ref = arrived.at[2, :, chunk(c), :]
            remote(ref, ref, ex_send.at[0], ex_recv.at[C * S + c], nbr_x, t).wait_recv()

        def rt_wait(q):
            ref = back_in.at[q]
            remote(ref, ref, rt_send.at[0], rt_recv.at[q], nbr_y, t).wait_recv()

        y_order = [nbr_y, diag, s, nbr_x]

        def project(i, j):
            with jax.named_scope("wpwait"):
                p_wait(j)
            cols = piece_cols(j)
            acc = residual[:, cols].astype(F32)
            acc = acc + jnp.dot(act[...], wfull[j], preferred_element_type=F32)
            state = acc.astype(BF16)
            hidden[:, cols] = state
            outgoing[1, j, :, :] = jnp.dot(
                picks[nbr_y], state, preferred_element_type=F32
            ).astype(BF16)
            b_copy(j, 0).start()
            if i == 0:
                for c in range(1, C):
                    b_copy(j, c).start()
            outgoing[0, j, :, :] = jnp.dot(
                picks[s], state, preferred_element_type=F32
            ).astype(BF16)
            a_copy(j, 0).start()

        def forward(c, first, last):
            with jax.named_scope(f"fwd{c}{first}"):
                for j in y_order[first:last]:
                    b_copy(j, c).wait_recv()
                    f_copy(j, c).start()

        router_lane = lax.broadcasted_iota(jnp.int32, (1, router_all.shape[0]), 1)
        group_lane = router_lane < G
        own_group_lane = router_lane == s // 2
        own_lane = router_lane == s + G
        mate_lane = (router_lane == s + G) | (router_lane == nbr_x + G)

        def gate_up(source, at, count, target):
            total = jnp.zeros((count, 1), F32)
            for j in range(S):
                x = source[j, at, :].astype(F32)
                total = total + jnp.sum(x * x, axis=1, keepdims=True)
            row_scale = lax.rsqrt(total / D + epsilon)
            for j in range(S):
                cols = slice(j * piece, (j + 1) * piece)
                x = source[j, at, :].astype(F32)
                normed_in[0:count, cols] = (x * row_scale * gain_moe_ref[:, cols]).astype(BF16)
            logits = lax.dot_general(
                normed_in[0:count, :],
                router_all[...],
                (((1,), (1,)), ((), ())),
                preferred_element_type=F32,
            )
            exps = jnp.exp(logits)

            def over(mask):
                return jnp.sum(jnp.where(mask, exps, zero), axis=1, keepdims=True)

            weight = over(own_group_lane) / over(group_lane) * over(own_lane) / over(mate_lane)

            for j in range(ff // ff_step):
                cols = slice(j * ff_step, (j + 1) * ff_step)
                x = normed_in[0:count, :]
                g = jnp.dot(x, gate_w[0, :, cols], preferred_element_type=F32)
                u = jnp.dot(x, up_w[0, :, cols], preferred_element_type=F32)
                target[at, cols] = (g / (1.0 + jnp.exp(-g)) * u * weight).astype(BF16)

        def each_block(k, act_on):
            def pair(o, side):
                for c2 in range(2):
                    act_on(2 * o + c2)

            if k == 0:
                pair(z, 0)
            else:
                each_slice(k, pair)

        def wide_cols(q):
            return pl.ds(pl.multiple_of(q * wide, wide), wide)

        def both(kind, at, q):
            acc = jnp.dot(
                h_own[kind, at, :], down_w[0, :, wide_cols(q)], preferred_element_type=F32
            )
            acc = acc + jnp.dot(h_in[kind, at, :], down_x[q], preferred_element_type=F32)
            return acc.astype(BF16)

        def down_b(k, c):
            def block_of(q):
                back_out[q, chunk(c), :] = both(1, chunk(c), q)
                rt_copy(q, c).start()

            with jax.named_scope(f"down{k}{c}"):
                if c == 0:
                    if k == 0:
                        dp_wait(z)
                    else:
                        each_slice(k, lambda o, side: dp_wait(o))
                each_block(k, block_of)

        everyone = pl.ds(0, cap)
        for i, j in enumerate(order):
            with jax.named_scope(f"project{i}"):
                project(i, j)
            if i == 1:
                finish_last()
            if i == 2:
                forward(0, 0, 1)
        for c in range(1, C):
            for j in order[1:]:
                b_copy(j, c).start()
        with jax.named_scope("guA"):
            gate_up(outgoing.at[0], everyone, cap, h_own.at[0])
        forward(0, 1, 3)
        d_step(1, False)
        forward(0, 3, 4)
        with jax.named_scope("guB0"):
            gate_up(arrived.at[1], chunk(0), part, h_own.at[1])
        forward(1, 0, 4)
        d_step(2, True)
        with jax.named_scope("fw0"):
            f_wait(0)
        with jax.named_scope("guF0"):
            gate_up(arrived.at[2], chunk(0), part, h_out.at[1])
        hx_copy(1, 0).start()
        a_copy(order[0], 1).start()
        a_copy(order[1], 1).start()
        with jax.named_scope("guB1"):
            gate_up(arrived.at[1], chunk(1), part, h_own.at[1])
        with jax.named_scope("aw0"):
            a_wait(0)
        with jax.named_scope("guX0"):
            gate_up(arrived.at[0], chunk(0), part, h_out.at[0])
        with jax.named_scope("fw1"):
            f_wait(1)
        with jax.named_scope("guF1"):
            gate_up(arrived.at[2], chunk(1), part, h_out.at[1])
        hx_copy(1, 1).start()
        a_copy(order[2], 1).start()
        a_copy(order[3], 1).start()
        hx_copy(0, 0).start()
        d_step(2, False)
        with jax.named_scope("hw0"):
            hx_copy(1, 0).wait_recv()
        down_b(0, 0)
        down_b(1, 0)
        down_b(2, 0)
        with jax.named_scope("own_down"):
            h_rows[0, :, :] = jnp.dot(
                spread_all[0], h_own[0], preferred_element_type=F32
            ).astype(BF16)
            for q in range(T):
                cols = slice(q * wide, (q + 1) * wide)
                base_out[q, :, :] = hidden[:, cols].astype(F32) + jnp.dot(
                    h_rows[0], down_w[0, :, cols], preferred_element_type=F32
                )
        with jax.named_scope("hw1"):
            hx_copy(1, 1).wait_recv()
        down_b(0, 1)
        down_b(1, 1)
        for k in range(3, Z):
            d_step(k)
        down_b(2, 1)
        with jax.named_scope("aw1"):
            a_wait(1)
        with jax.named_scope("guX1"):
            gate_up(arrived.at[0], chunk(1), part, h_out.at[0])
        hx_copy(0, 1).start()
        for k in range(3, Z):
            for c in range(C):
                down_b(k, c)

        def combine_b(q):
            rt_wait(q)
            base_out[q, :, :] += jnp.dot(
                spread_all[1], back_in[q], preferred_element_type=F32
            )

        def combine_a(q):
            mixed = jnp.dot(h_rows[1], down_x[q], preferred_element_type=F32)
            out_ref[:, wide_cols(q)] = (base_out[q] + mixed).astype(BF16)

        def combine(q):
            combine_b(q)
            combine_a(q)

        ahead = min(2, Z)
        for k in range(ahead):
            with jax.named_scope(f"comb_b{k}"):
                each_block(k, combine_b)
        with jax.named_scope("hwA"):
            for c in range(C):
                hx_copy(0, c).wait_recv()
            h_rows[1, :, :] = jnp.dot(
                spread_all[0], h_in[0], preferred_element_type=F32
            ).astype(BF16)
        for k in range(Z):
            with jax.named_scope(f"combine{k}"):
                each_block(k, combine_a if k < ahead else combine)

        with jax.named_scope("sendwait"):
            dx_copy.wait_send()
            sets = outgoing.at[0:3]
            remote(sets, sets, ex_send.at[0], ex_recv.at[0], nbr_x, t).wait_send()
            remote(h_out, h_out, hx_send.at[0], hx_recv.at[0, 0], nbr_x, t).wait_send()
            remote(back_out, back_out, rt_send.at[0], rt_recv.at[0], nbr_y, t).wait_send()
            ref = down_x.at[0:Z]
            remote(ref, ref, dp_send.at[0], dp_recv.at[0], s, partner).wait_send()

            for zz in range(Z):
                for side, count in ((0, zz + 1), (1, Z - zz)):
                    if count < Z:
                        ref = down_x.at[0:count]

                        @pl.when(z == zz)
                        def _():
                            remote(
                                ref, ref, zd_send.at[side], zd_recv.at[0], s, partner
                            ).wait_send()

    else:
        def disp_copy(expert, j):
            return remote(
                outgoing.at[expert, j],
                arrived.at[s, j],
                disp_send.at[expert, j],
                disp_recv.at[s, j],
                expert,
                t,
            )

        def disp_wait(sender, j):
            remote(
                outgoing.at[sender, j],
                arrived.at[sender, j],
                disp_send.at[sender, j],
                disp_recv.at[sender, j],
                sender,
                t,
            ).wait_recv()

        def ret_copy(sender, j):
            return remote(
                results.at[sender, j],
                returned.at[s, j],
                ret_send.at[sender, j],
                ret_recv.at[s, j],
                sender,
                t,
            )

        def ret_wait(expert, j):
            remote(
                results.at[expert, j],
                returned.at[expert, j],
                ret_send.at[expert, j],
                ret_recv.at[expert, j],
                expert,
                t,
            ).wait_recv()

        def project(j, squares):
            with jax.named_scope("wpwait"):
                p_wait(j)
            cols = piece_cols(j)
            acc = residual[:, cols].astype(F32)
            part = jnp.dot(act[...], wfull[j], preferred_element_type=F32)
            state = (acc + part).astype(BF16)
            hidden[:, cols] = state
            for expert in others:
                outgoing[expert, j, :, :] = jnp.dot(
                    picks[expert], state, preferred_element_type=F32
                ).astype(BF16)
            for expert in prompt:
                disp_copy(expert, j).start()
            arrived[s, j, :, :] = jnp.dot(picks[s], state, preferred_element_type=F32).astype(BF16)
            state = state.astype(F32)
            return squares + jnp.sum(state * state, axis=1, keepdims=True)

        squares = jnp.zeros((rows, 1), F32)
        if square:
            for i, j in enumerate(order):
                with jax.named_scope(f"project{i}"):
                    squares = project(j, squares)
                if i == 0:
                    finish_last()
        else:
            finish_last()
            squares = lax.fori_loop(0, S, project, squares)
        for expert in late:
            for j in order:
                disp_copy(expert, j).start()

        for c in loads[8:]:
            c.wait()

        def expert_block(sender, target, send):
            def square_step(j, squares):
                x = arrived[sender, j].astype(F32)
                return squares + jnp.sum(x * x, axis=1, keepdims=True)

            total = lax.fori_loop(0, S, square_step, jnp.zeros((cap, 1), F32))
            row_scale = lax.rsqrt(total / D + epsilon)

            def norm_step(j, _):
                cols = piece_cols(j)
                x = arrived[sender, j].astype(F32)
                normed_in[:, cols] = (x * row_scale * gain_moe_ref[:, cols]).astype(BF16)
                return 0

            lax.fori_loop(0, S, norm_step, 0)

            def up_step(j, _):
                cols = pl.ds(pl.multiple_of(j * ff_step, ff_step), ff_step)
                x = normed_in[...]
                g = jnp.dot(x, gate_w[0, :, cols], preferred_element_type=F32)
                u = jnp.dot(x, up_w[0, :, cols], preferred_element_type=F32)
                ffn_hidden[:, cols] = (g / (1.0 + jnp.exp(-g)) * u).astype(BF16)
                return 0

            lax.fori_loop(0, ff // ff_step, up_step, 0)

            def down_step(j, _):
                target[j, :, :] = jnp.dot(
                    ffn_hidden[...], down_w[0, :, piece_cols(j)], preferred_element_type=F32
                ).astype(BF16)
                if send:
                    ret_copy(sender, j).start()
                return 0

            lax.fori_loop(0, S, down_step, 0)

        with jax.named_scope("ffnown"):
            expert_block(s, returned.at[s], False)

        scale = lax.rsqrt(squares / D + epsilon)

        def norm_cols(j, _):
            cols = piece_cols(j)
            normed[:, cols] = (hidden[:, cols].astype(F32) * scale * gain_moe_ref[:, cols]).astype(BF16)
            return 0

        def logits(router):
            return lax.dot_general(
                normed[...], router[...], (((1,), (1,)), ((), ())), preferred_element_type=F32
            )

        with jax.named_scope("router"):
            lax.fori_loop(0, S, norm_cols, 0)
            group_exp = jnp.exp(logits(group_router_ref))
            expert_exp = jnp.exp(logits(expert_router_ref))
            group_prob = jnp.sum(
                jnp.where(in_group[:, :G], group_exp, zero), axis=1, keepdims=True
            ) / jnp.sum(group_exp, axis=1, keepdims=True)
            chosen_exp = jnp.where(chosen[:, :E], expert_exp, zero)
            mix = group_prob * chosen_exp / jnp.sum(chosen_exp, axis=1, keepdims=True)
            for e in range(E):
                spreads[e, :, :] = jnp.where(
                    column(slot, e) == slot_iota, column(mix, e), zero
                ).astype(BF16)

        for i, sender in enumerate(others):
            with jax.named_scope(f"dispwait{i}"):
                for j in range(S):
                    disp_wait(sender, j)
            with jax.named_scope(f"ffn{i}"):
                expert_block(sender, results.at[sender], True)

        def combine(j, _):
            cols = piece_cols(j)
            for expert in others:
                ret_wait(expert, j)
            acc = hidden[:, cols].astype(F32)
            for e in range(E):
                acc = acc + jnp.dot(spreads[e], returned[e, j], preferred_element_type=F32)
            out_ref[:, cols] = acc.astype(BF16)
            return 0

        with jax.named_scope("combine"):
            lax.fori_loop(0, S, combine, 0)


        for expert in others:
            for j in range(S):
                disp_copy(expert, j).wait_send()
                ret_copy(expert, j).wait_send()

    with jax.named_scope("sendwait"):
        for zz in range(Z):
            for side, count in ((0, zz + 1), (1, Z - zz)):
                if count < Z:
                    ref = wfull.at[0, pl.ds(0, count * wrows), :]

                    @pl.when(z == zz)
                    def _():
                        remote(
                            ref, ref, wz_send.at[side], wz_recv.at[0, 0], s, partner
                        ).wait_send()

        ref = wfull.at[0 : S - 1, pl.ds(0, (Z - 1) * wrows), :]
        remote(ref, ref, wx_send.at[0], wx_recv.at[0, 0, 0], order[1], t).wait_send()
        ref = wfull.at[:, pl.ds(0, Z * wrows), :]
        remote(ref, ref, wp_send.at[0], wp_recv.at[0], s, partner).wait_send()
        ref = conv_out.at[0 : T - 1]
        remote(ref, ref, a2a_send.at[0], a2a_recv.at[0], s, partner).wait_send()


def body(
    S,
    T,
    conv_value,
    conv_gate,
    doc_ids,
    conv_kernel,
    norm_gain_conv,
    norm_bias_conv,
    proj_weight,
    residual,
    norm_gain_moe,
    group_router,
    expert_router,
    routing,
    expert_gate_w,
    expert_up_w,
    expert_down_w,
):
    tokens, width = conv_value.shape
    rows, D = residual.shape
    wrows = proj_weight.shape[0]
    ff = expert_gate_w.shape[2]
    G = group_router.shape[1]
    E = expert_router.shape[1]
    cap = 2 * rows // E
    hbm = pl.BlockSpec(memory_space=pl.ANY)
    dma = pltpu.SemaphoreType.DMA
    piece = D // S
    Z = T // 2
    paired = S == 4 and E == S and E == 2 * G
    return pl.pallas_call(
        functools.partial(kernel, S, T, G),
        out_shape=pltpu.VMEM((rows, D), BF16),
        in_specs=[hbm] * 15,
        out_specs=pl.BlockSpec(memory_space=pltpu.VMEM),
        scratch_shapes=[
            pltpu.VMEM((1, tokens), jnp.int32),
            pltpu.VMEM(conv_kernel.shape, BF16),
            pltpu.VMEM((1, T * width), F32),
            pltpu.VMEM((1, T * width), F32),
            pltpu.VMEM((1, D), F32),
            pltpu.VMEM((G, D), BF16),
            pltpu.VMEM((E, D), BF16),
            pltpu.VMEM((2, rows), jnp.int32),
            pltpu.VMEM((tokens, width), BF16),
            pltpu.VMEM((tokens, width), BF16),
            pltpu.VMEM((S, T * wrows, piece), BF16),
            pltpu.VMEM((rows, D), BF16),
            pltpu.VMEM((1, D, ff), BF16),
            pltpu.VMEM((1, D, ff), BF16),
            pltpu.VMEM((1, ff, D), BF16),
            pltpu.VMEM((HALO + 16, width), BF16),
            pltpu.VMEM((HALO + 16, width), BF16),
            pltpu.VMEM((tokens + HALO, width), F32),
            pltpu.VMEM((32, width), F32),
            pltpu.VMEM((tokens, 128), F32),
            pltpu.VMEM((T, rows, width), BF16),
            pltpu.VMEM((T, rows, width), BF16),
            pltpu.VMEM((rows, T * width), BF16),
            pltpu.VMEM((rows, D), BF16),
            pltpu.VMEM((rows, D), BF16),
            pltpu.VMEM((cap, D), BF16),
            pltpu.VMEM((E, cap, rows), BF16),
            pltpu.VMEM((E, rows, cap), BF16),
            pltpu.VMEM((E, S, cap, piece), BF16),
            pltpu.VMEM((E, S, cap, piece), BF16),
            pltpu.VMEM((cap, ff), BF16),
            pltpu.VMEM((E, S, cap, piece), BF16),
            pltpu.VMEM((E, S, cap, piece), BF16),
            pltpu.VMEM((G + E + (-G - E) % 8, D), BF16),
            pltpu.VMEM((ff, D // T), BF16),
            pltpu.VMEM((T, ff, D // T), BF16),
            pltpu.VMEM((2, cap, ff), BF16),
            pltpu.VMEM((2, cap, ff), BF16),
            pltpu.VMEM((2, cap, ff), BF16),
            pltpu.VMEM((T, cap, D // T), BF16),
            pltpu.VMEM((T, cap, D // T), BF16),
            pltpu.VMEM((2, rows, ff), BF16),
            pltpu.VMEM((2, rows, cap), BF16),
            pltpu.VMEM((T, rows, D // T), F32),
            dma((15,)),
            dma((S,)),
            dma((2,)),
            dma((2,)),
            dma((Z, 2)),
            dma((1,)),
            dma((S - 1, Z, 2)),
            dma((1,)),
            dma((S,)),
            dma((1,)),
            dma((1,)),
            dma((1, 1) if paired else (S, S)),
            dma((1, 1) if paired else (S, S)),
            dma((1, 1) if paired else (S, S)),
            dma((1, 1) if paired else (S, S)),
            dma((1,)),
            dma((CHUNKS * (S + 2),)),
            dma((1,)),
            dma((2, CHUNKS)),
            dma((1,)),
            dma((T,)),
            dma((2,)),
            dma((Z,)),
            dma((1,)),
            dma((Z,)),
            dma((2,)),
        ],
        compiler_params=pltpu.CompilerParams(
            collective_id=0, has_side_effects=True, vmem_limit_bytes=60 * 1024 * 1024
        ),
    )(
        conv_value,
        conv_gate,
        doc_ids[None, :],
        conv_kernel,
        norm_gain_conv[None, :],
        norm_bias_conv[None, :],
        proj_weight,
        residual,
        norm_gain_moe[None, :],
        group_router.T,
        expert_router.T,
        routing.T,
        expert_gate_w,
        expert_up_w,
        expert_down_w,
    )


def solution(mesh):
    placed = (
        P("sp", "tp"),
        P("sp", "tp"),
        P("sp"),
        P(None, "tp"),
        P(),
        P(),
        P("tp", None),
        P(("sp", "tp"), None),
        P(),
        P(),
        P(),
        P(("sp", "tp"), None),
        P("sp", None, None),
        P("sp", None, None),
        P("sp", None, None),
    )
    return jax.shard_map(
        functools.partial(body, mesh.shape["sp"], mesh.shape["tp"]),
        mesh=mesh,
        in_specs=placed,
        out_specs=P(("sp", "tp"), None),
        check_vma=False,
    )
```

```python
import functools

import jax
import jax.numpy as jnp
from jax import lax
from jax.experimental import pallas as pl
from jax.experimental.pallas import tpu as pltpu
from jax.sharding import PartitionSpec as P

epsilon = 1e-06
MESH = pl.DeviceIdType.MESH
F32 = jnp.float32
BF16 = jnp.bfloat16
HALO = 32
CHUNKS = 2


def gate(value, gate_value):
    return (value.astype(F32) * jax.nn.sigmoid(gate_value.astype(F32))).astype(BF16)


def kernel(
    S,
    T,
    G,
    value_hbm,
    gate_hbm,
    ids_hbm,
    kernel_hbm,
    gain_conv_hbm,
    bias_conv_hbm,
    weight_hbm,
    residual_hbm,
    gain_moe_hbm,
    group_router_hbm,
    expert_router_hbm,
    routing_hbm,
    gate_w_hbm,
    up_w_hbm,
    down_w_hbm,
    out_ref,
    ids_row_ref,
    kernel_ref,
    gain_conv_ref,
    bias_conv_ref,
    gain_moe_ref,
    group_router_ref,
    expert_router_ref,
    routing_ref,
    value,
    gates,
    wfull,
    residual,
    gate_w,
    up_w,
    down_w,
    rim_out,
    rim_in,
    padded,
    taps,
    least_tap,
    conv_out,
    conv_in,
    act,
    hidden,
    normed,
    normed_in,
    picks,
    spreads,
    outgoing,
    arrived,
    ffn_hidden,
    results,
    returned,
    router_all,
    down_stage,
    down_x,
    h_own,
    h_out,
    h_in,
    back_out,
    back_in,
    h_rows,
    spread_all,
    base_out,
    local_sem,
    wl_sem,
    rim_sem,
    wz_send,
    wz_recv,
    wx_send,
    wx_recv,
    wp_send,
    wp_recv,
    a2a_send,
    a2a_recv,
    disp_send,
    disp_recv,
    ret_send,
    ret_recv,
    ex_send,
    ex_recv,
    hx_send,
    hx_recv,
    rt_send,
    rt_recv,
    zd_send,
    zd_recv,
    dp_send,
    dp_recv,
    dx_sem,
):
    s = lax.axis_index("sp")
    t = lax.axis_index("tp")
    Z = T // 2
    z = t // 2
    core = t % 2
    partner = 2 * z + 1 - core
    tokens, width = value.shape
    block = tokens // T
    n_taps = kernel_ref.shape[0]
    piece = wfull.shape[2]
    wrows = wfull.shape[1] // T
    D = S * piece
    square = S == 4
    E = S
    paired = square and expert_router_ref.shape[0] == S and E == 2 * G
    wide = D // T
    H = 2
    part_rows = wrows // H

    def remote(src, dst, send, recv, sp_to, tp_to):
        return pltpu.make_async_remote_copy(
            src_ref=src,
            dst_ref=dst,
            send_sem=send,
            recv_sem=recv,
            device_id=(sp_to, tp_to),
            device_id_type=MESH,
        )

    barrier = pltpu.get_barrier_semaphore()
    for k in range(1, T):
        pl.semaphore_signal(
            barrier, inc=1, device_id=(s, lax.rem(t + k, T)), device_id_type=MESH
        )
    for k in range(1, S):
        pl.semaphore_signal(
            barrier, inc=1, device_id=(lax.rem(s + k, S), t), device_id_type=MESH
        )

    loads = [
        pltpu.make_async_copy(a, b, local_sem.at[i])
        for i, (a, b) in enumerate(
            [
                (ids_hbm, ids_row_ref),
                (value_hbm, value),
                (gate_hbm, gates),
                (kernel_hbm, kernel_ref),
                (routing_hbm, routing_ref),
                (gain_conv_hbm, gain_conv_ref),
                (bias_conv_hbm, bias_conv_ref),
                (residual_hbm, residual),
                (gain_moe_hbm, gain_moe_ref),
                (group_router_hbm, group_router_ref),
                (expert_router_hbm, expert_router_ref),
                (gate_w_hbm, gate_w),
                (up_w_hbm, up_w),
                (down_w_hbm, down_w),
            ]
        )
    ]
    nbr_x = s + 1 - 2 * (s % 2)
    nbr_y = s + 2 - 4 * (s // 2)
    diag = 3 - s
    order = [s, nbr_x, nbr_y, diag] if square else [lax.rem(s + S - j, S) for j in range(S)]
    own_rows = pl.ds(pl.multiple_of(t * wrows, wrows), wrows)
    own_w = [
        pltpu.make_async_copy(
            weight_hbm.at[:, pl.ds(pl.multiple_of(j * piece, piece), piece)],
            wfull.at[j, own_rows, :],
            wl_sem.at[i],
        )
        for i, j in enumerate(order)
    ]
    stage = pltpu.make_async_copy(
        down_w_hbm.at[0, :, pl.ds(pl.multiple_of(t * wide, wide), wide)],
        down_stage,
        local_sem.at[14],
    )
    loads[0].start()
    own_w[0].start()
    if paired:
        stage.start()
    for c in loads[1:4]:
        c.start()

    with jax.named_scope("barrier"):
        pl.semaphore_wait(barrier, T + S - 2)

    def w_ref(o, p, h):
        base = pl.multiple_of((2 * o + core) * wrows + h * part_rows, part_rows)
        return wfull.at[p, pl.ds(base, part_rows), :]

    def z_copy(o, h, up, to):
        ref = w_ref(o, s, h)
        return remote(ref, ref, wz_send.at[up], wz_recv.at[o, h], s, 2 * to + core)

    def x_copy(o, p, h, role, to):
        ref = w_ref(o, p, h)
        return remote(ref, ref, wx_send.at[0], wx_recv.at[role, o, h], to, t)

    def p_copy(o, p):
        rows_at = pl.ds(pl.multiple_of((2 * o + core) * wrows, wrows), wrows)
        ref = wfull.at[p, rows_at, :]
        return remote(ref, ref, wp_send.at[0], wp_recv.at[p], s, partner)

    def p_wait(p):
        ref = wfull.at[p, pl.ds(0, Z * wrows), :]
        remote(ref, ref, wp_send.at[0], wp_recv.at[p], s, partner).wait_recv()

    has_up = z + 1 < Z
    has_down = z > 0
    own_w[0].wait()
    for h in range(H):

        @pl.when(has_up)
        def _():
            z_copy(z, h, 0, z + 1).start()

        @pl.when(has_down)
        def _():
            z_copy(z, h, 1, z - 1).start()

    for c in own_w[1:]:
        c.start()
    for c in loads[4:]:
        c.start()
    dx_copy = remote(down_stage, down_x.at[t], dx_sem.at[0], dx_sem.at[1], nbr_x, t)
    if paired:
        stage.wait()
        dx_copy.start()
    p_copy(z, s).start()

    def sides(k):
        return ((z - k, z - k >= 0, 0), (z + k, z + k < Z, 1))

    def each_slice(k, act_on):
        for o, there, side in sides(k):
            pl.when(there)(functools.partial(act_on, o, side))

    def z_step(k, h):
        def one(o, side):
            z_copy(o, h, side, z).wait_recv()
            beyond = has_down if side else has_up

            @pl.when(beyond)
            def _():
                z_copy(o, h, side, z - 1 if side else z + 1).start()

            if square:
                x_copy(o, s, h, 0, nbr_x).start()
                x_copy(o, s, h, 1, nbr_y).start()
            else:
                for j in range(1, S):
                    x_copy(o, s, h, j - 1, lax.rem(s + j, S)).start()
            if h == H - 1:
                p_copy(o, s).start()

        with jax.named_scope(f"z{k}{h}"):
            each_slice(k, one)

    def x_step(k):
        def one(o, side):
            x_copy(o, nbr_x, 0, 0, nbr_y).wait_recv()
            x_copy(o, nbr_x, 0, 2, nbr_y).start()

        if square:
            with jax.named_scope(f"x{k}"):
                each_slice(k, one)

    def y_step(k):
        def one(o, side):
            x_copy(o, nbr_y, 1, 1, nbr_x).wait_recv()
            x_copy(o, nbr_y, 1, 2, nbr_x).start()

        if square:
            with jax.named_scope(f"y{k}"):
                each_slice(k, one)

    def zd_copy(o, side, to):
        ref = down_x.at[2 * o + core]
        return remote(ref, ref, zd_send.at[side], zd_recv.at[o], s, 2 * to + core)

    def dp_copy(o):
        ref = down_x.at[2 * o + core]
        return remote(ref, ref, dp_send.at[0], dp_recv.at[o], s, partner)

    def dp_wait(o):
        ref = down_x.at[2 * o + 1 - core]
        remote(ref, ref, dp_send.at[0], dp_recv.at[o], s, partner).wait_recv()

    def at_edge(o):
        return (o == 0) | (o == Z - 1)

    def d_start(edges):
        if edges:
            dx_copy.wait_recv()
            dp_copy(z).start()
        mine = at_edge(z) if edges else jnp.logical_not(at_edge(z))

        @pl.when(mine & has_up)
        def _():
            zd_copy(z, 0, z + 1).start()

        @pl.when(mine & has_down)
        def _():
            zd_copy(z, 1, z - 1).start()

    def d_step(k, edges=None):
        def one(o, side):
            zd_copy(o, side, z).wait_recv()

            @pl.when(has_down if side else has_up)
            def _():
                zd_copy(o, side, z - 1 if side else z + 1).start()

            dp_copy(o).start()

        def some(o, side):
            pl.when(at_edge(o) if edges else jnp.logical_not(at_edge(o)))(
                functools.partial(one, o, side)
            )

        with jax.named_scope(f"d{k}"):
            each_slice(k, one if edges is None else some)

    def finish_row(k, parts):
        def one(o, side):
            for i in parts:
                p = order[i]
                if square:
                    for h in ((1,), (0,), (0, 1))[i - 1]:
                        x_copy(o, p, h, i - 1, p).wait_recv()
                else:
                    for h in range(H):
                        x_copy(o, p, h, i - 1, p).wait_recv()
                p_copy(o, p).start()

        with jax.named_scope(f"fin{k}{parts[0]}"):
            each_slice(k, one)

    loads[0].wait()
    ids_row = jnp.broadcast_to(ids_row_ref[...], (8, tokens))
    position = lax.broadcasted_iota(jnp.int32, (8, tokens), 1)
    low = jnp.int32(-n_taps)
    fresh = (ids_row != pltpu.roll(ids_row, 1, 1)) & (position > 0)
    begin = jnp.where(fresh, position, low)
    shift = 1
    while shift < n_taps:
        moved = jnp.where(position >= shift, pltpu.roll(begin, shift, 1), low)
        begin = jnp.maximum(begin, moved)
        shift *= 2
    least_row = (n_taps - 1 - position + begin).astype(F32)
    lanes = least_tap.shape[1]
    for c in range(tokens // lanes):
        across = jnp.broadcast_to(least_row[0:1, c * lanes : (c + 1) * lanes], (lanes, lanes))
        least_tap[c * lanes : (c + 1) * lanes, :] = across.T

    for c in loads[1:4]:
        c.wait()
    tail = pl.ds(tokens - HALO, HALO)
    last_reach = jnp.max(least_tap[tokens - 1 : tokens, :], axis=1, keepdims=True)
    row_at = lax.broadcasted_iota(jnp.int32, (HALO, width), 0).astype(F32)
    newer = row_at >= last_reach + (HALO - n_taps)
    rim = jnp.where(newer, gate(value[tail, :], gates[tail, :]).astype(F32), jnp.float32(0.0))
    rim_out[0:HALO, :] = rim.astype(BF16)
    last_id = ids_row_ref[0:1, tokens - 1 : tokens].astype(F32)
    rim_out[HALO : HALO + 16, :] = jnp.broadcast_to(last_id, (16, width)).astype(BF16)
    rim_copy = remote(
        rim_out, rim_in, rim_sem.at[0], rim_sem.at[1], lax.rem(s + 1, S), t
    )
    rim_copy.start()

    def gate_rows(i, _):
        rows = pl.ds(pl.multiple_of(i * 64, 64), 64)
        to_rows = pl.ds(pl.multiple_of(HALO + i * 64, 32), 64)
        padded[to_rows, :] = gate(value[rows, :], gates[rows, :]).astype(F32)
        return 0

    with jax.named_scope("gate"):
        lax.fori_loop(0, tokens // 64, gate_rows, 0)
    taps[0:n_taps, :] = kernel_ref[...].astype(F32)

    step_rows = 32 if block % 32 == 0 else 8
    lanes = min(width, 128)

    def conv_block(owner):
        def conv_rows(i, _):
            base = pl.multiple_of(owner * block + i * step_rows, 8)
            least = least_tap[pl.ds(base, step_rows), :]
            window = padded[pl.ds(base, step_rows + HALO), :]
            total = jnp.zeros((step_rows, width), F32)
            for tap in range(n_taps):
                at = tap + HALO + 1 - n_taps
                valid = least <= tap
                product = window[at : at + step_rows, :] * taps[tap : tap + 1, :]
                parts = [
                    jnp.where(valid, product[:, j : j + lanes], jnp.float32(0.0))
                    for j in range(0, width, lanes)
                ]
                total = total + jnp.concatenate(parts, axis=1)
            conv_out[
                owner, pl.ds(pl.multiple_of(i * step_rows, step_rows), step_rows), :
            ] = total.astype(BF16)
            return 0

        lax.fori_loop(0, block // step_rows, conv_rows, 0)

    def conv_some(first, last):
        with jax.named_scope("conv"):

            def one(owner, _):
                conv_block(owner)
                return 0

            lax.fori_loop(first, last, one, 0)

    def conv_copy(to):
        return remote(
            conv_out.at[to], conv_in.at[t], a2a_send.at[0], a2a_recv.at[0], s, to
        )

    def conv_flush(inner):
        if not inner:
            conv_copy(partner).start()
        for far in range(1, Z):
            for to, there, _ in sides(far):
                middle = (to > 0) & (to < Z - 1)

                @pl.when(there & (middle if inner else jnp.logical_not(middle)))
                def _():
                    for c in range(2):
                        conv_copy(2 * to + c).start()

    marks = [1 + (T - 2) * i // 6 for i in (1, 2, 4, 6)]
    conv_some(1, marks[0])
    for i in range(1, S):
        own_w[i].wait()
        p_copy(z, order[i]).start()
    conv_some(marks[0], marks[1])
    z_step(1, 0)
    conv_some(marks[1], marks[2])
    z_step(1, 1)
    conv_some(marks[2], marks[3])
    z_step(2, 0)
    conv_flush(True)
    conv_some(marks[3], T)
    with jax.named_scope("rimwait"):
        rim_copy.wait()
    same = (rim_in[HALO : HALO + 1, :].astype(F32) == ids_row_ref[0:1, 0:1].astype(F32)) & (s > 0)
    padded[0:HALO, :] = jnp.where(same, rim_in[0:HALO, :].astype(F32), jnp.float32(0.0))
    conv_some(0, 1)
    x_step(1)
    z_step(2, 1)
    conv_flush(False)
    if paired:
        d_start(True)
    y_step(1)
    conv_in[t, :, :] = conv_out[t, :, :]

    rows = block
    for c in loads[4:7]:
        c.wait()
    cap = 2 * rows // E
    lane = lax.broadcasted_iota(jnp.int32, (rows, 128), 1)
    eye = lax.broadcasted_iota(jnp.int32, (rows, rows), 0) == lax.broadcasted_iota(
        jnp.int32, (rows, rows), 1
    )
    named = lax.dot_general(
        eye.astype(F32).astype(BF16),
        routing_ref[...].astype(F32).astype(BF16),
        (((1,), (1,)), ((), ())),
        preferred_element_type=F32,
    )
    first = named[:, 0:1]
    second = named[:, 1:2]
    lane_f = lane.astype(F32)
    chosen = (lane_f == first) | (lane_f == second)
    per_group = E // G
    group_low = lane_f * per_group
    in_group = (first >= group_low) & (first < group_low + per_group)
    row_i = lax.broadcasted_iota(jnp.int32, (rows, rows), 0)
    col_i = lax.broadcasted_iota(jnp.int32, (rows, rows), 1)
    before = jnp.dot(
        (row_i > col_i).astype(F32).astype(BF16),
        chosen.astype(F32).astype(BF16),
        preferred_element_type=F32,
    )
    slot = jnp.where(chosen, before, jnp.float32(-1.0))
    width_e = max(E, 8)
    expert_i = lax.broadcasted_iota(jnp.int32, (width_e, rows), 0)
    chosen_r = (routing_ref[0:1, :] == expert_i) | (routing_ref[1:2, :] == expert_i)
    before_r = jnp.dot(
        chosen_r.astype(F32).astype(BF16),
        (row_i < col_i).astype(F32).astype(BF16),
        preferred_element_type=F32,
    )
    slot_r = jnp.where(chosen_r, before_r, jnp.float32(-1.0))
    cap_i = lax.broadcasted_iota(jnp.int32, (cap, rows), 0).astype(F32)
    for e in range(E):
        picks[e, :, :] = (slot_r[e : e + 1, :] == cap_i).astype(F32).astype(BF16)

    def piece_cols(j):
        return pl.ds(pl.multiple_of(j * piece, piece), piece)

    def finish_last():
        for k in (Z - 2, Z - 1):
            finish_row(k, all_parts[-1:])

    def column(array, expert):
        mine = lane[:, : array.shape[1]] == expert
        return jnp.sum(jnp.where(mine, array, jnp.float32(0.0)), axis=1, keepdims=True)

    zero = jnp.float32(0.0)
    slot_iota = lax.broadcasted_iota(jnp.int32, (rows, cap), 1).astype(F32)
    ff = gate_w.shape[2]
    ff_step = min(ff, 512)


    if paired:
        for c in loads[8:]:
            c.wait()
        blank = jnp.zeros((router_all.shape[0] - G - E, D), F32)
        router_all[...] = jnp.concatenate(
            [group_router_ref[...].astype(F32), expert_router_ref[...].astype(F32), blank], axis=0
        ).astype(BF16)
        for e, at in enumerate((s, nbr_y)):
            spread_all[e, :, :] = jnp.where(
                column(slot, at) == slot_iota, jnp.float32(1.0), zero
            ).astype(BF16)
    all_parts = tuple(range(1, S))
    for k in range(3, Z):
        z_step(k, 0)
        x_step(k - 1)
        z_step(k, 1)
        finish_row(k - 2, all_parts)
        y_step(k - 1)
    finish_row(Z - 2, all_parts[:-1])
    x_step(Z - 1)
    y_step(Z - 1)
    finish_row(Z - 1, all_parts[:-1])

    with jax.named_scope("a2await"):
        ref = conv_in.at[0 : T - 1]
        remote(ref, ref, a2a_send.at[0], a2a_recv.at[0], s, partner).wait_recv()
    if paired:
        with jax.named_scope("d0"):
            d_start(False)
            d_step(1, True)
    with jax.named_scope("act"):
        total = jnp.zeros((rows, 1), F32)
        for j in range(T):
            total = total + jnp.sum(conv_in[j].astype(F32), axis=1, keepdims=True)
        average = total / (T * width)
        total = jnp.zeros((rows, 1), F32)
        for j in range(T):
            centered = conv_in[j].astype(F32) - average
            total = total + jnp.sum(centered * centered, axis=1, keepdims=True)
        scale = lax.rsqrt(total / (T * width) + epsilon)
        for j in range(T):
            cols = slice(j * width, (j + 1) * width)
            v = (conv_in[j].astype(F32) - average) * scale * gain_conv_ref[
                :, cols
            ] + bias_conv_ref[:, cols]
            act[:, cols] = (v / (1.0 + jnp.exp(-v))).astype(BF16)

    loads[7].wait()

    others = order[1:]
    prompt = others[:2] if square else others
    late = others[2:] if square else []

    if paired:
        C = CHUNKS
        part = cap // C
        mates = (s, nbr_x)

        def chunk(c):
            return pl.ds(c * part, part)

        def a_copy(j, c):
            return remote(
                outgoing.at[0, j, chunk(c), :],
                arrived.at[0, j, chunk(c), :],
                ex_send.at[0],
                ex_recv.at[C * (S + 1) + c],
                nbr_x,
                t,
            )

        def b_copy(j, c):
            return remote(
                outgoing.at[1, j, chunk(c), :],
                arrived.at[1, j, chunk(c), :],
                ex_send.at[0],
                ex_recv.at[c * S + j],
                nbr_y,
                t,
            )

        def f_copy(j, c):
            return remote(
                arrived.at[1, j, chunk(c), :],
                arrived.at[2, j, chunk(c), :],
                ex_send.at[0],
                ex_recv.at[C * S + c],
                nbr_x,
                t,
            )

        def hx_copy(kind, c):
            at = chunk(c)
            return remote(
                h_out.at[kind, at, :],
                h_in.at[kind, at, :],
                hx_send.at[0],
                hx_recv.at[kind, c],
                nbr_x,
                t,
            )

        def rt_copy(q, c):
            return remote(
                back_out.at[q, chunk(c), :],
                back_in.at[q, chunk(c), :],
                rt_send.at[0],
                rt_recv.at[q],
                nbr_y,
                t,
            )

        def a_wait(c):
            ref = arrived.at[0, :, chunk(c), :]
            remote(ref, ref, ex_send.at[0], ex_recv.at[C * (S + 1) + c], nbr_x, t).wait_recv()

        def f_wait(c):
            ref = arrived.at[2, :, chunk(c), :]
            remote(ref, ref, ex_send.at[0], ex_recv.at[C * S + c], nbr_x, t).wait_recv()

        def rt_wait(q):
            ref = back_in.at[q]
            remote(ref, ref, rt_send.at[0], rt_recv.at[q], nbr_y, t).wait_recv()

        y_order = [nbr_y, diag, s, nbr_x]

        def project(i, j):
            with jax.named_scope("wpwait"):
                p_wait(j)
            cols = piece_cols(j)
            acc = residual[:, cols].astype(F32)
            acc = acc + jnp.dot(act[...], wfull[j], preferred_element_type=F32)
            state = acc.astype(BF16)
            hidden[:, cols] = state
            outgoing[1, j, :, :] = jnp.dot(
                picks[nbr_y], state, preferred_element_type=F32
            ).astype(BF16)
            b_copy(j, 0).start()
            if i == 0:
                for c in range(1, C):
                    b_copy(j, c).start()
            outgoing[0, j, :, :] = jnp.dot(
                picks[s], state, preferred_element_type=F32
            ).astype(BF16)
            a_copy(j, 0).start()

        def forward(c, first, last):
            with jax.named_scope(f"fwd{c}{first}"):
                for j in y_order[first:last]:
                    b_copy(j, c).wait_recv()
                    f_copy(j, c).start()

        router_lane = lax.broadcasted_iota(jnp.int32, (1, router_all.shape[0]), 1)
        group_lane = router_lane < G
        own_group_lane = router_lane == s // 2
        own_lane = router_lane == s + G
        mate_lane = (router_lane == s + G) | (router_lane == nbr_x + G)

        def gate_up(source, at, count, target):
            total = jnp.zeros((count, 1), F32)
            for j in range(S):
                x = source[j, at, :].astype(F32)
                total = total + jnp.sum(x * x, axis=1, keepdims=True)
            row_scale = lax.rsqrt(total / D + epsilon)
            for j in range(S):
                cols = slice(j * piece, (j + 1) * piece)
                x = source[j, at, :].astype(F32)
                normed_in[0:count, cols] = (x * row_scale * gain_moe_ref[:, cols]).astype(BF16)
            logits = lax.dot_general(
                normed_in[0:count, :],
                router_all[...],
                (((1,), (1,)), ((), ())),
                preferred_element_type=F32,
            )
            exps = jnp.exp(logits)

            def over(mask):
                return jnp.sum(jnp.where(mask, exps, zero), axis=1, keepdims=True)

            weight = over(own_group_lane) / over(group_lane) * over(own_lane) / over(mate_lane)

            for j in range(ff // ff_step):
                cols = slice(j * ff_step, (j + 1) * ff_step)
                x = normed_in[0:count, :]
                g = jnp.dot(x, gate_w[0, :, cols], preferred_element_type=F32)
                u = jnp.dot(x, up_w[0, :, cols], preferred_element_type=F32)
                target[at, cols] = (g / (1.0 + jnp.exp(-g)) * u * weight).astype(BF16)

        def each_block(k, act_on):
            def pair(o, side):
                for c2 in range(2):
                    act_on(2 * o + c2)

            if k == 0:
                pair(z, 0)
            else:
                each_slice(k, pair)

        def wide_cols(q):
            return pl.ds(pl.multiple_of(q * wide, wide), wide)

        def both(kind, at, q):
            acc = jnp.dot(
                h_own[kind, at, :], down_w[0, :, wide_cols(q)], preferred_element_type=F32
            )
            acc = acc + jnp.dot(h_in[kind, at, :], down_x[q], preferred_element_type=F32)
            return acc.astype(BF16)

        def down_b(k, c):
            def block_of(q):
                back_out[q, chunk(c), :] = both(1, chunk(c), q)
                rt_copy(q, c).start()

            with jax.named_scope(f"down{k}{c}"):
                if c == 0:
                    if k == 0:
                        dp_wait(z)
                    else:
                        each_slice(k, lambda o, side: dp_wait(o))
                each_block(k, block_of)

        everyone = pl.ds(0, cap)
        for i, j in enumerate(order):
            with jax.named_scope(f"project{i}"):
                project(i, j)
            if i == 1:
                finish_last()
            if i == 2:
                forward(0, 0, 1)
        for c in range(1, C):
            for j in order[1:]:
                b_copy(j, c).start()
        with jax.named_scope("guA"):
            gate_up(outgoing.at[0], everyone, cap, h_own.at[0])
        forward(0, 1, 3)
        d_step(1, False)
        forward(0, 3, 4)
        with jax.named_scope("guB0"):
            gate_up(arrived.at[1], chunk(0), part, h_own.at[1])
        forward(1, 0, 4)
        d_step(2, True)
        with jax.named_scope("fw0"):
            f_wait(0)
        with jax.named_scope("guF0"):
            gate_up(arrived.at[2], chunk(0), part, h_out.at[1])
        hx_copy(1, 0).start()
        a_copy(order[0], 1).start()
        a_copy(order[1], 1).start()
        with jax.named_scope("guB1"):
            gate_up(arrived.at[1], chunk(1), part, h_own.at[1])
        with jax.named_scope("aw0"):
            a_wait(0)
        with jax.named_scope("guX0"):
            gate_up(arrived.at[0], chunk(0), part, h_out.at[0])
        with jax.named_scope("fw1"):
            f_wait(1)
        with jax.named_scope("guF1"):
            gate_up(arrived.at[2], chunk(1), part, h_out.at[1])
        hx_copy(1, 1).start()
        a_copy(order[2], 1).start()
        a_copy(order[3], 1).start()
        hx_copy(0, 0).start()
        d_step(2, False)
        with jax.named_scope("hw0"):
            hx_copy(1, 0).wait_recv()
        down_b(0, 0)
        down_b(1, 0)
        down_b(2, 0)
        with jax.named_scope("own_down"):
            h_rows[0, :, :] = jnp.dot(
                spread_all[0], h_own[0], preferred_element_type=F32
            ).astype(BF16)
            for q in range(T):
                cols = slice(q * wide, (q + 1) * wide)
                base_out[q, :, :] = hidden[:, cols].astype(F32) + jnp.dot(
                    h_rows[0], down_w[0, :, cols], preferred_element_type=F32
                )
        for k in range(3, Z):
            d_step(k)
        with jax.named_scope("hw1"):
            hx_copy(1, 1).wait_recv()
        down_b(0, 1)
        down_b(1, 1)
        down_b(2, 1)
        with jax.named_scope("aw1"):
            a_wait(1)
        with jax.named_scope("guX1"):
            gate_up(arrived.at[0], chunk(1), part, h_out.at[0])
        hx_copy(0, 1).start()
        for k in range(3, Z):
            for c in range(C):
                down_b(k, c)

        def combine_b(q):
            rt_wait(q)
            base_out[q, :, :] += jnp.dot(
                spread_all[1], back_in[q], preferred_element_type=F32
            )

        def combine_a(q):
            mixed = jnp.dot(h_rows[1], down_x[q], preferred_element_type=F32)
            out_ref[:, wide_cols(q)] = (base_out[q] + mixed).astype(BF16)

        def combine(q):
            combine_b(q)
            combine_a(q)

        ahead = min(3, Z)
        for k in range(ahead):
            with jax.named_scope(f"comb_b{k}"):
                each_block(k, combine_b)
        with jax.named_scope("hwA"):
            for c in range(C):
                hx_copy(0, c).wait_recv()
            h_rows[1, :, :] = jnp.dot(
                spread_all[0], h_in[0], preferred_element_type=F32
            ).astype(BF16)
        for k in range(Z):
            with jax.named_scope(f"combine{k}"):
                each_block(k, combine_a if k < ahead else combine)

        with jax.named_scope("sendwait"):
            dx_copy.wait_send()
            sets = outgoing.at[0:3]
            remote(sets, sets, ex_send.at[0], ex_recv.at[0], nbr_x, t).wait_send()
            remote(h_out, h_out, hx_send.at[0], hx_recv.at[0, 0], nbr_x, t).wait_send()
            remote(back_out, back_out, rt_send.at[0], rt_recv.at[0], nbr_y, t).wait_send()
            ref = down_x.at[0:Z]
            remote(ref, ref, dp_send.at[0], dp_recv.at[0], s, partner).wait_send()

            for zz in range(Z):
                for side, count in ((0, zz + 1), (1, Z - zz)):
                    if count < Z:
                        ref = down_x.at[0:count]

                        @pl.when(z == zz)
                        def _():
                            remote(
                                ref, ref, zd_send.at[side], zd_recv.at[0], s, partner
                            ).wait_send()

    else:
        def disp_copy(expert, j):
            return remote(
                outgoing.at[expert, j],
                arrived.at[s, j],
                disp_send.at[expert, j],
                disp_recv.at[s, j],
                expert,
                t,
            )

        def disp_wait(sender, j):
            remote(
                outgoing.at[sender, j],
                arrived.at[sender, j],
                disp_send.at[sender, j],
                disp_recv.at[sender, j],
                sender,
                t,
            ).wait_recv()

        def ret_copy(sender, j):
            return remote(
                results.at[sender, j],
                returned.at[s, j],
                ret_send.at[sender, j],
                ret_recv.at[s, j],
                sender,
                t,
            )

        def ret_wait(expert, j):
            remote(
                results.at[expert, j],
                returned.at[expert, j],
                ret_send.at[expert, j],
                ret_recv.at[expert, j],
                expert,
                t,
            ).wait_recv()

        def project(j, squares):
            with jax.named_scope("wpwait"):
                p_wait(j)
            cols = piece_cols(j)
            acc = residual[:, cols].astype(F32)
            part = jnp.dot(act[...], wfull[j], preferred_element_type=F32)
            state = (acc + part).astype(BF16)
            hidden[:, cols] = state
            for expert in others:
                outgoing[expert, j, :, :] = jnp.dot(
                    picks[expert], state, preferred_element_type=F32
                ).astype(BF16)
            for expert in prompt:
                disp_copy(expert, j).start()
            arrived[s, j, :, :] = jnp.dot(picks[s], state, preferred_element_type=F32).astype(BF16)
            state = state.astype(F32)
            return squares + jnp.sum(state * state, axis=1, keepdims=True)

        squares = jnp.zeros((rows, 1), F32)
        if square:
            for i, j in enumerate(order):
                with jax.named_scope(f"project{i}"):
                    squares = project(j, squares)
                if i == 0:
                    finish_last()
        else:
            finish_last()
            squares = lax.fori_loop(0, S, project, squares)
        for expert in late:
            for j in order:
                disp_copy(expert, j).start()

        for c in loads[8:]:
            c.wait()

        def expert_block(sender, target, send):
            def square_step(j, squares):
                x = arrived[sender, j].astype(F32)
                return squares + jnp.sum(x * x, axis=1, keepdims=True)

            total = lax.fori_loop(0, S, square_step, jnp.zeros((cap, 1), F32))
            row_scale = lax.rsqrt(total / D + epsilon)

            def norm_step(j, _):
                cols = piece_cols(j)
                x = arrived[sender, j].astype(F32)
                normed_in[:, cols] = (x * row_scale * gain_moe_ref[:, cols]).astype(BF16)
                return 0

            lax.fori_loop(0, S, norm_step, 0)

            def up_step(j, _):
                cols = pl.ds(pl.multiple_of(j * ff_step, ff_step), ff_step)
                x = normed_in[...]
                g = jnp.dot(x, gate_w[0, :, cols], preferred_element_type=F32)
                u = jnp.dot(x, up_w[0, :, cols], preferred_element_type=F32)
                ffn_hidden[:, cols] = (g / (1.0 + jnp.exp(-g)) * u).astype(BF16)
                return 0

            lax.fori_loop(0, ff // ff_step, up_step, 0)

            def down_step(j, _):
                target[j, :, :] = jnp.dot(
                    ffn_hidden[...], down_w[0, :, piece_cols(j)], preferred_element_type=F32
                ).astype(BF16)
                if send:
                    ret_copy(sender, j).start()
                return 0

            lax.fori_loop(0, S, down_step, 0)

        with jax.named_scope("ffnown"):
            expert_block(s, returned.at[s], False)

        scale = lax.rsqrt(squares / D + epsilon)

        def norm_cols(j, _):
            cols = piece_cols(j)
            normed[:, cols] = (hidden[:, cols].astype(F32) * scale * gain_moe_ref[:, cols]).astype(BF16)
            return 0

        def logits(router):
            return lax.dot_general(
                normed[...], router[...], (((1,), (1,)), ((), ())), preferred_element_type=F32
            )

        with jax.named_scope("router"):
            lax.fori_loop(0, S, norm_cols, 0)
            group_exp = jnp.exp(logits(group_router_ref))
            expert_exp = jnp.exp(logits(expert_router_ref))
            group_prob = jnp.sum(
                jnp.where(in_group[:, :G], group_exp, zero), axis=1, keepdims=True
            ) / jnp.sum(group_exp, axis=1, keepdims=True)
            chosen_exp = jnp.where(chosen[:, :E], expert_exp, zero)
            mix = group_prob * chosen_exp / jnp.sum(chosen_exp, axis=1, keepdims=True)
            for e in range(E):
                spreads[e, :, :] = jnp.where(
                    column(slot, e) == slot_iota, column(mix, e), zero
                ).astype(BF16)

        for i, sender in enumerate(others):
            with jax.named_scope(f"dispwait{i}"):
                for j in range(S):
                    disp_wait(sender, j)
            with jax.named_scope(f"ffn{i}"):
                expert_block(sender, results.at[sender], True)

        def combine(j, _):
            cols = piece_cols(j)
            for expert in others:
                ret_wait(expert, j)
            acc = hidden[:, cols].astype(F32)
            for e in range(E):
                acc = acc + jnp.dot(spreads[e], returned[e, j], preferred_element_type=F32)
            out_ref[:, cols] = acc.astype(BF16)
            return 0

        with jax.named_scope("combine"):
            lax.fori_loop(0, S, combine, 0)


        for expert in others:
            for j in range(S):
                disp_copy(expert, j).wait_send()
                ret_copy(expert, j).wait_send()

    with jax.named_scope("sendwait"):
        for zz in range(Z):
            for side, count in ((0, zz + 1), (1, Z - zz)):
                if count < Z:
                    ref = wfull.at[0, pl.ds(0, count * wrows), :]

                    @pl.when(z == zz)
                    def _():
                        remote(
                            ref, ref, wz_send.at[side], wz_recv.at[0, 0], s, partner
                        ).wait_send()

        ref = wfull.at[0 : S - 1, pl.ds(0, (Z - 1) * wrows), :]
        remote(ref, ref, wx_send.at[0], wx_recv.at[0, 0, 0], order[1], t).wait_send()
        ref = wfull.at[:, pl.ds(0, Z * wrows), :]
        remote(ref, ref, wp_send.at[0], wp_recv.at[0], s, partner).wait_send()
        ref = conv_out.at[0 : T - 1]
        remote(ref, ref, a2a_send.at[0], a2a_recv.at[0], s, partner).wait_send()


def body(
    S,
    T,
    conv_value,
    conv_gate,
    doc_ids,
    conv_kernel,
    norm_gain_conv,
    norm_bias_conv,
    proj_weight,
    residual,
    norm_gain_moe,
    group_router,
    expert_router,
    routing,
    expert_gate_w,
    expert_up_w,
    expert_down_w,
):
    tokens, width = conv_value.shape
    rows, D = residual.shape
    wrows = proj_weight.shape[0]
    ff = expert_gate_w.shape[2]
    G = group_router.shape[1]
    E = expert_router.shape[1]
    cap = 2 * rows // E
    hbm = pl.BlockSpec(memory_space=pl.ANY)
    dma = pltpu.SemaphoreType.DMA
    piece = D // S
    Z = T // 2
    paired = S == 4 and E == S and E == 2 * G
    return pl.pallas_call(
        functools.partial(kernel, S, T, G),
        out_shape=pltpu.VMEM((rows, D), BF16),
        in_specs=[hbm] * 15,
        out_specs=pl.BlockSpec(memory_space=pltpu.VMEM),
        scratch_shapes=[
            pltpu.VMEM((1, tokens), jnp.int32),
            pltpu.VMEM(conv_kernel.shape, BF16),
            pltpu.VMEM((1, T * width), F32),
            pltpu.VMEM((1, T * width), F32),
            pltpu.VMEM((1, D), F32),
            pltpu.VMEM((G, D), BF16),
            pltpu.VMEM((E, D), BF16),
            pltpu.VMEM((2, rows), jnp.int32),
            pltpu.VMEM((tokens, width), BF16),
            pltpu.VMEM((tokens, width), BF16),
            pltpu.VMEM((S, T * wrows, piece), BF16),
            pltpu.VMEM((rows, D), BF16),
            pltpu.VMEM((1, D, ff), BF16),
            pltpu.VMEM((1, D, ff), BF16),
            pltpu.VMEM((1, ff, D), BF16),
            pltpu.VMEM((HALO + 16, width), BF16),
            pltpu.VMEM((HALO + 16, width), BF16),
            pltpu.VMEM((tokens + HALO, width), F32),
            pltpu.VMEM((32, width), F32),
            pltpu.VMEM((tokens, 128), F32),
            pltpu.VMEM((T, rows, width), BF16),
            pltpu.VMEM((T, rows, width), BF16),
            pltpu.VMEM((rows, T * width), BF16),
            pltpu.VMEM((rows, D), BF16),
            pltpu.VMEM((rows, D), BF16),
            pltpu.VMEM((cap, D), BF16),
            pltpu.VMEM((E, cap, rows), BF16),
            pltpu.VMEM((E, rows, cap), BF16),
            pltpu.VMEM((E, S, cap, piece), BF16),
            pltpu.VMEM((E, S, cap, piece), BF16),
            pltpu.VMEM((cap, ff), BF16),
            pltpu.VMEM((E, S, cap, piece), BF16),
            pltpu.VMEM((E, S, cap, piece), BF16),
            pltpu.VMEM((G + E + (-G - E) % 8, D), BF16),
            pltpu.VMEM((ff, D // T), BF16),
            pltpu.VMEM((T, ff, D // T), BF16),
            pltpu.VMEM((2, cap, ff), BF16),
            pltpu.VMEM((2, cap, ff), BF16),
            pltpu.VMEM((2, cap, ff), BF16),
            pltpu.VMEM((T, cap, D // T), BF16),
            pltpu.VMEM((T, cap, D // T), BF16),
            pltpu.VMEM((2, rows, ff), BF16),
            pltpu.VMEM((2, rows, cap), BF16),
            pltpu.VMEM((T, rows, D // T), F32),
            dma((15,)),
            dma((S,)),
            dma((2,)),
            dma((2,)),
            dma((Z, 2)),
            dma((1,)),
            dma((S - 1, Z, 2)),
            dma((1,)),
            dma((S,)),
            dma((1,)),
            dma((1,)),
            dma((1, 1) if paired else (S, S)),
            dma((1, 1) if paired else (S, S)),
            dma((1, 1) if paired else (S, S)),
            dma((1, 1) if paired else (S, S)),
            dma((1,)),
            dma((CHUNKS * (S + 2),)),
            dma((1,)),
            dma((2, CHUNKS)),
            dma((1,)),
            dma((T,)),
            dma((2,)),
            dma((Z,)),
            dma((1,)),
            dma((Z,)),
            dma((2,)),
        ],
        compiler_params=pltpu.CompilerParams(
            collective_id=0, has_side_effects=True, vmem_limit_bytes=60 * 1024 * 1024
        ),
    )(
        conv_value,
        conv_gate,
        doc_ids[None, :],
        conv_kernel,
        norm_gain_conv[None, :],
        norm_bias_conv[None, :],
        proj_weight,
        residual,
        norm_gain_moe[None, :],
        group_router.T,
        expert_router.T,
        routing.T,
        expert_gate_w,
        expert_up_w,
        expert_down_w,
    )


def solution(mesh):
    placed = (
        P("sp", "tp"),
        P("sp", "tp"),
        P("sp"),
        P(None, "tp"),
        P(),
        P(),
        P("tp", None),
        P(("sp", "tp"), None),
        P(),
        P(),
        P(),
        P(("sp", "tp"), None),
        P("sp", None, None),
        P("sp", None, None),
        P("sp", None, None),
    )
    return jax.shard_map(
        functools.partial(body, mesh.shape["sp"], mesh.shape["tp"]),
        mesh=mesh,
        in_specs=placed,
        out_specs=P(("sp", "tp"), None),
        check_vma=False,
    )
```
